32 devices in a mesh: ep: 8 (over z, core), tp: 4 (over y, x).
Axes of the slice: x: 2, y: 2, z: 4, core: 2. Of those that a mesh axis runs over, the one named last changes fastest.
Arguments:
- mixer_rows: bfloat16 [4096, 2048], P('ep', 'tp'), may hold values from -6 to 6
- expert_rows: bfloat16 [4096, 2048], P('ep', 'tp'), may hold values from -6 to 6
- mixer_gain: float32 [2048], replicated, may hold values from 0.1 to 1.9
- pool_scale: float32 [2048], P('tp'), may hold values from 0.1 to 1.9
- w_in: bfloat16 [2048, 2048], P(None, 'tp'), may hold values from -0.125 to 0.125
- w_mix_out: bfloat16 [2048, 2048], P(None, 'tp'), may hold values from -0.125 to 0.125
- expert_gain: float32 [2048], replicated, may hold values from 0.1 to 1.9
- expert_gate: bfloat16 [8, 2048, 2048], P('ep', None, 'tp'), may hold values from -0.125 to 0.125
- expert_up: bfloat16 [8, 2048, 2048], P('ep', None, 'tp'), may hold values from -0.125 to 0.125
- expert_down: bfloat16 [8, 2048, 2048], P('ep', None, 'tp'), may hold values from -0.125 to 0.125
- routes: int32 [4096, 2], P('ep'), may hold values from 0 to 7, all different within a row; in each aligned block of 512 rows (0 to 511, 512 to 1023, ...) at most 192 rows name the same one
- route_weight: float32 [4096, 2], P('ep'), may hold values from 0.1 to 1
Outputs:
- mixer_output: bfloat16 [4096, 2048], P('ep', 'tp')
- expert_output: bfloat16 [4096, 2048], P('ep', 'tp')
The draws below stay inside these ranges and needn't reach their ends.
Inputs may be any that keep to these rules, and one draw needn't show every extreme that they name: `routes`: each row names 2 different experts. Among the rows of one device (aligned blocks of 512 rows) no expert is named more than 192 times, a bound that some block reaches.
All inputs are finite; a program needn't handle non-finite values.
Results may differ from the reference program's by a relative error of at most 0.0071.
Values may be sent and summed in bfloat16 or wider, within the bound.
A program may use at most 64 MiB of HBM per device.

```python
import math
import jax
import jax.numpy as jnp
import numpy as np
from jax import lax

D = 2048
PW = 2048
FE = 2048
TOP = 2
TOK_DEV = 512
TOKENS = 4096
EXPERTS = 8
CAP = 192
N_EP = 8


def steps_of(own_key, dims, pieces, smallest, top_value):
    def one(axis_at, parts):
        draws = jax.random.uniform(jax.random.fold_in(jax.random.fold_in(own_key, 6), axis_at), (parts,), jnp.float32, smallest / len(pieces), top_value / len(pieces))
        return jnp.repeat(jnp.exp(draws), dims[axis_at] // parts).reshape((-1,) + (1,) * (len(dims) - axis_at - 1))

    loudness = one(*pieces[0])
    for cut in pieces[1:]:
        loudness = loudness * one(*cut)
    return loudness


def shared_out(key, own, number, rows, amount, top, most, skew):
    sequence = jax.random.permutation(key, amount)
    crowded, common = portions_of(amount, rows * top, most, skew, True), portions_of(amount, rows * top, most, skew, False)
    places = jnp.arange(amount)

    def named(tallies, turn):
        used = int((tallies > 0).sum())
        fixed = max(1, used // 4)
        moved = fixed + (places - fixed + turn * (used - fixed)) % max(1, amount - fixed)
        return jnp.zeros((amount,), jnp.int32).at[sequence[jnp.where(places < fixed, places, moved)]].set(jnp.asarray(tallies, jnp.int32))

    tallies = jnp.where(number % 4 == 0, named(crowded, number // 4), named(common, number - number // 4 - 1))
    mixed = jax.random.permutation(jax.random.fold_in(own, 3), amount)
    donor, sink = mixed[0:amount // 2 * 2:2], mixed[1:amount // 2 * 2:2]
    room = jnp.minimum(tallies[donor] - 1, most - tallies[sink]) // 2
    room = jnp.where((donor == sequence[0]) | (sink == sequence[0]) | (tallies[sink] == 0), 0, jnp.maximum(room, 0))
    moved = jax.random.randint(jax.random.fold_in(own, 4), (amount // 2,), 0, 1 << 20) % (room + 1)
    tallies = tallies.at[donor].add(-moved).at[sink].add(moved)
    members = jnp.searchsorted(jnp.cumsum(tallies), jnp.arange(rows * top), side="right").astype(jnp.int32)
    listing = members.reshape(top, rows).T
    listing = listing[jax.random.permutation(jax.random.fold_in(own, 1), rows)]
    turn = jax.random.randint(jax.random.fold_in(own, 2), (rows, 1), 0, top)
    return jnp.take_along_axis(listing, (jnp.arange(top)[None, :] + turn) % top, axis=1)


def portions_of(count, total, reach, slope, full):
    loads = [(1 << 20) // math.isqrt(grade ** slope) + 1 for grade in range(1, count + 1)]
    largest = reach if full else min(reach, max(-(-total // count), total * loads[0] // sum(loads)))
    least = 1 if total - largest >= count - 1 else 0
    holding, rest = [largest] + [least] * (count - 1), total - largest - least * (count - 1)
    while rest > 0:
        movable = [i for i in range(1, count) if holding[i] < largest] or [i for i in range(1, count) if holding[i] < reach]
        pool, remaining = sum([loads[i] for i in movable]), rest
        for i in movable:
            extra = min(reach - holding[i], max(1, remaining * loads[i] // pool), rest)
            holding[i] = holding[i] + extra
            rest = rest - extra
    return np.array(holding)


def gaussian(stream_key, extent, deviation, most, shards=(), kind=jnp.bfloat16):
    entries = jax.random.normal(stream_key, extent, jnp.float32) * deviation
    if len(shards) > 0:
        entries = steps_of(stream_key, extent, shards, -0.22, 0.18) * entries
    return jnp.clip(entries, min=-most, max=most).astype(kind)


def setup_inputs(seed: int = 0) -> dict:
    key_list = jax.random.split(jax.random.key(seed), 13)
    mixer_rows = gaussian(key_list[0], (TOKENS, D), 1.0, 6.0, ((0, 8), (1, 4)))
    expert_rows = gaussian(key_list[1], (TOKENS, D), 1.0, 6.0, ((0, 8), (1, 4)))
    mixer_gain = jnp.clip(1.0 + 0.18 * jax.random.normal(key_list[2], (D,), jnp.float32), 0.1, 1.9)
    pool_scale = jnp.clip(1.0 + 0.18 * jax.random.normal(key_list[3], (PW,), jnp.float32), 0.1, 1.9)
    w_in = gaussian(key_list[4], (D, PW), D ** -0.5, 0.125, ((1, 4),))
    w_mix_out = gaussian(key_list[5], (PW, D), PW ** -0.5, 0.125, ((1, 4),))
    expert_gain = jnp.clip(1.0 + 0.18 * jax.random.normal(key_list[6], (D,), jnp.float32), 0.1, 1.9)
    expert_gate = gaussian(key_list[7], (EXPERTS, D, FE), D ** -0.5, 0.125, ((0, 8), (2, 4)))
    expert_up = gaussian(key_list[8], (EXPERTS, D, FE), D ** -0.5, 0.125, ((0, 8), (2, 4)))
    expert_down = gaussian(key_list[9], (EXPERTS, FE, D), FE ** -0.5, 0.125, ((0, 8), (2, 4)))
    routes_keys = jax.random.split(jax.random.fold_in(key_list[10], 1), TOKENS // TOK_DEV)
    routes_turns = jax.random.permutation(jax.random.fold_in(key_list[10], 3), TOKENS // TOK_DEV)
    routes = jax.vmap(lambda own, number: shared_out(jax.random.fold_in(key_list[10], 2), own, number, TOK_DEV, EXPERTS, TOP, CAP, 1))(routes_keys, routes_turns).reshape((TOKENS, TOP))
    route_weight = jnp.clip(jnp.exp(math.log(1.0) - 2.3025851 * jax.random.uniform(key_list[11], (TOKENS, TOP), jnp.float32) ** steps_of(key_list[11], (TOKENS, TOP), ((0, 8),), -0.2, 0.2)), 0.1, 1.0)
    return {"mixer_rows": mixer_rows, "expert_rows": expert_rows, "mixer_gain": mixer_gain, "pool_scale": pool_scale, "w_in": w_in, "w_mix_out": w_mix_out, "expert_gain": expert_gain, "expert_gate": expert_gate, "expert_up": expert_up, "expert_down": expert_down, "routes": routes, "route_weight": route_weight}


norm_eps = 1e-05
pool_windows = (2, 4, 8, 16)

def layer_norm(row_block, gain_vec):
    values = row_block.astype(jnp.float32)
    center = values - lax.optimization_barrier(jnp.mean(values, axis=-1, keepdims=True))
    spread = lax.optimization_barrier(jnp.mean(center * center, axis=-1, keepdims=True))
    return (center * lax.rsqrt(spread + norm_eps) * gain_vec).astype(jnp.bfloat16)

def reference(mixer_rows, expert_rows, mixer_gain, pool_scale, w_in, w_mix_out, expert_gain, expert_gate, expert_up, expert_down, routes, route_weight):
    normed_mix = layer_norm(mixer_rows, mixer_gain)
    inner_proj = jnp.dot(normed_mix, w_in, preferred_element_type=jnp.float32).astype(jnp.bfloat16)
    values = inner_proj.astype(jnp.float32)
    seq_len = values.shape[0]
    prefix = jnp.concatenate([jnp.zeros((1, PW), jnp.float32), jnp.cumsum(values, axis=0)], axis=0)
    position = jnp.arange(seq_len, dtype=jnp.int32)
    group_width = PW // 4
    window_means = []
    for group_id, window in enumerate(pool_windows):
        lower_end = jnp.clip(position - window // 2, 0, seq_len)
        upper_end = jnp.clip(position - window // 2 + window, 0, seq_len)
        counts = (upper_end - lower_end).astype(jnp.float32)[:, None]
        columns = prefix[:, group_id * group_width:(group_id + 1) * group_width]
        window_means.append((columns[upper_end] - columns[lower_end]) / counts)
    pooled = ((jnp.concatenate(window_means, axis=1) - values) * pool_scale).astype(jnp.bfloat16)
    mixer_output = jnp.dot(pooled, w_mix_out, preferred_element_type=jnp.float32).astype(jnp.bfloat16)
    normed_expert = layer_norm(expert_rows, expert_gain)
    flat_route = routes.reshape(-1).astype(jnp.int32)
    onehot = (flat_route[:, None] == jnp.arange(EXPERTS, dtype=jnp.int32)[None, :]).astype(jnp.int32)
    running = jnp.cumsum(onehot.reshape(N_EP, TOK_DEV * TOP, EXPERTS), axis=1).reshape(-1, EXPERTS)
    ranking = lax.optimization_barrier(jnp.sum(onehot * (running - 1), axis=1))
    source_dev = jnp.arange(TOKENS * TOP, dtype=jnp.int32) // (TOK_DEV * TOP)
    slot_index = (flat_route * N_EP + source_dev) * CAP + ranking
    token_index = jnp.arange(TOKENS * TOP, dtype=jnp.int32) // TOP
    slot_table = jnp.zeros((EXPERTS * N_EP * CAP, D), jnp.bfloat16).at[slot_index].set(normed_expert[token_index])

    def run_expert(packed):
        slot_rows, gate_weight, up_weight, down_weight = packed
        gate_val = jnp.dot(slot_rows, gate_weight, preferred_element_type=jnp.float32)
        up_val = jnp.dot(slot_rows, up_weight, preferred_element_type=jnp.float32)
        hidden = (jax.nn.silu(gate_val) * up_val).astype(jnp.bfloat16)
        return jnp.dot(hidden, down_weight, preferred_element_type=jnp.float32).astype(jnp.bfloat16)
    results = lax.map(run_expert, (slot_table.reshape(EXPERTS, N_EP * CAP, D), expert_gate, expert_up, expert_down))
    picked = results.reshape(-1, D)[slot_index].astype(jnp.float32).reshape(TOKENS, TOP, D)
    expert_output = lax.optimization_barrier(jnp.sum(picked * route_weight[:, :, None], axis=1)).astype(jnp.bfloat16)
    return (mixer_output, expert_output)
```

```python
import functools

import jax
import jax.numpy as jnp
from jax import lax
from jax.experimental import pallas as pl
from jax.experimental.pallas import tpu as pltpu
from jax.sharding import PartitionSpec as P

TOP = 2
norm_eps = 1e-05
pool_windows = (2, 4, 8, 16)
RIM = 16
AHEAD = 3
BEHIND = 3
POOL_AT = 7
MESH = pl.DeviceIdType.MESH
f32 = jnp.float32
bf16 = jnp.bfloat16


def fused(
    ep,
    tp,
    xm_in,
    xe_in,
    gain_m,
    gain_e,
    scale,
    route_rows,
    rw_rows,
    w_in_h,
    w_mix_h,
    gate_h,
    up_h,
    down_h,
    out_m,
    out_e,
    w_in,
    w_mix,
    gate,
    up,
    down,
    xm,
    normed,
    block,
    disp_send,
    slots,
    hid,
    pooled,
    back_send,
    back_recv,
    ext,
    rim_send,
    rim_recv,
    acc,
    as_rows,
    as_cols,
    w_sem,
    sl_s,
    sl_r,
    xm_s,
    xm_r,
    dp_s,
    dp_r,
    rim_s,
    rim_r,
    po_s,
    po_r,
    hi_s,
    hi_r,
    bk_s,
    bk_r,
):
    me_ep = lax.axis_index("ep")
    me_tp = lax.axis_index("tp")
    rows, feat = xm_in.shape
    cap = slots.shape[2]
    chan = out_m.shape[1]
    width = feat * tp
    chunk = min(rows, 128)

    barrier = pltpu.get_barrier_semaphore()
    for d in range(1, tp):
        pl.semaphore_signal(
            barrier, inc=1, device_id={"tp": lax.rem(me_tp + d, tp)}, device_id_type=MESH
        )
    for d in range(1, ep):
        pl.semaphore_signal(
            barrier, inc=1, device_id={"ep": lax.rem(me_ep + d, ep)}, device_id_type=MESH
        )
    pl.semaphore_wait(barrier, tp + ep - 2)

    def tp_copy(ref, s, r, peer):
        return pltpu.make_async_remote_copy(
            src_ref=ref,
            dst_ref=ref,
            send_sem=s,
            recv_sem=r,
            device_id={"tp": peer},
            device_id_type=MESH,
        )

    def ep_copy(src, dst, s, r, d):
        return pltpu.make_async_remote_copy(
            src_ref=src,
            dst_ref=dst,
            send_sem=s,
            recv_sem=r,
            device_id={"ep": lax.rem(me_ep + d, ep)},
            device_id_type=MESH,
        )

    relayed = tp == 4
    col = lax.rem(me_tp, 2)
    row = me_tp // 2
    beside = row * 2 + (1 - col)
    above = (1 - row) * 2 + col
    across = (1 - row) * 2 + (1 - col)

    def send(slot, s, r):
        if relayed:
            tp_copy(slot(me_tp), s(0), r(0), beside).start()
            tp_copy(slot(me_tp), s(1), r(1), above).start()
        else:
            for d in range(1, tp):
                tp_copy(slot(me_tp), s(d - 1), r(d - 1), lax.rem(me_tp + d, tp)).start()

    def relay(slot, s, r, turn):
        if relayed:
            tp_copy(slot(beside), s(0), r(0), beside).wait_recv()
            tp_copy(slot(above), s(1), r(1), above).wait_recv()
            source = (1 - turn) * beside + turn * above
            peer = (1 - turn) * above + turn * beside
            tp_copy(slot(source), s(2), r(2), peer).start()

    def finish(slot, s, r):
        if relayed:
            tp_copy(slot(across), s(2), r(2), across).wait_recv()
        else:
            for d in range(1, tp):
                p = lax.rem(me_tp - d + tp, tp)
                tp_copy(slot(p), s(d - 1), r(d - 1), p).wait_recv()

    def drain(slot, s, r):
        for d in range(1, tp):
            tp_copy(slot(me_tp), s(d - 1), r(d - 1), lax.rem(me_tp + d, tp)).wait_send()

    def mixer_part():
        return lambda p: xm.at[p], lambda j: xm_s.at[j], lambda j: xm_r.at[j]

    def pooled_part():
        return lambda p: pooled.at[p], lambda j: po_s.at[j], lambda j: po_r.at[j]

    def slot_part(k):
        q = ep_from(k)
        return lambda p: slots.at[q, p], lambda j: sl_s.at[k, j], lambda j: sl_r.at[k, j]

    def hidden_part(k):
        q = ep_from(k)
        return lambda p: hid.at[q, p], lambda j: hi_s.at[k, j], lambda j: hi_r.at[k, j]

    def ep_from(d):
        return lax.rem(me_ep - d + ep, ep)

    xm_load = pltpu.make_async_copy(xm_in, xm.at[me_tp], w_sem.at[5])
    xm_load.start()
    xm_load.wait()
    send(*mixer_part())

    loads = [
        pltpu.make_async_copy(h, v, w_sem.at[i])
        for i, (h, v) in enumerate(
            ((w_in_h, w_in), (gate_h, gate), (up_h, up), (w_mix_h, w_mix), (down_h, down))
        )
    ]
    for load in loads:
        load.start()

    t0 = lax.broadcasted_iota(jnp.int32, (rows, rows), 0)
    t1 = lax.broadcasted_iota(jnp.int32, (rows, rows), 1)
    names = lax.broadcasted_iota(jnp.int32, (ep, rows), 0)
    named = [jnp.where(route_rows[j : j + 1, :] == names, 1.0, 0.0) for j in range(TOP)]
    ahead = jnp.dot(
        sum(named).astype(bf16),
        jnp.where(t0 < t1, 1.0, 0.0).astype(bf16),
        preferred_element_type=f32,
    )
    trow = [
        route_rows[j : j + 1, :] * cap
        + jnp.sum(named[j] * ahead, axis=0, keepdims=True).astype(jnp.int32)
        for j in range(TOP)
    ]
    as_rows[...] = jnp.zeros_like(as_rows)
    for j in range(TOP):
        as_rows[j : j + 1, :] = trow[j].astype(f32)
        as_rows[TOP + j : TOP + j + 1, :] = rw_rows[j : j + 1, :]
    as_cols[...] = as_rows[...].T

    def picked_rows(e):
        slot = lax.broadcasted_iota(jnp.int32, (cap, rows), 0) + e * cap
        hit = (slot == trow[0]) | (slot == trow[1])
        pick = jnp.where(hit, 1.0, 0.0).astype(bf16)
        return jnp.dot(pick, xe_in[...], preferred_element_type=f32).astype(bf16)

    def send_rows(d, carry):
        e = lax.rem(me_ep + d, ep)
        disp_send[e] = picked_rows(e)
        ep_copy(disp_send.at[e], slots.at[me_ep, me_tp], dp_s.at[d], dp_r.at[d], d).start()
        return carry

    lax.fori_loop(1, ep, send_rows, 0)
    slots[me_ep, me_tp] = picked_rows(me_ep)
    relay(*mixer_part(), 0)

    def arrive(k):
        q = ep_from(k)
        ep_copy(disp_send.at[q], slots.at[q, me_tp], dp_s.at[k], dp_r.at[k], k).wait_recv()
        send(*slot_part(k))

    arrive(1)

    def pass_slots(k, carry):
        arrive(k)
        relay(*slot_part(k - 1), lax.rem(k, 2))
        return carry

    early = ep // 2
    lax.fori_loop(2, early, pass_slots, 0)

    def norm_rows(parts, gain):
        parts = [v.astype(f32) for v in parts]
        mean = sum(jnp.sum(v, axis=-1, keepdims=True) for v in parts) / width
        parts = [v - mean for v in parts]
        spread = sum(jnp.sum(v * v, axis=-1, keepdims=True) for v in parts) / width
        inv = lax.rsqrt(spread + norm_eps)
        return [
            (v * inv * gain[:, p * feat : (p + 1) * feat]).astype(bf16)
            for p, v in enumerate(parts)
        ]

    finish(*mixer_part())
    loads[0].wait()

    def project(i, carry):
        at = pl.ds(pl.multiple_of(i * chunk, chunk), chunk)
        for p, v in enumerate(norm_rows([xm[p, at, :] for p in range(tp)], gain_m)):
            normed[:, p * feat : (p + 1) * feat] = v
        inner = jnp.dot(normed[...], w_in[...], preferred_element_type=f32).astype(bf16)
        ext[pl.ds(pl.multiple_of(RIM + i * chunk, RIM), chunk), :] = inner.astype(f32)
        return carry

    lax.fori_loop(0, rows // chunk, project, 0)
    rim_send[0] = ext[rows : rows + RIM, :].astype(bf16)
    rim_send[1] = ext[RIM : 2 * RIM, :].astype(bf16)
    up_rim = ep_copy(rim_send.at[0], rim_recv.at[0], rim_s.at[0], rim_r.at[0], 1)
    down_rim = ep_copy(rim_send.at[1], rim_recv.at[1], rim_s.at[1], rim_r.at[1], ep - 1)
    up_rim.start()
    down_rim.start()

    lax.fori_loop(early, ep - 1, pass_slots, 0)

    up_rim.wait_recv()
    down_rim.wait_recv()
    low = rim_recv[0].astype(f32)
    high = rim_recv[1].astype(f32)
    ext[0:RIM, :] = jnp.where(me_ep > 0, low, 0.0)
    ext[RIM + rows : 2 * RIM + rows, :] = jnp.where(me_ep < ep - 1, high, 0.0)

    group_width = chan * tp // len(pool_windows)
    channel = me_tp * chan + lax.broadcasted_iota(jnp.int32, (1, chan), 1)
    seq_len = rows * ep
    for i in range(rows // chunk):
        first = RIM + i * chunk
        position = me_ep * rows + i * chunk + lax.broadcasted_iota(jnp.int32, (chunk, 1), 0)
        running = jnp.zeros((chunk, chan), f32)
        result = jnp.zeros((chunk, chan), f32)
        last = 0
        for g, window in enumerate(pool_windows):
            half = window // 2
            for o in list(range(-half, -last)) + list(range(last, half)):
                running = running + ext[first + o : first + o + chunk, :]
            last = half
            lower = jnp.maximum(position - half, 0)
            upper = jnp.minimum(position + half, seq_len)
            counts = (upper - lower).astype(f32)
            member = (channel >= g * group_width) & (channel < (g + 1) * group_width)
            result = jnp.where(member, running / counts, result)
        values = ext[first : first + chunk, :]
        pooled[me_tp, i * chunk : (i + 1) * chunk, :] = (
            (result - values) * scale[...]
        ).astype(bf16)
    send(*pooled_part())
    pass_slots(ep - 1, 0)
    send(*slot_part(0))

    loads[1].wait()
    loads[2].wait()

    def hidden_step(k):
        q = ep_from(k)
        finish(*slot_part(k))
        for p, v in enumerate(norm_rows([slots[q, p] for p in range(tp)], gain_e)):
            block[:, p * feat : (p + 1) * feat] = v
        x = block[...]
        g = jnp.dot(x, gate[...], preferred_element_type=f32)
        u = jnp.dot(x, up[...], preferred_element_type=f32)
        hid[q, me_tp] = (g / (1.0 + jnp.exp(-g)) * u).astype(bf16)
        send(*hidden_part(k))

    units = hid.shape[3]

    def value_step(k):
        q = ep_from(k)
        finish(*hidden_part(k))
        total = jnp.zeros((cap, out_e.shape[1]), f32)
        for p in range(tp):
            total = total + jnp.dot(
                hid[q, p],
                down[p * units : (p + 1) * units, :],
                preferred_element_type=f32,
            )
        return total.astype(bf16)

    def send_value(k):
        q = ep_from(k)
        back_send[q] = value_step(k)
        ep_copy(back_send.at[q], back_recv.at[me_ep], bk_s.at[k], bk_r.at[k], ep - k).start()

    hidden_step(1)
    relay(*slot_part(ep - 1), ep % 2)
    hidden_step(2)
    relay(*slot_part(0), 1 - ep % 2)
    relay(*pooled_part(), 1)
    relay(*hidden_part(1), 0)

    loads[3].wait()
    finish(*pooled_part())

    def mix_out(i, carry):
        at = pl.ds(pl.multiple_of(i * chunk, chunk), chunk)
        total = jnp.zeros((chunk, chan), f32)
        for p in range(tp):
            total = total + jnp.dot(
                pooled[p, at, :],
                w_mix[p * chan : (p + 1) * chan, :],
                preferred_element_type=f32,
            )
        out_m[at, :] = total.astype(bf16)
        return carry

    lax.fori_loop(0, rows // chunk, mix_out, 0)
    loads[4].wait()

    def expert(k, carry):
        hidden_step(k)
        relay(*hidden_part(k - 1), lax.rem(k, 2))
        send_value(k - 2)
        return carry

    lax.fori_loop(3, ep, expert, 0)
    hidden_step(0)
    relay(*hidden_part(ep - 1), ep % 2)
    send_value(ep - 2)
    relay(*hidden_part(0), 1 - ep % 2)
    send_value(ep - 1)

    def combine(e):
        slot = lax.broadcasted_iota(jnp.int32, (rows, cap), 1) + e * cap
        weight = jnp.zeros((rows, cap), f32)
        for j in range(TOP):
            own_slot = as_cols[:, j : j + 1].astype(jnp.int32)
            weight = weight + jnp.where(slot == own_slot, as_cols[:, TOP + j : TOP + j + 1], 0.0)
        coarse = weight.astype(bf16)
        fine = (weight - coarse.astype(f32)).astype(bf16)
        v = back_recv[e]
        return jnp.dot(coarse, v, preferred_element_type=f32) + jnp.dot(
            fine, v, preferred_element_type=f32
        )

    acc[...] = jnp.zeros_like(acc)

    def gather_value(k, carry):
        e = lax.rem(me_ep + k, ep)
        ep_copy(back_send.at[e], back_recv.at[e], bk_s.at[k], bk_r.at[k], k).wait_recv()
        acc[...] += combine(e)
        return carry

    lax.fori_loop(1, ep - 2, gather_value, 0)
    back_recv[me_ep] = value_step(0)
    acc[...] += combine(me_ep)
    lax.fori_loop(ep - 2, ep, gather_value, 0)
    out_e[...] = acc[...].astype(bf16)

    drain(*mixer_part())
    drain(*pooled_part())
    up_rim.wait_send()
    down_rim.wait_send()

    def drain_ep(k, carry):
        e = lax.rem(me_ep + k, ep)
        q = ep_from(k)
        ep_copy(disp_send.at[e], slots.at[me_ep, me_tp], dp_s.at[k], dp_r.at[k], k).wait_send()
        ep_copy(back_send.at[q], back_recv.at[me_ep], bk_s.at[k], bk_r.at[k], ep - k).wait_send()
        return carry

    lax.fori_loop(1, ep, drain_ep, 0)

    def drain_tp(k, carry):
        drain(*slot_part(k))
        drain(*hidden_part(k))
        return carry

    lax.fori_loop(0, ep, drain_tp, 0)


def square(
    ep,
    tp,
    xm_in,
    xe_in,
    gain_m,
    gain_e,
    scale,
    route_rows,
    rw_rows,
    w_in_h,
    w_mix_h,
    gate_h,
    up_h,
    down_h,
    out_m,
    out_e,
    w_in,
    w_mix,
    gate,
    up,
    down,
    xm,
    normed,
    block,
    disp_send,
    slots,
    hid,
    pooled,
    back_send,
    back_recv,
    ext,
    rim_send,
    rim_recv,
    acc,
    fin_send,
    fin_recv,
    as_rows,
    as_cols,
    w_sem,
    sl_s,
    sl_r,
    xm_s,
    xm_r,
    dp_s,
    dp_r,
    rim_s,
    rim_r,
    po_s,
    po_r,
    hi_s,
    hi_r,
    bk_s,
    bk_r,
    dn_s,
    dn_r,
    fi_s,
    fi_r,
):
    me_ep = lax.axis_index("ep")
    me_tp = lax.axis_index("tp")
    rows, feat = xe_in.shape
    cap = slots.shape[2]
    chan = out_m.shape[1]
    units = hid.shape[3]
    cols = out_e.shape[1]
    width = feat * tp
    chunk = min(rows, 128)

    col = lax.rem(me_tp, 2)
    row = me_tp // 2
    beside = row * 2 + (1 - col)
    above = (1 - row) * 2 + col
    across = (1 - row) * 2 + (1 - col)

    barrier = pltpu.get_barrier_semaphore()
    for d in range(1, tp):
        pl.semaphore_signal(
            barrier, inc=1, device_id={"tp": lax.rem(me_tp + d, tp)}, device_id_type=MESH
        )
    for d in range(1, ep):
        pl.semaphore_signal(
            barrier, inc=1, device_id={"ep": lax.rem(me_ep + d, ep)}, device_id_type=MESH
        )

    xm_load = pltpu.make_async_copy(xm_in, xm.at[me_tp], w_sem.at[0])
    xm_load.start()

    def unit_rows(r, c):
        return pl.ds(pl.multiple_of((r * 2 + c) * units, units), units)

    loads = [
        pltpu.make_async_copy(h, v, w_sem.at[i + 1])
        for i, (h, v) in enumerate(
            (
                (w_in_h, w_in),
                (gate_h, gate),
                (up_h, up),
                (w_mix_h, w_mix),
                (down_h.at[unit_rows(0, col), :], down.at[col, 0]),
                (down_h.at[unit_rows(1, col), :], down.at[col, 1]),
            )
        )
    ]
    for load in loads:
        load.start()

    def tp_copy(src, dst, s, r, peer):
        return pltpu.make_async_remote_copy(
            src_ref=src,
            dst_ref=dst,
            send_sem=s,
            recv_sem=r,
            device_id={"tp": peer},
            device_id_type=MESH,
        )

    def ep_copy(src, dst, s, r, d):
        return pltpu.make_async_remote_copy(
            src_ref=src,
            dst_ref=dst,
            send_sem=s,
            recv_sem=r,
            device_id={"ep": lax.rem(me_ep + d, ep)},
            device_id_type=MESH,
        )

    def send(slot, s, r):
        mine = slot(me_tp)
        tp_copy(mine, mine, s(0), r(0), beside).start()
        tp_copy(mine, mine, s(1), r(1), above).start()

    def relay(slot, s, r, turn):
        tp_copy(slot(beside), slot(beside), s(0), r(0), beside).wait_recv()
        tp_copy(slot(above), slot(above), s(1), r(1), above).wait_recv()
        source = slot((1 - turn) * beside + turn * above)
        tp_copy(source, source, s(2), r(2), (1 - turn) * above + turn * beside).start()

    def finish(slot, s, r):
        tp_copy(slot(across), slot(across), s(2), r(2), across).wait_recv()

    def drain(slot, s, r):
        mine = slot(me_tp)
        for j in range(3):
            tp_copy(mine, mine, s(j), r(j), beside).wait_send()

    def mixer_part():
        return lambda p: xm.at[p], lambda j: xm_s.at[j], lambda j: xm_r.at[j]

    def pooled_part():
        return lambda p: pooled.at[p], lambda j: po_s.at[j], lambda j: po_r.at[j]

    def ep_from(d):
        return lax.rem(me_ep - d + ep, ep)

    def slot_part(k):
        q = ep_from(k)
        return lambda p: slots.at[q, p], lambda j: sl_s.at[k, j], lambda j: sl_r.at[k, j]

    def hidden_copy(k, part):
        ref = hid.at[ep_from(k), part]
        return tp_copy(ref, ref, hi_s.at[k], hi_r.at[k], above)

    def down_copy(r):
        return tp_copy(
            down_h.at[unit_rows(r, 1 - col), :], down.at[col, r], dn_s.at[r], dn_r.at[r], beside
        )

    t0 = lax.broadcasted_iota(jnp.int32, (rows, rows), 0)
    t1 = lax.broadcasted_iota(jnp.int32, (rows, rows), 1)
    names = lax.broadcasted_iota(jnp.int32, (ep, rows), 0)
    named = [jnp.where(route_rows[j : j + 1, :] == names, 1.0, 0.0) for j in range(TOP)]
    ahead = jnp.dot(
        sum(named).astype(bf16),
        jnp.where(t0 < t1, 1.0, 0.0).astype(bf16),
        preferred_element_type=f32,
    )
    trow = [
        route_rows[j : j + 1, :] * cap
        + jnp.sum(named[j] * ahead, axis=0, keepdims=True).astype(jnp.int32)
        for j in range(TOP)
    ]
    as_rows[...] = jnp.zeros_like(as_rows)
    for j in range(TOP):
        as_rows[j : j + 1, :] = trow[j].astype(f32)
        as_rows[TOP + j : TOP + j + 1, :] = rw_rows[j : j + 1, :]
    as_cols[...] = as_rows[...].T

    xm_load.wait()
    pl.semaphore_wait(barrier, tp + ep - 2)
    send(*mixer_part())

    def picked_rows(e):
        slot = lax.broadcasted_iota(jnp.int32, (cap, rows), 0) + e * cap
        hit = (slot == trow[0]) | (slot == trow[1])
        pick = jnp.where(hit, 1.0, 0.0).astype(bf16)
        return jnp.dot(pick, xe_in[...], preferred_element_type=f32).astype(bf16)

    def send_rows(d, carry):
        e = lax.rem(me_ep + d, ep)
        disp_send[e] = picked_rows(e)
        ep_copy(disp_send.at[e], slots.at[me_ep, me_tp], dp_s.at[d], dp_r.at[d], d).start()
        return carry

    lax.fori_loop(1, ep, send_rows, 0)
    slots[me_ep, me_tp] = picked_rows(me_ep)
    down_copy(0).start()

    def arrive(k):
        q = ep_from(k)
        ep_copy(disp_send.at[q], slots.at[q, me_tp], dp_s.at[k], dp_r.at[k], k).wait_recv()
        send(*slot_part(k))

    arrive(1)
    down_copy(1).start()
    relay(*mixer_part(), 0)
    for k in range(2, AHEAD + 1):
        arrive(k)

    def norm_rows(parts, gain):
        parts = [v.astype(f32) for v in parts]
        mean = sum(jnp.sum(v, axis=-1, keepdims=True) for v in parts) / width
        parts = [v - mean for v in parts]
        spread = sum(jnp.sum(v * v, axis=-1, keepdims=True) for v in parts) / width
        inv = lax.rsqrt(spread + norm_eps)
        return [
            (v * inv * gain[:, p * feat : (p + 1) * feat]).astype(bf16)
            for p, v in enumerate(parts)
        ]

    relay(*slot_part(1), 0)
    finish(*mixer_part())
    loads[0].wait()

    def project(i, carry):
        at = pl.ds(pl.multiple_of(i * chunk, chunk), chunk)
        for p, v in enumerate(norm_rows([xm[p, at, :] for p in range(tp)], gain_m)):
            normed[:, p * feat : (p + 1) * feat] = v
        inner = jnp.dot(normed[...], w_in[...], preferred_element_type=f32).astype(bf16)
        ext[pl.ds(pl.multiple_of(RIM + i * chunk, RIM), chunk), :] = inner.astype(f32)
        return carry

    lax.fori_loop(0, rows // chunk, project, 0)
    rim_send[0] = ext[rows : rows + RIM, :].astype(bf16)
    rim_send[1] = ext[RIM : 2 * RIM, :].astype(bf16)
    up_rim = ep_copy(rim_send.at[0], rim_recv.at[0], rim_s.at[0], rim_r.at[0], 1)
    down_rim = ep_copy(rim_send.at[1], rim_recv.at[1], rim_s.at[1], rim_r.at[1], ep - 1)
    up_rim.start()
    down_rim.start()
    for load in loads[1:]:
        load.wait()

    def hidden_step(k):
        q = ep_from(k)
        finish(*slot_part(k))
        for p, v in enumerate(norm_rows([slots[q, p] for p in range(tp)], gain_e)):
            block[:, p * feat : (p + 1) * feat] = v
        x = block[...]
        g = jnp.dot(x, gate[...], preferred_element_type=f32)
        u = jnp.dot(x, up[...], preferred_element_type=f32)
        hid[q, row] = (g / (1.0 + jnp.exp(-g)) * u).astype(bf16)
        hidden_copy(k, row).start()

    def value_step(k):
        q = ep_from(k)
        hidden_copy(k, 1 - row).wait_recv()
        return [
            (
                jnp.dot(hid[q, 0], down[c, 0], preferred_element_type=f32)
                + jnp.dot(hid[q, 1], down[c, 1], preferred_element_type=f32)
            ).astype(bf16)
            for c in range(2)
        ]

    def send_value(k):
        q = ep_from(k)
        for c, v in enumerate(value_step(k)):
            back_send[q, c] = v
        ep_copy(back_send.at[q], back_recv.at[me_ep], bk_s.at[k], bk_r.at[k], ep - k).start()

    def combine(e):
        slot = lax.broadcasted_iota(jnp.int32, (rows, cap), 1) + e * cap
        weight = jnp.zeros((rows, cap), f32)
        for j in range(TOP):
            own_slot = as_cols[:, j : j + 1].astype(jnp.int32)
            weight = weight + jnp.where(slot == own_slot, as_cols[:, TOP + j : TOP + j + 1], 0.0)
        coarse = weight.astype(bf16)
        fine = (weight - coarse.astype(f32)).astype(bf16)
        for c in range(2):
            v = back_recv[e, c]
            acc[c] += jnp.dot(coarse, v, preferred_element_type=f32) + jnp.dot(
                fine, v, preferred_element_type=f32
            )

    def gather_value(k):
        e = lax.rem(me_ep + k, ep)
        ep_copy(back_send.at[e], back_recv.at[e], bk_s.at[k], bk_r.at[k], k).wait_recv()
        combine(e)

    def pool():
        up_rim.wait_recv()
        down_rim.wait_recv()
        low = rim_recv[0].astype(f32)
        high = rim_recv[1].astype(f32)
        ext[0:RIM, :] = jnp.where(me_ep > 0, low, 0.0)
        ext[RIM + rows : 2 * RIM + rows, :] = jnp.where(me_ep < ep - 1, high, 0.0)
        group_width = chan * tp // len(pool_windows)
        channel = me_tp * chan + lax.broadcasted_iota(jnp.int32, (1, chan), 1)
        seq_len = rows * ep
        for i in range(rows // chunk):
            first = RIM + i * chunk
            position = me_ep * rows + i * chunk + lax.broadcasted_iota(jnp.int32, (chunk, 1), 0)
            running = jnp.zeros((chunk, chan), f32)
            result = jnp.zeros((chunk, chan), f32)
            last = 0
            for g, window in enumerate(pool_windows):
                half = window // 2
                for o in list(range(-half, -last)) + list(range(last, half)):
                    running = running + ext[first + o : first + o + chunk, :]
                last = half
                lower = jnp.maximum(position - half, 0)
                upper = jnp.minimum(position + half, seq_len)
                counts = (upper - lower).astype(f32)
                member = (channel >= g * group_width) & (channel < (g + 1) * group_width)
                result = jnp.where(member, running / counts, result)
            values = ext[first : first + chunk, :]
            pooled[me_tp, i * chunk : (i + 1) * chunk, :] = (
                (result - values) * scale[...]
            ).astype(bf16)
        send(*pooled_part())

    acc[...] = jnp.zeros_like(acc)

    def step(i, carry):
        @pl.when(i + AHEAD + 1 < ep)
        def _():
            arrive(lax.rem(i + AHEAD + 1, ep))

        @pl.when(i + AHEAD + 1 == ep)
        def _():
            send(*slot_part(0))

        @pl.when(i + 1 < ep)
        def _():
            relay(*slot_part(lax.rem(i + 2, ep)), 1)

        hidden_step(lax.rem(i + 1, ep))

        @pl.when(i == POOL_AT)
        def _():
            pool()

        @pl.when(i == 0)
        def _():
            for r in range(2):
                down_copy(r).wait_recv()

        @pl.when(i > 0)
        def _():
            send_value(i)

        @pl.when(i > BEHIND)
        def _():
            gather_value(i - BEHIND)

        return carry

    lax.fori_loop(0, ep, step, 0)
    relay(*pooled_part(), 0)
    for c, v in enumerate(value_step(0)):
        back_recv[me_ep, c] = v
    combine(me_ep)

    def rest(k, carry):
        gather_value(k)
        return carry

    lax.fori_loop(ep - BEHIND, ep, rest, 0)
    fin_send[...] = acc[1 - col].astype(bf16)
    final = tp_copy(fin_send, fin_recv, fi_s.at[0], fi_r.at[0], beside)
    final.start()

    finish(*pooled_part())

    def mix_out(i, carry):
        at = pl.ds(pl.multiple_of(i * chunk, chunk), chunk)
        total = jnp.zeros((chunk, chan), f32)
        for p in range(tp):
            total = total + jnp.dot(
                pooled[p, at, :],
                w_mix[p * chan : (p + 1) * chan, :],
                preferred_element_type=f32,
            )
        out_m[at, :] = total.astype(bf16)
        return carry

    lax.fori_loop(0, rows // chunk, mix_out, 0)
    final.wait_recv()
    out_e[...] = (acc[col] + fin_recv[...].astype(f32)).astype(bf16)

    final.wait_send()
    drain(*mixer_part())
    drain(*pooled_part())
    up_rim.wait_send()
    down_rim.wait_send()
    for r in range(2):
        down_copy(r).wait_send()

    def drain_ep(k, carry):
        e = lax.rem(me_ep + k, ep)
        q = ep_from(k)
        ep_copy(disp_send.at[e], slots.at[me_ep, me_tp], dp_s.at[k], dp_r.at[k], k).wait_send()
        ep_copy(back_send.at[q], back_recv.at[me_ep], bk_s.at[k], bk_r.at[k], ep - k).wait_send()
        return carry

    lax.fori_loop(1, ep, drain_ep, 0)

    def drain_tp(k, carry):
        drain(*slot_part(k))
        hidden_copy(k, row).wait_send()
        return carry

    lax.fori_loop(0, ep, drain_tp, 0)


def square_scratch(ep, tp, rows, feat, cap, chan, units, cols, shapes):
    dma = pltpu.SemaphoreType.DMA
    width = feat * tp
    w_in, w_mix, gate, up = shapes
    return [
        pltpu.VMEM(w_in, bf16),
        pltpu.VMEM(w_mix, bf16),
        pltpu.VMEM(gate, bf16),
        pltpu.VMEM(up, bf16),
        pltpu.VMEM((2, 2, units, cols), bf16),
        pltpu.VMEM((tp, rows, feat), bf16),
        pltpu.VMEM((min(rows, 128), width), bf16),
        pltpu.VMEM((cap, width), bf16),
        pltpu.VMEM((ep, cap, feat), bf16),
        pltpu.VMEM((ep, tp, cap, feat), bf16),
        pltpu.VMEM((ep, 2, cap, units), bf16),
        pltpu.VMEM((tp, rows, chan), bf16),
        pltpu.VMEM((ep, 2, cap, cols), bf16),
        pltpu.VMEM((ep, 2, cap, cols), bf16),
        pltpu.VMEM((rows + 2 * RIM, chan), f32),
        pltpu.VMEM((2, RIM, chan), bf16),
        pltpu.VMEM((2, RIM, chan), bf16),
        pltpu.VMEM((2, rows, cols), f32),
        pltpu.VMEM((rows, cols), bf16),
        pltpu.VMEM((rows, cols), bf16),
        pltpu.VMEM((8, rows), f32),
        pltpu.VMEM((rows, 8), f32),
        dma((7,)),
        dma((ep, 3)),
        dma((ep, 3)),
        dma((3,)),
        dma((3,)),
        dma((ep,)),
        dma((ep,)),
        dma((2,)),
        dma((2,)),
        dma((3,)),
        dma((3,)),
        dma((ep,)),
        dma((ep,)),
        dma((ep,)),
        dma((ep,)),
        dma((2,)),
        dma((2,)),
        dma((1,)),
        dma((1,)),
    ]


def on_device(
    mixer_rows,
    expert_rows,
    mixer_gain,
    pool_scale,
    w_in,
    w_mix_out,
    expert_gain,
    expert_gate,
    expert_up,
    expert_down,
    routes,
    route_weight,
    *,
    ep,
    tp,
):
    rows, feat = mixer_rows.shape
    width = feat * tp
    cap = (3 * TOP * rows + 2 * ep - 1) // (2 * ep)
    chan = w_in.shape[1]
    units = expert_gate.shape[2]
    vmem = pl.BlockSpec(memory_space=pltpu.VMEM)
    hbm = pl.BlockSpec(memory_space=pl.ANY)
    dma = pltpu.SemaphoreType.DMA
    square_ok = tp == 4 and ep > AHEAD + 1
    whole_scratch = [
        pltpu.VMEM(w_in.shape, bf16),
        pltpu.VMEM(w_mix_out.shape, bf16),
        pltpu.VMEM(expert_gate.shape[1:], bf16),
        pltpu.VMEM(expert_up.shape[1:], bf16),
        pltpu.VMEM(expert_down.shape[1:], bf16),
        pltpu.VMEM((tp, rows, feat), bf16),
        pltpu.VMEM((min(rows, 128), width), bf16),
        pltpu.VMEM((cap, width), bf16),
        pltpu.VMEM((ep, cap, feat), bf16),
        pltpu.VMEM((ep, tp, cap, feat), bf16),
        pltpu.VMEM((ep, tp, cap, units), bf16),
        pltpu.VMEM((tp, rows, chan), bf16),
        pltpu.VMEM((ep, cap, expert_down.shape[2]), bf16),
        pltpu.VMEM((ep, cap, expert_down.shape[2]), bf16),
        pltpu.VMEM((rows + 2 * RIM, chan), f32),
        pltpu.VMEM((2, RIM, chan), bf16),
        pltpu.VMEM((2, RIM, chan), bf16),
        pltpu.VMEM((rows, expert_down.shape[2]), f32),
        pltpu.VMEM((8, rows), f32),
        pltpu.VMEM((rows, 8), f32),
        dma((6,)),
        dma((ep, tp - 1)),
        dma((ep, tp - 1)),
        dma((tp - 1,)),
        dma((tp - 1,)),
        dma((ep,)),
        dma((ep,)),
        dma((2,)),
        dma((2,)),
        dma((tp - 1,)),
        dma((tp - 1,)),
        dma((ep, tp - 1)),
        dma((ep, tp - 1)),
        dma((ep,)),
        dma((ep,)),
    ]
    if square_ok:
        shapes = (w_in.shape, w_mix_out.shape, expert_gate.shape[1:], expert_up.shape[1:])
        cols = expert_down.shape[2]
        whole_scratch = square_scratch(ep, tp, rows, feat, cap, chan, units, cols, shapes)
    return pl.pallas_call(
        functools.partial(square if square_ok else fused, ep, tp),
        out_shape=(
            jax.ShapeDtypeStruct((rows, w_mix_out.shape[1]), bf16),
            jax.ShapeDtypeStruct((rows, expert_down.shape[2]), bf16),
        ),
        in_specs=[hbm if square_ok else vmem] + [vmem] * 6 + [hbm] * 5,
        out_specs=(vmem, vmem),
        scratch_shapes=whole_scratch,
        compiler_params=pltpu.CompilerParams(
            collective_id=0, has_side_effects=True, vmem_limit_bytes=62 * 1024 * 1024
        ),
    )(
        mixer_rows,
        expert_rows,
        mixer_gain.reshape(1, width),
        expert_gain.reshape(1, width),
        pool_scale.reshape(1, chan),
        routes.T,
        route_weight.T,
        w_in,
        w_mix_out,
        expert_gate.reshape(expert_gate.shape[1:]),
        expert_up.reshape(expert_up.shape[1:]),
        expert_down.reshape(expert_down.shape[1:]),
    )


def solution(mesh):
    return jax.shard_map(
        functools.partial(on_device, ep=mesh.shape["ep"], tp=mesh.shape["tp"]),
        mesh=mesh,
        in_specs=(
            P("ep", "tp"),
            P("ep", "tp"),
            P(),
            P("tp"),
            P(None, "tp"),
            P(None, "tp"),
            P(),
            P("ep", None, "tp"),
            P("ep", None, "tp"),
            P("ep", None, "tp"),
            P("ep", None),
            P("ep", None),
        ),
        out_specs=(P("ep", "tp"), P("ep", "tp")),
        check_vma=False,
    )
```

```python
import functools

import jax
import jax.numpy as jnp
from jax import lax
from jax.experimental import pallas as pl
from jax.experimental.pallas import tpu as pltpu
from jax.sharding import PartitionSpec as P

TOP = 2
norm_eps = 1e-05
pool_windows = (2, 4, 8, 16)
RIM = 16
ORDER = (
    ("W", 1), ("XMY", 1), ("P", -1), ("XMY", 0), ("W", 2), ("A", 6),
    ("W", 3), ("A", 2), ("A", 7), ("W", 0), ("R", 6), ("R", 2),
    ("R", 7), ("H", 6), ("A", 3), ("A", 1), ("H", 7), ("R", 3),
    ("H", 2), ("V", 6), ("A", 4), ("H", 3), ("R", 1), ("XMX", 1),
    ("V", 7), ("V", 2), ("R", 4), ("A", 5), ("XMX", 0), ("H", 4),
    ("A", 0), ("V", 3), ("R", 5), ("RXM", 1), ("V", 4), ("H", 1),
    ("R", 0), ("G", 6), ("RXM", 0), ("H", 5), ("V", 1), ("ENT", -1),
    ("H", 0), ("POOL", -1), ("V", 5), ("V", 0), ("G", 3), ("G", 7),
    ("G", 0), ("G", 1), ("G", 2), ("G", 4), ("RPO", 0), ("G", 5),
    ("RPO", 1), ("EX", -1), ("MIX", 0), ("MIX", 1),
)
SENDS = (
    6, 2, 7, 3, 4, 1, 5,
)
OVER_X = (
    ("R", 0), ("R", 3), ("R", 4), ("R", 5), ("R", 7), ("RXM", 1),
)
PLACES = (
    "ENT", "XMY", "W", "R", "G", "RXM", "A", "RPO",
    "XMX", "H", "EX", "POOL", "MIX", "V",
)
MESH = pl.DeviceIdType.MESH
f32 = jnp.float32
bf16 = jnp.bfloat16


def fused(
    ep,
    tp,
    xm_in,
    xe_in,
    gain_m,
    gain_e,
    scale,
    route_rows,
    rw_rows,
    w_in_h,
    w_mix_h,
    gate_h,
    up_h,
    down_h,
    out_m,
    out_e,
    w_in,
    w_mix,
    gate,
    up,
    down,
    xm,
    normed,
    block,
    disp_send,
    slots,
    hid,
    pooled,
    back_send,
    back_recv,
    ext,
    rim_send,
    rim_recv,
    acc,
    as_rows,
    as_cols,
    w_sem,
    sl_s,
    sl_r,
    xm_s,
    xm_r,
    dp_s,
    dp_r,
    rim_s,
    rim_r,
    po_s,
    po_r,
    hi_s,
    hi_r,
    bk_s,
    bk_r,
):
    me_ep = lax.axis_index("ep")
    me_tp = lax.axis_index("tp")
    rows, feat = xm_in.shape
    cap = slots.shape[2]
    chan = out_m.shape[1]
    width = feat * tp
    chunk = min(rows, 128)

    barrier = pltpu.get_barrier_semaphore()
    for d in range(1, tp):
        pl.semaphore_signal(
            barrier, inc=1, device_id={"tp": lax.rem(me_tp + d, tp)}, device_id_type=MESH
        )
    for d in range(1, ep):
        pl.semaphore_signal(
            barrier, inc=1, device_id={"ep": lax.rem(me_ep + d, ep)}, device_id_type=MESH
        )
    pl.semaphore_wait(barrier, tp + ep - 2)

    def tp_copy(ref, s, r, peer):
        return pltpu.make_async_remote_copy(
            src_ref=ref,
            dst_ref=ref,
            send_sem=s,
            recv_sem=r,
            device_id={"tp": peer},
            device_id_type=MESH,
        )

    def ep_copy(src, dst, s, r, d):
        return pltpu.make_async_remote_copy(
            src_ref=src,
            dst_ref=dst,
            send_sem=s,
            recv_sem=r,
            device_id={"ep": lax.rem(me_ep + d, ep)},
            device_id_type=MESH,
        )

    relayed = tp == 4
    col = lax.rem(me_tp, 2)
    row = me_tp // 2
    beside = row * 2 + (1 - col)
    above = (1 - row) * 2 + col
    across = (1 - row) * 2 + (1 - col)

    def send(slot, s, r):
        if relayed:
            tp_copy(slot(me_tp), s(0), r(0), beside).start()
            tp_copy(slot(me_tp), s(1), r(1), above).start()
        else:
            for d in range(1, tp):
                tp_copy(slot(me_tp), s(d - 1), r(d - 1), lax.rem(me_tp + d, tp)).start()

    def relay(slot, s, r, turn):
        if relayed:
            tp_copy(slot(beside), s(0), r(0), beside).wait_recv()
            tp_copy(slot(above), s(1), r(1), above).wait_recv()
            source = (1 - turn) * beside + turn * above
            peer = (1 - turn) * above + turn * beside
            tp_copy(slot(source), s(2), r(2), peer).start()

    def finish(slot, s, r):
        if relayed:
            tp_copy(slot(across), s(2), r(2), across).wait_recv()
        else:
            for d in range(1, tp):
                p = lax.rem(me_tp - d + tp, tp)
                tp_copy(slot(p), s(d - 1), r(d - 1), p).wait_recv()

    def drain(slot, s, r):
        for d in range(1, tp):
            tp_copy(slot(me_tp), s(d - 1), r(d - 1), lax.rem(me_tp + d, tp)).wait_send()

    def mixer_part():
        return lambda p: xm.at[p], lambda j: xm_s.at[j], lambda j: xm_r.at[j]

    def pooled_part():
        return lambda p: pooled.at[p], lambda j: po_s.at[j], lambda j: po_r.at[j]

    def slot_part(k):
        q = ep_from(k)
        return lambda p: slots.at[q, p], lambda j: sl_s.at[k, j], lambda j: sl_r.at[k, j]

    def hidden_part(k):
        q = ep_from(k)
        return lambda p: hid.at[q, p], lambda j: hi_s.at[k, j], lambda j: hi_r.at[k, j]

    def ep_from(d):
        return lax.rem(me_ep - d + ep, ep)

    xm_load = pltpu.make_async_copy(xm_in, xm.at[me_tp], w_sem.at[5])
    xm_load.start()
    xm_load.wait()
    send(*mixer_part())

    loads = [
        pltpu.make_async_copy(h, v, w_sem.at[i])
        for i, (h, v) in enumerate(
            ((w_in_h, w_in), (gate_h, gate), (up_h, up), (w_mix_h, w_mix), (down_h, down))
        )
    ]
    for load in loads:
        load.start()

    t0 = lax.broadcasted_iota(jnp.int32, (rows, rows), 0)
    t1 = lax.broadcasted_iota(jnp.int32, (rows, rows), 1)
    names = lax.broadcasted_iota(jnp.int32, (ep, rows), 0)
    named = [jnp.where(route_rows[j : j + 1, :] == names, 1.0, 0.0) for j in range(TOP)]
    ahead = jnp.dot(
        sum(named).astype(bf16),
        jnp.where(t0 < t1, 1.0, 0.0).astype(bf16),
        preferred_element_type=f32,
    )
    trow = [
        route_rows[j : j + 1, :] * cap
        + jnp.sum(named[j] * ahead, axis=0, keepdims=True).astype(jnp.int32)
        for j in range(TOP)
    ]
    as_rows[...] = jnp.zeros_like(as_rows)
    for j in range(TOP):
        as_rows[j : j + 1, :] = trow[j].astype(f32)
        as_rows[TOP + j : TOP + j + 1, :] = rw_rows[j : j + 1, :]
    as_cols[...] = as_rows[...].T

    def picked_rows(e):
        slot = lax.broadcasted_iota(jnp.int32, (cap, rows), 0) + e * cap
        hit = (slot == trow[0]) | (slot == trow[1])
        pick = jnp.where(hit, 1.0, 0.0).astype(bf16)
        return jnp.dot(pick, xe_in[...], preferred_element_type=f32).astype(bf16)

    def send_rows(d, carry):
        e = lax.rem(me_ep + d, ep)
        disp_send[e] = picked_rows(e)
        ep_copy(disp_send.at[e], slots.at[me_ep, me_tp], dp_s.at[d], dp_r.at[d], d).start()
        return carry

    lax.fori_loop(1, ep, send_rows, 0)
    slots[me_ep, me_tp] = picked_rows(me_ep)
    relay(*mixer_part(), 0)

    def arrive(k):
        q = ep_from(k)
        ep_copy(disp_send.at[q], slots.at[q, me_tp], dp_s.at[k], dp_r.at[k], k).wait_recv()
        send(*slot_part(k))

    arrive(1)

    def pass_slots(k, carry):
        arrive(k)
        relay(*slot_part(k - 1), lax.rem(k, 2))
        return carry

    early = ep // 2
    lax.fori_loop(2, early, pass_slots, 0)

    def norm_rows(parts, gain):
        parts = [v.astype(f32) for v in parts]
        mean = sum(jnp.sum(v, axis=-1, keepdims=True) for v in parts) / width
        parts = [v - mean for v in parts]
        spread = sum(jnp.sum(v * v, axis=-1, keepdims=True) for v in parts) / width
        inv = lax.rsqrt(spread + norm_eps)
        return [
            (v * inv * gain[:, p * feat : (p + 1) * feat]).astype(bf16)
            for p, v in enumerate(parts)
        ]

    finish(*mixer_part())
    loads[0].wait()

    def project(i, carry):
        at = pl.ds(pl.multiple_of(i * chunk, chunk), chunk)
        for p, v in enumerate(norm_rows([xm[p, at, :] for p in range(tp)], gain_m)):
            normed[:, p * feat : (p + 1) * feat] = v
        inner = jnp.dot(normed[...], w_in[...], preferred_element_type=f32).astype(bf16)
        ext[pl.ds(pl.multiple_of(RIM + i * chunk, RIM), chunk), :] = inner.astype(f32)
        return carry

    lax.fori_loop(0, rows // chunk, project, 0)
    rim_send[0] = ext[rows : rows + RIM, :].astype(bf16)
    rim_send[1] = ext[RIM : 2 * RIM, :].astype(bf16)
    up_rim = ep_copy(rim_send.at[0], rim_recv.at[0], rim_s.at[0], rim_r.at[0], 1)
    down_rim = ep_copy(rim_send.at[1], rim_recv.at[1], rim_s.at[1], rim_r.at[1], ep - 1)
    up_rim.start()
    down_rim.start()

    lax.fori_loop(early, ep - 1, pass_slots, 0)

    up_rim.wait_recv()
    down_rim.wait_recv()
    low = rim_recv[0].astype(f32)
    high = rim_recv[1].astype(f32)
    ext[0:RIM, :] = jnp.where(me_ep > 0, low, 0.0)
    ext[RIM + rows : 2 * RIM + rows, :] = jnp.where(me_ep < ep - 1, high, 0.0)

    group_width = chan * tp // len(pool_windows)
    channel = me_tp * chan + lax.broadcasted_iota(jnp.int32, (1, chan), 1)
    seq_len = rows * ep
    for i in range(rows // chunk):
        first = RIM + i * chunk
        position = me_ep * rows + i * chunk + lax.broadcasted_iota(jnp.int32, (chunk, 1), 0)
        running = jnp.zeros((chunk, chan), f32)
        result = jnp.zeros((chunk, chan), f32)
        last = 0
        for g, window in enumerate(pool_windows):
            half = window // 2
            for o in list(range(-half, -last)) + list(range(last, half)):
                running = running + ext[first + o : first + o + chunk, :]
            last = half
            lower = jnp.maximum(position - half, 0)
            upper = jnp.minimum(position + half, seq_len)
            counts = (upper - lower).astype(f32)
            member = (channel >= g * group_width) & (channel < (g + 1) * group_width)
            result = jnp.where(member, running / counts, result)
        values = ext[first : first + chunk, :]
        pooled[me_tp, i * chunk : (i + 1) * chunk, :] = (
            (result - values) * scale[...]
        ).astype(bf16)
    send(*pooled_part())
    pass_slots(ep - 1, 0)
    send(*slot_part(0))

    loads[1].wait()
    loads[2].wait()

    def hidden_step(k):
        q = ep_from(k)
        finish(*slot_part(k))
        for p, v in enumerate(norm_rows([slots[q, p] for p in range(tp)], gain_e)):
            block[:, p * feat : (p + 1) * feat] = v
        x = block[...]
        g = jnp.dot(x, gate[...], preferred_element_type=f32)
        u = jnp.dot(x, up[...], preferred_element_type=f32)
        hid[q, me_tp] = (g / (1.0 + jnp.exp(-g)) * u).astype(bf16)
        send(*hidden_part(k))

    units = hid.shape[3]

    def value_step(k):
        q = ep_from(k)
        finish(*hidden_part(k))
        total = jnp.zeros((cap, out_e.shape[1]), f32)
        for p in range(tp):
            total = total + jnp.dot(
                hid[q, p],
                down[p * units : (p + 1) * units, :],
                preferred_element_type=f32,
            )
        return total.astype(bf16)

    def send_value(k):
        q = ep_from(k)
        back_send[q] = value_step(k)
        ep_copy(back_send.at[q], back_recv.at[me_ep], bk_s.at[k], bk_r.at[k], ep - k).start()

    hidden_step(1)
    relay(*slot_part(ep - 1), ep % 2)
    hidden_step(2)
    relay(*slot_part(0), 1 - ep % 2)
    relay(*pooled_part(), 1)
    relay(*hidden_part(1), 0)

    loads[3].wait()
    finish(*pooled_part())

    def mix_out(i, carry):
        at = pl.ds(pl.multiple_of(i * chunk, chunk), chunk)
        total = jnp.zeros((chunk, chan), f32)
        for p in range(tp):
            total = total + jnp.dot(
                pooled[p, at, :],
                w_mix[p * chan : (p + 1) * chan, :],
                preferred_element_type=f32,
            )
        out_m[at, :] = total.astype(bf16)
        return carry

    lax.fori_loop(0, rows // chunk, mix_out, 0)
    loads[4].wait()

    def expert(k, carry):
        hidden_step(k)
        relay(*hidden_part(k - 1), lax.rem(k, 2))
        send_value(k - 2)
        return carry

    lax.fori_loop(3, ep, expert, 0)
    hidden_step(0)
    relay(*hidden_part(ep - 1), ep % 2)
    send_value(ep - 2)
    relay(*hidden_part(0), 1 - ep % 2)
    send_value(ep - 1)

    def combine(e):
        slot = lax.broadcasted_iota(jnp.int32, (rows, cap), 1) + e * cap
        weight = jnp.zeros((rows, cap), f32)
        for j in range(TOP):
            own_slot = as_cols[:, j : j + 1].astype(jnp.int32)
            weight = weight + jnp.where(slot == own_slot, as_cols[:, TOP + j : TOP + j + 1], 0.0)
        coarse = weight.astype(bf16)
        fine = (weight - coarse.astype(f32)).astype(bf16)
        v = back_recv[e]
        return jnp.dot(coarse, v, preferred_element_type=f32) + jnp.dot(
            fine, v, preferred_element_type=f32
        )

    acc[...] = jnp.zeros_like(acc)

    def gather_value(k, carry):
        e = lax.rem(me_ep + k, ep)
        ep_copy(back_send.at[e], back_recv.at[e], bk_s.at[k], bk_r.at[k], k).wait_recv()
        acc[...] += combine(e)
        return carry

    lax.fori_loop(1, ep - 2, gather_value, 0)
    back_recv[me_ep] = value_step(0)
    acc[...] += combine(me_ep)
    lax.fori_loop(ep - 2, ep, gather_value, 0)
    out_e[...] = acc[...].astype(bf16)

    drain(*mixer_part())
    drain(*pooled_part())
    up_rim.wait_send()
    down_rim.wait_send()

    def drain_ep(k, carry):
        e = lax.rem(me_ep + k, ep)
        q = ep_from(k)
        ep_copy(disp_send.at[e], slots.at[me_ep, me_tp], dp_s.at[k], dp_r.at[k], k).wait_send()
        ep_copy(back_send.at[q], back_recv.at[me_ep], bk_s.at[k], bk_r.at[k], ep - k).wait_send()
        return carry

    lax.fori_loop(1, ep, drain_ep, 0)

    def drain_tp(k, carry):
        drain(*slot_part(k))
        drain(*hidden_part(k))
        return carry

    lax.fori_loop(0, ep, drain_tp, 0)


def square(
    ep,
    tp,
    xm_in,
    xe_in,
    gain_m,
    gain_e,
    scale,
    route_rows,
    rw_rows,
    w_in_h,
    w_mix_h,
    gate_h,
    up_h,
    down_h,
    out_m,
    out_e,
    w_in,
    w_mix,
    gate,
    up,
    down,
    xm,
    normed,
    block,
    disp_send,
    slots,
    hid,
    pooled,
    back_send,
    back_recv,
    ext,
    rim_send,
    rim_recv,
    acc,
    fin_send,
    fin_recv,
    as_rows,
    as_cols,
    w_sem,
    sl_s,
    sl_r,
    xm_s,
    xm_r,
    dp_s,
    dp_r,
    rim_s,
    rim_r,
    po_s,
    po_r,
    hi_s,
    hi_r,
    bk_s,
    bk_r,
    dn_s,
    dn_r,
    fi_s,
    fi_r,
):
    me_ep = lax.axis_index("ep")
    me_tp = lax.axis_index("tp")
    rows, feat = xe_in.shape
    cap = slots.shape[2]
    chan = out_m.shape[1]
    units = hid.shape[3]
    cols = out_e.shape[1]
    width = feat * tp
    chunk = min(rows, 128)

    col = lax.rem(me_tp, 2)
    row = me_tp // 2
    beside = row * 2 + (1 - col)
    above = (1 - row) * 2 + col
    across = (1 - row) * 2 + (1 - col)

    barrier = pltpu.get_barrier_semaphore()
    for d in range(1, tp):
        pl.semaphore_signal(
            barrier, inc=1, device_id={"tp": lax.rem(me_tp + d, tp)}, device_id_type=MESH
        )
    for d in range(1, ep):
        pl.semaphore_signal(
            barrier, inc=1, device_id={"ep": lax.rem(me_ep + d, ep)}, device_id_type=MESH
        )

    xm_load = pltpu.make_async_copy(xm_in, xm.at[me_tp], w_sem.at[0])
    xm_load.start()

    def unit_rows(r, c):
        return pl.ds(pl.multiple_of((r * 2 + c) * units, units), units)

    piece = units // 2

    loads = [
        pltpu.make_async_copy(h, v, w_sem.at[i + 1])
        for i, (h, v) in enumerate(
            (
                (w_in_h, w_in),
                (gate_h, gate),
                (up_h, up),
                (w_mix_h, w_mix),
                (down_h.at[unit_rows(0, col), :], down.at[col, 0]),
                (down_h.at[unit_rows(1, col), :], down.at[col, 1]),
            )
        )
    ]
    for load in loads:
        load.start()

    def tp_copy(src, dst, s, r, peer):
        return pltpu.make_async_remote_copy(
            src_ref=src,
            dst_ref=dst,
            send_sem=s,
            recv_sem=r,
            device_id={"tp": peer},
            device_id_type=MESH,
        )

    def ep_copy(src, dst, s, r, d):
        return pltpu.make_async_remote_copy(
            src_ref=src,
            dst_ref=dst,
            send_sem=s,
            recv_sem=r,
            device_id={"ep": lax.rem(me_ep + d, ep)},
            device_id_type=MESH,
        )

    def send(slot, s, r):
        mine = slot(me_tp)
        tp_copy(mine, mine, s(0), r(0), beside).start()
        tp_copy(mine, mine, s(1), r(1), above).start()

    def relay(slot, s, r, turn):
        tp_copy(slot(beside), slot(beside), s(0), r(0), beside).wait_recv()
        tp_copy(slot(above), slot(above), s(1), r(1), above).wait_recv()
        source = slot((1 - turn) * beside + turn * above)
        tp_copy(source, source, s(2), r(2), (1 - turn) * above + turn * beside).start()

    def finish(slot, s, r):
        tp_copy(slot(across), slot(across), s(2), r(2), across).wait_recv()

    def drain(slot, s, r):
        mine = slot(me_tp)
        for j in range(3):
            tp_copy(mine, mine, s(j), r(j), beside).wait_send()

    def half_rows(h):
        return pl.ds(pl.multiple_of(h * (rows // 2), rows // 2), rows // 2)

    def mixer_part(h):
        at = half_rows(h)
        return lambda p: xm.at[p, at], lambda j: xm_s.at[h, j], lambda j: xm_r.at[h, j]

    def pooled_part(h):
        at = half_rows(h)
        return lambda p: pooled.at[p, at], lambda j: po_s.at[h, j], lambda j: po_r.at[h, j]

    def ep_from(d):
        return lax.rem(me_ep - d + ep, ep)

    def slot_part(k):
        q = ep_from(k)
        return lambda p: slots.at[q, p], lambda j: sl_s.at[k, j], lambda j: sl_r.at[k, j]

    def hidden_copy(k, part):
        ref = hid.at[ep_from(k), part]
        return tp_copy(ref, ref, hi_s.at[k], hi_r.at[k], above)

    def down_copy(i):
        r, part = i // 2, i % 2
        first = (r * 2 + 1 - col) * units + part * piece
        return tp_copy(
            down_h.at[pl.ds(pl.multiple_of(first, piece), piece), :],
            down.at[col, r, pl.ds(pl.multiple_of(part * piece, piece), piece)],
            dn_s.at[i],
            dn_r.at[i],
            beside,
        )

    def mixer_x(h):
        slot, s, r = mixer_part(h)
        tp_copy(slot(me_tp), slot(me_tp), s(0), r(0), beside).start()

    def mixer_y(h):
        slot, s, r = mixer_part(h)
        tp_copy(slot(me_tp), slot(me_tp), s(1), r(1), above).start()

    t0 = lax.broadcasted_iota(jnp.int32, (rows, rows), 0)
    t1 = lax.broadcasted_iota(jnp.int32, (rows, rows), 1)
    names = lax.broadcasted_iota(jnp.int32, (ep, rows), 0)
    named = [jnp.where(route_rows[j : j + 1, :] == names, 1.0, 0.0) for j in range(TOP)]
    ahead = jnp.dot(
        sum(named).astype(bf16),
        jnp.where(t0 < t1, 1.0, 0.0).astype(bf16),
        preferred_element_type=f32,
    )
    trow = [
        route_rows[j : j + 1, :] * cap
        + jnp.sum(named[j] * ahead, axis=0, keepdims=True).astype(jnp.int32)
        for j in range(TOP)
    ]
    as_rows[...] = jnp.zeros_like(as_rows)
    for j in range(TOP):
        as_rows[j : j + 1, :] = trow[j].astype(f32)
        as_rows[TOP + j : TOP + j + 1, :] = rw_rows[j : j + 1, :]
    as_cols[...] = as_rows[...].T

    xm_load.wait()
    pl.semaphore_wait(barrier, tp + ep - 2)
    starts = {
        "W": lambda k: down_copy(k).start(),
        "XMX": mixer_x,
        "XMY": mixer_y,
    }
    picks_at = ORDER.index(("P", -1))
    for op, k in ORDER[:picks_at]:
        starts[op](k)

    def picked_rows(e):
        slot = lax.broadcasted_iota(jnp.int32, (cap, rows), 0) + e * cap
        hit = (slot == trow[0]) | (slot == trow[1])
        pick = jnp.where(hit, 1.0, 0.0).astype(bf16)
        return jnp.dot(pick, xe_in[...], preferred_element_type=f32).astype(bf16)

    def send_rows(n, carry):
        d = sum(jnp.where(n == i, k, 0) for i, k in enumerate(SENDS))
        e = lax.rem(me_ep + d, ep)
        disp_send[e] = picked_rows(e)
        ep_copy(disp_send.at[e], slots.at[me_ep, me_tp], dp_s.at[d], dp_r.at[d], d).start()
        return carry

    lax.fori_loop(0, ep - 1, send_rows, 0)
    slots[me_ep, me_tp] = picked_rows(me_ep)

    def arrive(k):
        @pl.when(k > 0)
        def _():
            q = ep_from(k)
            ep_copy(disp_send.at[q], slots.at[q, me_tp], dp_s.at[k], dp_r.at[k], k).wait_recv()

        send(*slot_part(k))

    def norm_rows(parts, gain):
        parts = [v.astype(f32) for v in parts]
        mean = sum(jnp.sum(v, axis=-1, keepdims=True) for v in parts) / width
        parts = [v - mean for v in parts]
        spread = sum(jnp.sum(v * v, axis=-1, keepdims=True) for v in parts) / width
        inv = lax.rsqrt(spread + norm_eps)
        return [
            (v * inv * gain[:, p * feat : (p + 1) * feat]).astype(bf16)
            for p, v in enumerate(parts)
        ]

    def project(i, carry):
        at = pl.ds(pl.multiple_of(i * chunk, chunk), chunk)
        for p, v in enumerate(norm_rows([xm[p, at, :] for p in range(tp)], gain_m)):
            normed[:, p * feat : (p + 1) * feat] = v
        inner = jnp.dot(normed[...], w_in[...], preferred_element_type=f32).astype(bf16)
        ext[pl.ds(pl.multiple_of(RIM + i * chunk, RIM), chunk), :] = inner.astype(f32)
        return carry

    up_rim = ep_copy(rim_send.at[0], rim_recv.at[0], rim_s.at[0], rim_r.at[0], 1)
    down_rim = ep_copy(rim_send.at[1], rim_recv.at[1], rim_s.at[1], rim_r.at[1], ep - 1)

    def enter():
        for h in range(2):
            finish(*mixer_part(h))
        lax.fori_loop(0, rows // chunk, project, 0)
        rim_send[0] = ext[rows : rows + RIM, :].astype(bf16)
        rim_send[1] = ext[RIM : 2 * RIM, :].astype(bf16)
        up_rim.start()
        down_rim.start()

    for load in loads:
        load.wait()

    def hidden_step(k):
        q = ep_from(k)
        finish(*slot_part(k))
        for p, v in enumerate(norm_rows([slots[q, p] for p in range(tp)], gain_e)):
            block[:, p * feat : (p + 1) * feat] = v
        x = block[...]
        g = jnp.dot(x, gate[...], preferred_element_type=f32)
        u = jnp.dot(x, up[...], preferred_element_type=f32)
        hid[q, row] = (g / (1.0 + jnp.exp(-g)) * u).astype(bf16)
        hidden_copy(k, row).start()

    def value_step(k):
        q = ep_from(k)
        hidden_copy(k, 1 - row).wait_recv()
        return [
            (
                jnp.dot(hid[q, 0], down[c, 0], preferred_element_type=f32)
                + jnp.dot(hid[q, 1], down[c, 1], preferred_element_type=f32)
            ).astype(bf16)
            for c in range(2)
        ]

    def send_value(k):
        q = ep_from(k)
        values = value_step(k)

        @pl.when(k > 0)
        def _():
            for c in range(2):
                back_send[q, c] = values[c]
            ep_copy(back_send.at[q], back_recv.at[me_ep], bk_s.at[k], bk_r.at[k], ep - k).start()

        @pl.when(k == 0)
        def _():
            for c in range(2):
                back_recv[me_ep, c] = values[c]

    def combine(e):
        slot = lax.broadcasted_iota(jnp.int32, (rows, cap), 1) + e * cap
        weight = jnp.zeros((rows, cap), f32)
        for j in range(TOP):
            own_slot = as_cols[:, j : j + 1].astype(jnp.int32)
            weight = weight + jnp.where(slot == own_slot, as_cols[:, TOP + j : TOP + j + 1], 0.0)
        coarse = weight.astype(bf16)
        fine = (weight - coarse.astype(f32)).astype(bf16)
        for c in range(2):
            v = back_recv[e, c]
            acc[c] += jnp.dot(coarse, v, preferred_element_type=f32) + jnp.dot(
                fine, v, preferred_element_type=f32
            )

    def gather_value(k):
        e = lax.rem(me_ep + k, ep)

        @pl.when(k > 0)
        def _():
            ep_copy(back_send.at[e], back_recv.at[e], bk_s.at[k], bk_r.at[k], k).wait_recv()

        combine(e)

    def pool():
        up_rim.wait_recv()
        down_rim.wait_recv()
        low = rim_recv[0].astype(f32)
        high = rim_recv[1].astype(f32)
        ext[0:RIM, :] = jnp.where(me_ep > 0, low, 0.0)
        ext[RIM + rows : 2 * RIM + rows, :] = jnp.where(me_ep < ep - 1, high, 0.0)
        group_width = chan * tp // len(pool_windows)
        channel = me_tp * chan + lax.broadcasted_iota(jnp.int32, (1, chan), 1)
        seq_len = rows * ep
        for i in range(rows // chunk):
            first = RIM + i * chunk
            position = me_ep * rows + i * chunk + lax.broadcasted_iota(jnp.int32, (chunk, 1), 0)
            running = jnp.zeros((chunk, chan), f32)
            result = jnp.zeros((chunk, chan), f32)
            last = 0
            for g, window in enumerate(pool_windows):
                half = window // 2
                for o in list(range(-half, -last)) + list(range(last, half)):
                    running = running + ext[first + o : first + o + chunk, :]
                last = half
                lower = jnp.maximum(position - half, 0)
                upper = jnp.minimum(position + half, seq_len)
                counts = (upper - lower).astype(f32)
                member = (channel >= g * group_width) & (channel < (g + 1) * group_width)
                result = jnp.where(member, running / counts, result)
            values = ext[first : first + chunk, :]
            pooled[me_tp, i * chunk : (i + 1) * chunk, :] = (
                (result - values) * scale[...]
            ).astype(bf16)
        for h in range(2):
            send(*pooled_part(h))

    acc[...] = jnp.zeros_like(acc)

    final = tp_copy(fin_send, fin_recv, fi_s.at[0], fi_r.at[0], beside)

    def exchange(k):
        fin_send[...] = acc[1 - col].astype(bf16)
        final.start()

    def mix_out(h):
        finish(*pooled_part(h))

        def mix(i, carry):
            at = pl.ds(pl.multiple_of(h * (rows // 2) + i * chunk, chunk), chunk)
            total = jnp.zeros((chunk, chan), f32)
            for p in range(tp):
                total = total + jnp.dot(
                    pooled[p, at, :],
                    w_mix[p * chan : (p + 1) * chan, :],
                    preferred_element_type=f32,
                )
            out_m[at, :] = total.astype(bf16)
            return carry

        lax.fori_loop(0, rows // 2 // chunk, mix, 0)

    def await_down():
        for i in range(4):
            down_copy(i).wait_recv()

    body = dict(
        starts,
        A=arrive,
        H=hidden_step,
        V=send_value,
        G=gather_value,
        ENT=lambda k: enter(),
        POOL=lambda k: pool(),
        EX=exchange,
        MIX=mix_out,
    )
    turned = {
        "R": lambda k, turn: relay(*slot_part(k), turn),
        "RXM": lambda k, turn: relay(*mixer_part(k), turn),
        "RPO": lambda k, turn: relay(*pooled_part(k), turn),
    }

    steps = [[]]
    for op, k in ORDER[picks_at + 1 :]:
        if steps[-1] and PLACES.index(op) <= PLACES.index(steps[-1][-1][0]):
            steps.append([])
        steps[-1].append((op, k))
    where = {op: [] for op in PLACES}
    for n, entries in enumerate(steps):
        for op, k in entries:
            where[op].append((n, k))

    def step(n, carry):
        for op in PLACES:
            spots = where[op]
            if not spots:
                continue
            due = functools.reduce(jnp.logical_or, [n == i for i, _ in spots])
            k = sum(jnp.where(n == i, v, 0) for i, v in spots)

            @pl.when(due)
            def _(op=op, k=k, spots=spots):
                if op == "V":
                    pl.when(n == spots[0][0])(await_down)
                if op in turned:
                    ups = [i for i, v in spots if (op, v) in OVER_X]
                    turned[op](k, sum(jnp.where(n == i, 1, 0) for i in ups) if ups else 0)
                else:
                    body[op](k)

        return carry

    lax.fori_loop(0, len(steps), step, 0)
    final.wait_recv()
    out_e[...] = (acc[col] + fin_recv[...].astype(f32)).astype(bf16)

    final.wait_send()
    for h in range(2):
        drain(*mixer_part(h))
        drain(*pooled_part(h))
    up_rim.wait_send()
    down_rim.wait_send()
    for i in range(4):
        down_copy(i).wait_send()

    def drain_ep(k, carry):
        e = lax.rem(me_ep + k, ep)
        q = ep_from(k)
        ep_copy(disp_send.at[e], slots.at[me_ep, me_tp], dp_s.at[k], dp_r.at[k], k).wait_send()
        ep_copy(back_send.at[q], back_recv.at[me_ep], bk_s.at[k], bk_r.at[k], ep - k).wait_send()
        return carry

    lax.fori_loop(1, ep, drain_ep, 0)

    def drain_tp(k, carry):
        drain(*slot_part(k))
        hidden_copy(k, row).wait_send()
        return carry

    lax.fori_loop(0, ep, drain_tp, 0)


def square_scratch(ep, tp, rows, feat, cap, chan, units, cols, shapes):
    dma = pltpu.SemaphoreType.DMA
    width = feat * tp
    w_in, w_mix, gate, up = shapes
    return [
        pltpu.VMEM(w_in, bf16),
        pltpu.VMEM(w_mix, bf16),
        pltpu.VMEM(gate, bf16),
        pltpu.VMEM(up, bf16),
        pltpu.VMEM((2, 2, units, cols), bf16),
        pltpu.VMEM((tp, rows, feat), bf16),
        pltpu.VMEM((min(rows, 128), width), bf16),
        pltpu.VMEM((cap, width), bf16),
        pltpu.VMEM((ep, cap, feat), bf16),
        pltpu.VMEM((ep, tp, cap, feat), bf16),
        pltpu.VMEM((ep, 2, cap, units), bf16),
        pltpu.VMEM((tp, rows, chan), bf16),
        pltpu.VMEM((ep, 2, cap, cols), bf16),
        pltpu.VMEM((ep, 2, cap, cols), bf16),
        pltpu.VMEM((rows + 2 * RIM, chan), f32),
        pltpu.VMEM((2, RIM, chan), bf16),
        pltpu.VMEM((2, RIM, chan), bf16),
        pltpu.VMEM((2, rows, cols), f32),
        pltpu.VMEM((rows, cols), bf16),
        pltpu.VMEM((rows, cols), bf16),
        pltpu.VMEM((8, rows), f32),
        pltpu.VMEM((rows, 8), f32),
        dma((7,)),
        dma((ep, 3)),
        dma((ep, 3)),
        dma((2, 3)),
        dma((2, 3)),
        dma((ep,)),
        dma((ep,)),
        dma((2,)),
        dma((2,)),
        dma((2, 3)),
        dma((2, 3)),
        dma((ep,)),
        dma((ep,)),
        dma((ep,)),
        dma((ep,)),
        dma((4,)),
        dma((4,)),
        dma((1,)),
        dma((1,)),
    ]


def on_device(
    mixer_rows,
    expert_rows,
    mixer_gain,
    pool_scale,
    w_in,
    w_mix_out,
    expert_gain,
    expert_gate,
    expert_up,
    expert_down,
    routes,
    route_weight,
    *,
    ep,
    tp,
):
    rows, feat = mixer_rows.shape
    width = feat * tp
    cap = (3 * TOP * rows + 2 * ep - 1) // (2 * ep)
    chan = w_in.shape[1]
    units = expert_gate.shape[2]
    vmem = pl.BlockSpec(memory_space=pltpu.VMEM)
    hbm = pl.BlockSpec(memory_space=pl.ANY)
    dma = pltpu.SemaphoreType.DMA
    square_ok = tp == 4 and ep == len(SENDS) + 1
    whole_scratch = [
        pltpu.VMEM(w_in.shape, bf16),
        pltpu.VMEM(w_mix_out.shape, bf16),
        pltpu.VMEM(expert_gate.shape[1:], bf16),
        pltpu.VMEM(expert_up.shape[1:], bf16),
        pltpu.VMEM(expert_down.shape[1:], bf16),
        pltpu.VMEM((tp, rows, feat), bf16),
        pltpu.VMEM((min(rows, 128), width), bf16),
        pltpu.VMEM((cap, width), bf16),
        pltpu.VMEM((ep, cap, feat), bf16),
        pltpu.VMEM((ep, tp, cap, feat), bf16),
        pltpu.VMEM((ep, tp, cap, units), bf16),
        pltpu.VMEM((tp, rows, chan), bf16),
        pltpu.VMEM((ep, cap, expert_down.shape[2]), bf16),
        pltpu.VMEM((ep, cap, expert_down.shape[2]), bf16),
        pltpu.VMEM((rows + 2 * RIM, chan), f32),
        pltpu.VMEM((2, RIM, chan), bf16),
        pltpu.VMEM((2, RIM, chan), bf16),
        pltpu.VMEM((rows, expert_down.shape[2]), f32),
        pltpu.VMEM((8, rows), f32),
        pltpu.VMEM((rows, 8), f32),
        dma((6,)),
        dma((ep, tp - 1)),
        dma((ep, tp - 1)),
        dma((tp - 1,)),
        dma((tp - 1,)),
        dma((ep,)),
        dma((ep,)),
        dma((2,)),
        dma((2,)),
        dma((tp - 1,)),
        dma((tp - 1,)),
        dma((ep, tp - 1)),
        dma((ep, tp - 1)),
        dma((ep,)),
        dma((ep,)),
    ]
    if square_ok:
        shapes = (w_in.shape, w_mix_out.shape, expert_gate.shape[1:], expert_up.shape[1:])
        cols = expert_down.shape[2]
        whole_scratch = square_scratch(ep, tp, rows, feat, cap, chan, units, cols, shapes)
    return pl.pallas_call(
        functools.partial(square if square_ok else fused, ep, tp),
        out_shape=(
            jax.ShapeDtypeStruct((rows, w_mix_out.shape[1]), bf16),
            jax.ShapeDtypeStruct((rows, expert_down.shape[2]), bf16),
        ),
        in_specs=[hbm if square_ok else vmem] + [vmem] * 6 + [hbm] * 5,
        out_specs=(vmem, vmem),
        scratch_shapes=whole_scratch,
        compiler_params=pltpu.CompilerParams(
            collective_id=0, has_side_effects=True, vmem_limit_bytes=62 * 1024 * 1024
        ),
    )(
        mixer_rows,
        expert_rows,
        mixer_gain.reshape(1, width),
        expert_gain.reshape(1, width),
        pool_scale.reshape(1, chan),
        routes.T,
        route_weight.T,
        w_in,
        w_mix_out,
        expert_gate.reshape(expert_gate.shape[1:]),
        expert_up.reshape(expert_up.shape[1:]),
        expert_down.reshape(expert_down.shape[1:]),
    )


def solution(mesh):
    return jax.shard_map(
        functools.partial(on_device, ep=mesh.shape["ep"], tp=mesh.shape["tp"]),
        mesh=mesh,
        in_specs=(
            P("ep", "tp"),
            P("ep", "tp"),
            P(),
            P("tp"),
            P(None, "tp"),
            P(None, "tp"),
            P(),
            P("ep", None, "tp"),
            P("ep", None, "tp"),
            P("ep", None, "tp"),
            P("ep", None),
            P("ep", None),
        ),
        out_specs=(P("ep", "tp"), P("ep", "tp")),
        check_vma=False,
    )
```

```python
import functools

import jax
import jax.numpy as jnp
from jax import lax
from jax.experimental import pallas as pl
from jax.experimental.pallas import tpu as pltpu
from jax.sharding import PartitionSpec as P

TOP = 2
norm_eps = 1e-05
pool_windows = (2, 4, 8, 16)
RIM = 16
ORDER = (
    ("XMY", 0), ("W", 2), ("W", 1), ("P", -1), ("XMY", 1), ("A", 0),
    ("A", 3), ("A", 4), ("R", 0), ("R", 3), ("R", 4), ("W", 0),
    ("W", 3), ("H", 3), ("H", 4), ("XMX", 0), ("A", 1), ("A", 5),
    ("A", 6), ("A", 2), ("V", 3), ("XMX", 1), ("V", 4), ("R", 5),
    ("R", 6), ("H", 5), ("A", 7), ("R", 2), ("R", 1), ("V", 5),
    ("H", 6), ("G", 4), ("RXM", 1), ("H", 2), ("RXM", 0), ("H", 0),
    ("V", 6), ("R", 7), ("G", 5), ("H", 1), ("ENT", -1), ("V", 2),
    ("H", 7), ("G", 3), ("POOL", -1), ("V", 1), ("V", 0), ("G", 0),
    ("G", 6), ("G", 2), ("V", 7), ("G", 7), ("G", 1), ("EX", -1),
    ("RPO", 0), ("RPO", 1), ("MIX", 0), ("MIX", 1),
)
SENDS = (
    3, 4, 1, 6, 5, 2, 7,
)
OVER_X = (
    ("R", 0), ("R", 2), ("R", 7), ("RXM", 0), ("RXM", 1),
)
PLACES = (
    "W", "RXM", "POOL", "H", "XMY", "XMX", "A", "ENT",
    "V", "R", "G", "EX", "RPO", "MIX",
)
MESH = pl.DeviceIdType.MESH
f32 = jnp.float32
bf16 = jnp.bfloat16


def fused(
    ep,
    tp,
    xm_in,
    xe_in,
    gain_m,
    gain_e,
    scale,
    route_rows,
    rw_rows,
    w_in_h,
    w_mix_h,
    gate_h,
    up_h,
    down_h,
    out_m,
    out_e,
    w_in,
    w_mix,
    gate,
    up,
    down,
    xm,
    normed,
    block,
    disp_send,
    slots,
    hid,
    pooled,
    back_send,
    back_recv,
    ext,
    rim_send,
    rim_recv,
    acc,
    as_rows,
    as_cols,
    w_sem,
    sl_s,
    sl_r,
    xm_s,
    xm_r,
    dp_s,
    dp_r,
    rim_s,
    rim_r,
    po_s,
    po_r,
    hi_s,
    hi_r,
    bk_s,
    bk_r,
):
    me_ep = lax.axis_index("ep")
    me_tp = lax.axis_index("tp")
    rows, feat = xm_in.shape
    cap = slots.shape[2]
    chan = out_m.shape[1]
    width = feat * tp
    chunk = min(rows, 128)

    barrier = pltpu.get_barrier_semaphore()
    for d in range(1, tp):
        pl.semaphore_signal(
            barrier, inc=1, device_id={"tp": lax.rem(me_tp + d, tp)}, device_id_type=MESH
        )
    for d in range(1, ep):
        pl.semaphore_signal(
            barrier, inc=1, device_id={"ep": lax.rem(me_ep + d, ep)}, device_id_type=MESH
        )
    pl.semaphore_wait(barrier, tp + ep - 2)

    def tp_copy(ref, s, r, peer):
        return pltpu.make_async_remote_copy(
            src_ref=ref,
            dst_ref=ref,
            send_sem=s,
            recv_sem=r,
            device_id={"tp": peer},
            device_id_type=MESH,
        )

    def ep_copy(src, dst, s, r, d):
        return pltpu.make_async_remote_copy(
            src_ref=src,
            dst_ref=dst,
            send_sem=s,
            recv_sem=r,
            device_id={"ep": lax.rem(me_ep + d, ep)},
            device_id_type=MESH,
        )

    relayed = tp == 4
    col = lax.rem(me_tp, 2)
    row = me_tp // 2
    beside = row * 2 + (1 - col)
    above = (1 - row) * 2 + col
    across = (1 - row) * 2 + (1 - col)

    def send(slot, s, r):
        if relayed:
            tp_copy(slot(me_tp), s(0), r(0), beside).start()
            tp_copy(slot(me_tp), s(1), r(1), above).start()
        else:
            for d in range(1, tp):
                tp_copy(slot(me_tp), s(d - 1), r(d - 1), lax.rem(me_tp + d, tp)).start()

    def relay(slot, s, r, turn):
        if relayed:
            tp_copy(slot(beside), s(0), r(0), beside).wait_recv()
            tp_copy(slot(above), s(1), r(1), above).wait_recv()
            source = (1 - turn) * beside + turn * above
            peer = (1 - turn) * above + turn * beside
            tp_copy(slot(source), s(2), r(2), peer).start()

    def finish(slot, s, r):
        if relayed:
            tp_copy(slot(across), s(2), r(2), across).wait_recv()
        else:
            for d in range(1, tp):
                p = lax.rem(me_tp - d + tp, tp)
                tp_copy(slot(p), s(d - 1), r(d - 1), p).wait_recv()

    def drain(slot, s, r):
        for d in range(1, tp):
            tp_copy(slot(me_tp), s(d - 1), r(d - 1), lax.rem(me_tp + d, tp)).wait_send()

    def mixer_part():
        return lambda p: xm.at[p], lambda j: xm_s.at[j], lambda j: xm_r.at[j]

    def pooled_part():
        return lambda p: pooled.at[p], lambda j: po_s.at[j], lambda j: po_r.at[j]

    def slot_part(k):
        q = ep_from(k)
        return lambda p: slots.at[q, p], lambda j: sl_s.at[k, j], lambda j: sl_r.at[k, j]

    def hidden_part(k):
        q = ep_from(k)
        return lambda p: hid.at[q, p], lambda j: hi_s.at[k, j], lambda j: hi_r.at[k, j]

    def ep_from(d):
        return lax.rem(me_ep - d + ep, ep)

    xm_load = pltpu.make_async_copy(xm_in, xm.at[me_tp], w_sem.at[5])
    xm_load.start()
    xm_load.wait()
    send(*mixer_part())

    loads = [
        pltpu.make_async_copy(h, v, w_sem.at[i])
        for i, (h, v) in enumerate(
            ((w_in_h, w_in), (gate_h, gate), (up_h, up), (w_mix_h, w_mix), (down_h, down))
        )
    ]
    for load in loads:
        load.start()

    t0 = lax.broadcasted_iota(jnp.int32, (rows, rows), 0)
    t1 = lax.broadcasted_iota(jnp.int32, (rows, rows), 1)
    names = lax.broadcasted_iota(jnp.int32, (ep, rows), 0)
    named = [jnp.where(route_rows[j : j + 1, :] == names, 1.0, 0.0) for j in range(TOP)]
    ahead = jnp.dot(
        sum(named).astype(bf16),
        jnp.where(t0 < t1, 1.0, 0.0).astype(bf16),
        preferred_element_type=f32,
    )
    trow = [
        route_rows[j : j + 1, :] * cap
        + jnp.sum(named[j] * ahead, axis=0, keepdims=True).astype(jnp.int32)
        for j in range(TOP)
    ]
    as_rows[...] = jnp.zeros_like(as_rows)
    for j in range(TOP):
        as_rows[j : j + 1, :] = trow[j].astype(f32)
        as_rows[TOP + j : TOP + j + 1, :] = rw_rows[j : j + 1, :]
    as_cols[...] = as_rows[...].T

    def picked_rows(e):
        slot = lax.broadcasted_iota(jnp.int32, (cap, rows), 0) + e * cap
        hit = (slot == trow[0]) | (slot == trow[1])
        pick = jnp.where(hit, 1.0, 0.0).astype(bf16)
        return jnp.dot(pick, xe_in[...], preferred_element_type=f32).astype(bf16)

    def send_rows(d, carry):
        e = lax.rem(me_ep + d, ep)
        disp_send[e] = picked_rows(e)
        ep_copy(disp_send.at[e], slots.at[me_ep, me_tp], dp_s.at[d], dp_r.at[d], d).start()
        return carry

    lax.fori_loop(1, ep, send_rows, 0)
    slots[me_ep, me_tp] = picked_rows(me_ep)
    relay(*mixer_part(), 0)

    def arrive(k):
        q = ep_from(k)
        ep_copy(disp_send.at[q], slots.at[q, me_tp], dp_s.at[k], dp_r.at[k], k).wait_recv()
        send(*slot_part(k))

    arrive(1)

    def pass_slots(k, carry):
        arrive(k)
        relay(*slot_part(k - 1), lax.rem(k, 2))
        return carry

    early = ep // 2
    lax.fori_loop(2, early, pass_slots, 0)

    def norm_rows(parts, gain):
        parts = [v.astype(f32) for v in parts]
        mean = sum(jnp.sum(v, axis=-1, keepdims=True) for v in parts) / width
        parts = [v - mean for v in parts]
        spread = sum(jnp.sum(v * v, axis=-1, keepdims=True) for v in parts) / width
        inv = lax.rsqrt(spread + norm_eps)
        return [
            (v * inv * gain[:, p * feat : (p + 1) * feat]).astype(bf16)
            for p, v in enumerate(parts)
        ]

    finish(*mixer_part())
    loads[0].wait()

    def project(i, carry):
        at = pl.ds(pl.multiple_of(i * chunk, chunk), chunk)
        for p, v in enumerate(norm_rows([xm[p, at, :] for p in range(tp)], gain_m)):
            normed[:, p * feat : (p + 1) * feat] = v
        inner = jnp.dot(normed[...], w_in[...], preferred_element_type=f32).astype(bf16)
        ext[pl.ds(pl.multiple_of(RIM + i * chunk, RIM), chunk), :] = inner.astype(f32)
        return carry

    lax.fori_loop(0, rows // chunk, project, 0)
    rim_send[0] = ext[rows : rows + RIM, :].astype(bf16)
    rim_send[1] = ext[RIM : 2 * RIM, :].astype(bf16)
    up_rim = ep_copy(rim_send.at[0], rim_recv.at[0], rim_s.at[0], rim_r.at[0], 1)
    down_rim = ep_copy(rim_send.at[1], rim_recv.at[1], rim_s.at[1], rim_r.at[1], ep - 1)
    up_rim.start()
    down_rim.start()

    lax.fori_loop(early, ep - 1, pass_slots, 0)

    up_rim.wait_recv()
    down_rim.wait_recv()
    low = rim_recv[0].astype(f32)
    high = rim_recv[1].astype(f32)
    ext[0:RIM, :] = jnp.where(me_ep > 0, low, 0.0)
    ext[RIM + rows : 2 * RIM + rows, :] = jnp.where(me_ep < ep - 1, high, 0.0)

    group_width = chan * tp // len(pool_windows)
    channel = me_tp * chan + lax.broadcasted_iota(jnp.int32, (1, chan), 1)
    seq_len = rows * ep
    for i in range(rows // chunk):
        first = RIM + i * chunk
        position = me_ep * rows + i * chunk + lax.broadcasted_iota(jnp.int32, (chunk, 1), 0)
        running = jnp.zeros((chunk, chan), f32)
        result = jnp.zeros((chunk, chan), f32)
        last = 0
        for g, window in enumerate(pool_windows):
            half = window // 2
            for o in list(range(-half, -last)) + list(range(last, half)):
                running = running + ext[first + o : first + o + chunk, :]
            last = half
            lower = jnp.maximum(position - half, 0)
            upper = jnp.minimum(position + half, seq_len)
            counts = (upper - lower).astype(f32)
            member = (channel >= g * group_width) & (channel < (g + 1) * group_width)
            result = jnp.where(member, running / counts, result)
        values = ext[first : first + chunk, :]
        pooled[me_tp, i * chunk : (i + 1) * chunk, :] = (
            (result - values) * scale[...]
        ).astype(bf16)
    send(*pooled_part())
    pass_slots(ep - 1, 0)
    send(*slot_part(0))

    loads[1].wait()
    loads[2].wait()

    def hidden_step(k):
        q = ep_from(k)
        finish(*slot_part(k))
        for p, v in enumerate(norm_rows([slots[q, p] for p in range(tp)], gain_e)):
            block[:, p * feat : (p + 1) * feat] = v
        x = block[...]
        g = jnp.dot(x, gate[...], preferred_element_type=f32)
        u = jnp.dot(x, up[...], preferred_element_type=f32)
        hid[q, me_tp] = (g / (1.0 + jnp.exp(-g)) * u).astype(bf16)
        send(*hidden_part(k))

    units = hid.shape[3]

    def value_step(k):
        q = ep_from(k)
        finish(*hidden_part(k))
        total = jnp.zeros((cap, out_e.shape[1]), f32)
        for p in range(tp):
            total = total + jnp.dot(
                hid[q, p],
                down[p * units : (p + 1) * units, :],
                preferred_element_type=f32,
            )
        return total.astype(bf16)

    def send_value(k):
        q = ep_from(k)
        back_send[q] = value_step(k)
        ep_copy(back_send.at[q], back_recv.at[me_ep], bk_s.at[k], bk_r.at[k], ep - k).start()

    hidden_step(1)
    relay(*slot_part(ep - 1), ep % 2)
    hidden_step(2)
    relay(*slot_part(0), 1 - ep % 2)
    relay(*pooled_part(), 1)
    relay(*hidden_part(1), 0)

    loads[3].wait()
    finish(*pooled_part())

    def mix_out(i, carry):
        at = pl.ds(pl.multiple_of(i * chunk, chunk), chunk)
        total = jnp.zeros((chunk, chan), f32)
        for p in range(tp):
            total = total + jnp.dot(
                pooled[p, at, :],
                w_mix[p * chan : (p + 1) * chan, :],
                preferred_element_type=f32,
            )
        out_m[at, :] = total.astype(bf16)
        return carry

    lax.fori_loop(0, rows // chunk, mix_out, 0)
    loads[4].wait()

    def expert(k, carry):
        hidden_step(k)
        relay(*hidden_part(k - 1), lax.rem(k, 2))
        send_value(k - 2)
        return carry

    lax.fori_loop(3, ep, expert, 0)
    hidden_step(0)
    relay(*hidden_part(ep - 1), ep % 2)
    send_value(ep - 2)
    relay(*hidden_part(0), 1 - ep % 2)
    send_value(ep - 1)

    def combine(e):
        slot = lax.broadcasted_iota(jnp.int32, (rows, cap), 1) + e * cap
        weight = jnp.zeros((rows, cap), f32)
        for j in range(TOP):
            own_slot = as_cols[:, j : j + 1].astype(jnp.int32)
            weight = weight + jnp.where(slot == own_slot, as_cols[:, TOP + j : TOP + j + 1], 0.0)
        coarse = weight.astype(bf16)
        fine = (weight - coarse.astype(f32)).astype(bf16)
        v = back_recv[e]
        return jnp.dot(coarse, v, preferred_element_type=f32) + jnp.dot(
            fine, v, preferred_element_type=f32
        )

    acc[...] = jnp.zeros_like(acc)

    def gather_value(k, carry):
        e = lax.rem(me_ep + k, ep)
        ep_copy(back_send.at[e], back_recv.at[e], bk_s.at[k], bk_r.at[k], k).wait_recv()
        acc[...] += combine(e)
        return carry

    lax.fori_loop(1, ep - 2, gather_value, 0)
    back_recv[me_ep] = value_step(0)
    acc[...] += combine(me_ep)
    lax.fori_loop(ep - 2, ep, gather_value, 0)
    out_e[...] = acc[...].astype(bf16)

    drain(*mixer_part())
    drain(*pooled_part())
    up_rim.wait_send()
    down_rim.wait_send()

    def drain_ep(k, carry):
        e = lax.rem(me_ep + k, ep)
        q = ep_from(k)
        ep_copy(disp_send.at[e], slots.at[me_ep, me_tp], dp_s.at[k], dp_r.at[k], k).wait_send()
        ep_copy(back_send.at[q], back_recv.at[me_ep], bk_s.at[k], bk_r.at[k], ep - k).wait_send()
        return carry

    lax.fori_loop(1, ep, drain_ep, 0)

    def drain_tp(k, carry):
        drain(*slot_part(k))
        drain(*hidden_part(k))
        return carry

    lax.fori_loop(0, ep, drain_tp, 0)


def square(
    ep,
    tp,
    xm_in,
    xe_in,
    gain_m,
    gain_e,
    scale,
    route_rows,
    rw_rows,
    w_in_h,
    w_mix_h,
    gate_h,
    up_h,
    down_h,
    out_m,
    out_e,
    w_in,
    w_mix,
    gate,
    up,
    down,
    xm,
    normed,
    block,
    disp_send,
    slots,
    hid,
    pooled,
    back_send,
    back_recv,
    ext,
    rim_send,
    rim_recv,
    acc,
    fin_send,
    fin_recv,
    as_rows,
    as_cols,
    w_sem,
    sl_s,
    sl_r,
    xm_s,
    xm_r,
    dp_s,
    dp_r,
    rim_s,
    rim_r,
    po_s,
    po_r,
    hi_s,
    hi_r,
    bk_s,
    bk_r,
    dn_s,
    dn_r,
    fi_s,
    fi_r,
):
    me_ep = lax.axis_index("ep")
    me_tp = lax.axis_index("tp")
    rows, feat = xe_in.shape
    cap = slots.shape[2]
    chan = out_m.shape[1]
    units = hid.shape[3]
    cols = out_e.shape[1]
    width = feat * tp
    chunk = min(rows, 128)

    not_first = me_ep > 0
    not_last = me_ep < ep - 1
    col = lax.rem(me_tp, 2)
    row = me_tp // 2
    beside = row * 2 + (1 - col)
    above = (1 - row) * 2 + col
    across = (1 - row) * 2 + (1 - col)

    barrier = pltpu.get_barrier_semaphore()
    for d in range(1, tp):
        pl.semaphore_signal(
            barrier, inc=1, device_id={"tp": lax.rem(me_tp + d, tp)}, device_id_type=MESH
        )
    for d in range(1, ep):
        pl.semaphore_signal(
            barrier, inc=1, device_id={"ep": lax.rem(me_ep + d, ep)}, device_id_type=MESH
        )

    xm_load = pltpu.make_async_copy(xm_in, xm.at[me_tp], w_sem.at[0])
    xm_load.start()

    def unit_rows(r, c):
        return pl.ds(pl.multiple_of((r * 2 + c) * units, units), units)

    piece = units // 2

    loads = [
        pltpu.make_async_copy(h, v, w_sem.at[i + 1])
        for i, (h, v) in enumerate(
            (
                (w_in_h, w_in),
                (gate_h, gate),
                (up_h, up),
                (w_mix_h, w_mix),
                (down_h.at[unit_rows(0, col), :], down.at[col, 0]),
                (down_h.at[unit_rows(1, col), :], down.at[col, 1]),
            )
        )
    ]
    for load in loads:
        load.start()

    def tp_copy(src, dst, s, r, peer):
        return pltpu.make_async_remote_copy(
            src_ref=src,
            dst_ref=dst,
            send_sem=s,
            recv_sem=r,
            device_id={"tp": peer},
            device_id_type=MESH,
        )

    def ep_copy(src, dst, s, r, d):
        return pltpu.make_async_remote_copy(
            src_ref=src,
            dst_ref=dst,
            send_sem=s,
            recv_sem=r,
            device_id={"ep": lax.rem(me_ep + d, ep)},
            device_id_type=MESH,
        )

    def send(slot, s, r):
        mine = slot(me_tp)
        tp_copy(mine, mine, s(0), r(0), beside).start()
        tp_copy(mine, mine, s(1), r(1), above).start()

    def relay(slot, s, r, turn):
        tp_copy(slot(beside), slot(beside), s(0), r(0), beside).wait_recv()
        tp_copy(slot(above), slot(above), s(1), r(1), above).wait_recv()
        source = slot((1 - turn) * beside + turn * above)
        tp_copy(source, source, s(2), r(2), (1 - turn) * above + turn * beside).start()

    def finish(slot, s, r):
        tp_copy(slot(across), slot(across), s(2), r(2), across).wait_recv()

    def drain(slot, s, r):
        mine = slot(me_tp)
        for j in range(3):
            tp_copy(mine, mine, s(j), r(j), beside).wait_send()

    def half_rows(h):
        return pl.ds(pl.multiple_of(h * (rows // 2), rows // 2), rows // 2)

    def mixer_part(h):
        at = half_rows(h)
        return lambda p: xm.at[p, at], lambda j: xm_s.at[h, j], lambda j: xm_r.at[h, j]

    def pooled_part(h):
        at = half_rows(h)
        return lambda p: pooled.at[p, at], lambda j: po_s.at[h, j], lambda j: po_r.at[h, j]

    def ep_from(d):
        return lax.rem(me_ep - d + ep, ep)

    def slot_part(k):
        q = ep_from(k)
        return lambda p: slots.at[q, p], lambda j: sl_s.at[k, j], lambda j: sl_r.at[k, j]

    def hidden_copy(k, part):
        ref = hid.at[ep_from(k), part]
        return tp_copy(ref, ref, hi_s.at[k], hi_r.at[k], above)

    def down_copy(i):
        r, part = i // 2, i % 2
        first = (r * 2 + 1 - col) * units + part * piece
        return tp_copy(
            down_h.at[pl.ds(pl.multiple_of(first, piece), piece), :],
            down.at[col, r, pl.ds(pl.multiple_of(part * piece, piece), piece)],
            dn_s.at[i],
            dn_r.at[i],
            beside,
        )

    def mixer_x(h):
        slot, s, r = mixer_part(h)
        tp_copy(slot(me_tp), slot(me_tp), s(0), r(0), beside).start()

    def mixer_y(h):
        slot, s, r = mixer_part(h)
        tp_copy(slot(me_tp), slot(me_tp), s(1), r(1), above).start()

    t0 = lax.broadcasted_iota(jnp.int32, (rows, rows), 0)
    t1 = lax.broadcasted_iota(jnp.int32, (rows, rows), 1)
    names = lax.broadcasted_iota(jnp.int32, (ep, rows), 0)
    named = [jnp.where(route_rows[j : j + 1, :] == names, 1.0, 0.0) for j in range(TOP)]
    ahead = jnp.dot(
        sum(named).astype(bf16),
        jnp.where(t0 < t1, 1.0, 0.0).astype(bf16),
        preferred_element_type=f32,
    )
    trow = [
        route_rows[j : j + 1, :] * cap
        + jnp.sum(named[j] * ahead, axis=0, keepdims=True).astype(jnp.int32)
        for j in range(TOP)
    ]
    as_rows[...] = jnp.zeros_like(as_rows)
    for j in range(TOP):
        as_rows[j : j + 1, :] = trow[j].astype(f32)
        as_rows[TOP + j : TOP + j + 1, :] = rw_rows[j : j + 1, :]
    as_cols[...] = as_rows[...].T

    xm_load.wait()
    pl.semaphore_wait(barrier, tp + ep - 2)
    starts = {
        "W": lambda k: down_copy(k).start(),
        "XMX": mixer_x,
        "XMY": mixer_y,
    }
    picks_at = ORDER.index(("P", -1))
    for op, k in ORDER[:picks_at]:
        starts[op](k)

    def picked_rows(e):
        slot = lax.broadcasted_iota(jnp.int32, (cap, rows), 0) + e * cap
        hit = (slot == trow[0]) | (slot == trow[1])
        pick = jnp.where(hit, 1.0, 0.0).astype(bf16)
        return jnp.dot(pick, xe_in[...], preferred_element_type=f32).astype(bf16)

    def send_rows(n, carry):
        d = sum(jnp.where(n == i, k, 0) for i, k in enumerate(SENDS))
        e = lax.rem(me_ep + d, ep)
        disp_send[e] = picked_rows(e)
        ep_copy(disp_send.at[e], slots.at[me_ep, me_tp], dp_s.at[d], dp_r.at[d], d).start()
        return carry

    lax.fori_loop(0, ep - 1, send_rows, 0)
    slots[me_ep, me_tp] = picked_rows(me_ep)

    def arrive(k):
        @pl.when(k > 0)
        def _():
            q = ep_from(k)
            ep_copy(disp_send.at[q], slots.at[q, me_tp], dp_s.at[k], dp_r.at[k], k).wait_recv()

        send(*slot_part(k))

    def norm_rows(parts, gain):
        parts = [v.astype(f32) for v in parts]
        mean = sum(jnp.sum(v, axis=-1, keepdims=True) for v in parts) / width
        parts = [v - mean for v in parts]
        spread = sum(jnp.sum(v * v, axis=-1, keepdims=True) for v in parts) / width
        inv = lax.rsqrt(spread + norm_eps)
        return [
            (v * inv * gain[:, p * feat : (p + 1) * feat]).astype(bf16)
            for p, v in enumerate(parts)
        ]

    def project(i, carry):
        at = pl.ds(pl.multiple_of(i * chunk, chunk), chunk)
        for p, v in enumerate(norm_rows([xm[p, at, :] for p in range(tp)], gain_m)):
            normed[:, p * feat : (p + 1) * feat] = v
        inner = jnp.dot(normed[...], w_in[...], preferred_element_type=f32).astype(bf16)
        ext[pl.ds(pl.multiple_of(RIM + i * chunk, RIM), chunk), :] = inner.astype(f32)
        return carry

    up_rim = ep_copy(rim_send.at[0], rim_recv.at[0], rim_s.at[0], rim_r.at[0], 1)
    down_rim = ep_copy(rim_send.at[1], rim_recv.at[1], rim_s.at[1], rim_r.at[1], ep - 1)

    def enter():
        for h in range(2):
            finish(*mixer_part(h))
        lax.fori_loop(0, rows // chunk, project, 0)
        rim_send[0] = ext[rows : rows + RIM, :].astype(bf16)
        rim_send[1] = ext[RIM : 2 * RIM, :].astype(bf16)
        pl.when(not_last)(up_rim.start)
        pl.when(not_first)(down_rim.start)

    for load in loads:
        load.wait()

    def hidden_step(k):
        q = ep_from(k)
        finish(*slot_part(k))
        for p, v in enumerate(norm_rows([slots[q, p] for p in range(tp)], gain_e)):
            block[:, p * feat : (p + 1) * feat] = v
        x = block[...]
        g = jnp.dot(x, gate[...], preferred_element_type=f32)
        u = jnp.dot(x, up[...], preferred_element_type=f32)
        hid[q, row] = (g / (1.0 + jnp.exp(-g)) * u).astype(bf16)
        hidden_copy(k, row).start()

    def value_step(k):
        q = ep_from(k)
        hidden_copy(k, 1 - row).wait_recv()
        return [
            (
                jnp.dot(hid[q, 0], down[c, 0], preferred_element_type=f32)
                + jnp.dot(hid[q, 1], down[c, 1], preferred_element_type=f32)
            ).astype(bf16)
            for c in range(2)
        ]

    def send_value(k):
        q = ep_from(k)
        values = value_step(k)

        @pl.when(k > 0)
        def _():
            for c in range(2):
                back_send[q, c] = values[c]
            ep_copy(back_send.at[q], back_recv.at[me_ep], bk_s.at[k], bk_r.at[k], ep - k).start()

        @pl.when(k == 0)
        def _():
            for c in range(2):
                back_recv[me_ep, c] = values[c]

    def combine(e):
        slot = lax.broadcasted_iota(jnp.int32, (rows, cap), 1) + e * cap
        weight = jnp.zeros((rows, cap), f32)
        for j in range(TOP):
            own_slot = as_cols[:, j : j + 1].astype(jnp.int32)
            weight = weight + jnp.where(slot == own_slot, as_cols[:, TOP + j : TOP + j + 1], 0.0)
        coarse = weight.astype(bf16)
        fine = (weight - coarse.astype(f32)).astype(bf16)
        for c in range(2):
            v = back_recv[e, c]
            acc[c] += jnp.dot(coarse, v, preferred_element_type=f32) + jnp.dot(
                fine, v, preferred_element_type=f32
            )

    def gather_value(k):
        e = lax.rem(me_ep + k, ep)

        @pl.when(k > 0)
        def _():
            ep_copy(back_send.at[e], back_recv.at[e], bk_s.at[k], bk_r.at[k], k).wait_recv()

        combine(e)

    def pool():
        ext[0:RIM, :] = jnp.zeros((RIM, chan), f32)
        ext[RIM + rows : 2 * RIM + rows, :] = jnp.zeros((RIM, chan), f32)

        @pl.when(not_first)
        def _():
            up_rim.wait_recv()
            ext[0:RIM, :] = rim_recv[0].astype(f32)

        @pl.when(not_last)
        def _():
            down_rim.wait_recv()
            ext[RIM + rows : 2 * RIM + rows, :] = rim_recv[1].astype(f32)

        group_width = chan * tp // len(pool_windows)
        channel = me_tp * chan + lax.broadcasted_iota(jnp.int32, (1, chan), 1)
        seq_len = rows * ep
        for i in range(rows // chunk):
            first = RIM + i * chunk
            position = me_ep * rows + i * chunk + lax.broadcasted_iota(jnp.int32, (chunk, 1), 0)
            running = jnp.zeros((chunk, chan), f32)
            result = jnp.zeros((chunk, chan), f32)
            last = 0
            for g, window in enumerate(pool_windows):
                half = window // 2
                for o in list(range(-half, -last)) + list(range(last, half)):
                    running = running + ext[first + o : first + o + chunk, :]
                last = half
                lower = jnp.maximum(position - half, 0)
                upper = jnp.minimum(position + half, seq_len)
                counts = (upper - lower).astype(f32)
                member = (channel >= g * group_width) & (channel < (g + 1) * group_width)
                result = jnp.where(member, running / counts, result)
            values = ext[first : first + chunk, :]
            pooled[me_tp, i * chunk : (i + 1) * chunk, :] = (
                (result - values) * scale[...]
            ).astype(bf16)
        for h in range(2):
            send(*pooled_part(h))

    acc[...] = jnp.zeros_like(acc)

    final = tp_copy(fin_send, fin_recv, fi_s.at[0], fi_r.at[0], beside)

    def exchange(k):
        fin_send[...] = acc[1 - col].astype(bf16)
        final.start()

    def mix_out(h):
        finish(*pooled_part(h))

        def mix(i, carry):
            at = pl.ds(pl.multiple_of(h * (rows // 2) + i * chunk, chunk), chunk)
            total = jnp.zeros((chunk, chan), f32)
            for p in range(tp):
                total = total + jnp.dot(
                    pooled[p, at, :],
                    w_mix[p * chan : (p + 1) * chan, :],
                    preferred_element_type=f32,
                )
            out_m[at, :] = total.astype(bf16)
            return carry

        lax.fori_loop(0, rows // 2 // chunk, mix, 0)

    def await_down():
        for i in range(4):
            down_copy(i).wait_recv()

    body = dict(
        starts,
        A=arrive,
        H=hidden_step,
        V=send_value,
        G=gather_value,
        ENT=lambda k: enter(),
        POOL=lambda k: pool(),
        EX=exchange,
        MIX=mix_out,
    )
    turned = {
        "R": lambda k, turn: relay(*slot_part(k), turn),
        "RXM": lambda k, turn: relay(*mixer_part(k), turn),
        "RPO": lambda k, turn: relay(*pooled_part(k), turn),
    }

    steps = [[]]
    for op, k in ORDER[picks_at + 1 :]:
        if steps[-1] and PLACES.index(op) <= PLACES.index(steps[-1][-1][0]):
            steps.append([])
        steps[-1].append((op, k))
    where = {op: [] for op in PLACES}
    for n, entries in enumerate(steps):
        for op, k in entries:
            where[op].append((n, k))

    def step(n, carry):
        for op in PLACES:
            spots = where[op]
            if not spots:
                continue
            due = functools.reduce(jnp.logical_or, [n == i for i, _ in spots])
            k = sum(jnp.where(n == i, v, 0) for i, v in spots)

            @pl.when(due)
            def _(op=op, k=k, spots=spots):
                if op == "V":
                    pl.when(n == spots[0][0])(await_down)
                if op in turned:
                    ups = [i for i, v in spots if (op, v) in OVER_X]
                    turned[op](k, sum(jnp.where(n == i, 1, 0) for i in ups) if ups else 0)
                else:
                    body[op](k)

        return carry

    lax.fori_loop(0, len(steps), step, 0)
    final.wait_recv()
    out_e[...] = (acc[col] + fin_recv[...].astype(f32)).astype(bf16)

    final.wait_send()
    for h in range(2):
        drain(*mixer_part(h))
        drain(*pooled_part(h))
    pl.when(not_last)(up_rim.wait_send)
    pl.when(not_first)(down_rim.wait_send)
    for i in range(4):
        down_copy(i).wait_send()

    def drain_ep(k, carry):
        e = lax.rem(me_ep + k, ep)
        q = ep_from(k)
        ep_copy(disp_send.at[e], slots.at[me_ep, me_tp], dp_s.at[k], dp_r.at[k], k).wait_send()
        ep_copy(back_send.at[q], back_recv.at[me_ep], bk_s.at[k], bk_r.at[k], ep - k).wait_send()
        return carry

    lax.fori_loop(1, ep, drain_ep, 0)

    def drain_tp(k, carry):
        drain(*slot_part(k))
        hidden_copy(k, row).wait_send()
        return carry

    lax.fori_loop(0, ep, drain_tp, 0)


def square_scratch(ep, tp, rows, feat, cap, chan, units, cols, shapes):
    dma = pltpu.SemaphoreType.DMA
    width = feat * tp
    w_in, w_mix, gate, up = shapes
    return [
        pltpu.VMEM(w_in, bf16),
        pltpu.VMEM(w_mix, bf16),
        pltpu.VMEM(gate, bf16),
        pltpu.VMEM(up, bf16),
        pltpu.VMEM((2, 2, units, cols), bf16),
        pltpu.VMEM((tp, rows, feat), bf16),
        pltpu.VMEM((min(rows, 128), width), bf16),
        pltpu.VMEM((cap, width), bf16),
        pltpu.VMEM((ep, cap, feat), bf16),
        pltpu.VMEM((ep, tp, cap, feat), bf16),
        pltpu.VMEM((ep, 2, cap, units), bf16),
        pltpu.VMEM((tp, rows, chan), bf16),
        pltpu.VMEM((ep, 2, cap, cols), bf16),
        pltpu.VMEM((ep, 2, cap, cols), bf16),
        pltpu.VMEM((rows + 2 * RIM, chan), f32),
        pltpu.VMEM((2, RIM, chan), bf16),
        pltpu.VMEM((2, RIM, chan), bf16),
        pltpu.VMEM((2, rows, cols), f32),
        pltpu.VMEM((rows, cols), bf16),
        pltpu.VMEM((rows, cols), bf16),
        pltpu.VMEM((8, rows), f32),
        pltpu.VMEM((rows, 8), f32),
        dma((7,)),
        dma((ep, 3)),
        dma((ep, 3)),
        dma((2, 3)),
        dma((2, 3)),
        dma((ep,)),
        dma((ep,)),
        dma((2,)),
        dma((2,)),
        dma((2, 3)),
        dma((2, 3)),
        dma((ep,)),
        dma((ep,)),
        dma((ep,)),
        dma((ep,)),
        dma((4,)),
        dma((4,)),
        dma((1,)),
        dma((1,)),
    ]


def hand_over(m_in, e_in, m_out, e_out):
    m_out[...] = m_in[...]
    e_out[...] = e_in[...]


def on_device(
    mixer_rows,
    expert_rows,
    mixer_gain,
    pool_scale,
    w_in,
    w_mix_out,
    expert_gain,
    expert_gate,
    expert_up,
    expert_down,
    routes,
    route_weight,
    *,
    ep,
    tp,
):
    rows, feat = mixer_rows.shape
    width = feat * tp
    cap = (3 * TOP * rows + 2 * ep - 1) // (2 * ep)
    chan = w_in.shape[1]
    units = expert_gate.shape[2]
    vmem = pl.BlockSpec(memory_space=pltpu.VMEM)
    hbm = pl.BlockSpec(memory_space=pl.ANY)
    dma = pltpu.SemaphoreType.DMA
    square_ok = tp == 4 and ep == len(SENDS) + 1
    whole_scratch = [
        pltpu.VMEM(w_in.shape, bf16),
        pltpu.VMEM(w_mix_out.shape, bf16),
        pltpu.VMEM(expert_gate.shape[1:], bf16),
        pltpu.VMEM(expert_up.shape[1:], bf16),
        pltpu.VMEM(expert_down.shape[1:], bf16),
        pltpu.VMEM((tp, rows, feat), bf16),
        pltpu.VMEM((min(rows, 128), width), bf16),
        pltpu.VMEM((cap, width), bf16),
        pltpu.VMEM((ep, cap, feat), bf16),
        pltpu.VMEM((ep, tp, cap, feat), bf16),
        pltpu.VMEM((ep, tp, cap, units), bf16),
        pltpu.VMEM((tp, rows, chan), bf16),
        pltpu.VMEM((ep, cap, expert_down.shape[2]), bf16),
        pltpu.VMEM((ep, cap, expert_down.shape[2]), bf16),
        pltpu.VMEM((rows + 2 * RIM, chan), f32),
        pltpu.VMEM((2, RIM, chan), bf16),
        pltpu.VMEM((2, RIM, chan), bf16),
        pltpu.VMEM((rows, expert_down.shape[2]), f32),
        pltpu.VMEM((8, rows), f32),
        pltpu.VMEM((rows, 8), f32),
        dma((6,)),
        dma((ep, tp - 1)),
        dma((ep, tp - 1)),
        dma((tp - 1,)),
        dma((tp - 1,)),
        dma((ep,)),
        dma((ep,)),
        dma((2,)),
        dma((2,)),
        dma((tp - 1,)),
        dma((tp - 1,)),
        dma((ep, tp - 1)),
        dma((ep, tp - 1)),
        dma((ep,)),
        dma((ep,)),
    ]
    if square_ok:
        shapes = (w_in.shape, w_mix_out.shape, expert_gate.shape[1:], expert_up.shape[1:])
        cols = expert_down.shape[2]
        whole_scratch = square_scratch(ep, tp, rows, feat, cap, chan, units, cols, shapes)
    result = pl.pallas_call(
        functools.partial(square if square_ok else fused, ep, tp),
        out_shape=(
            jax.ShapeDtypeStruct((rows, w_mix_out.shape[1]), bf16),
            jax.ShapeDtypeStruct((rows, expert_down.shape[2]), bf16),
        ),
        in_specs=[hbm if square_ok else vmem] + [vmem] * 6 + [hbm] * 5,
        out_specs=(vmem, vmem),
        scratch_shapes=whole_scratch,
        compiler_params=pltpu.CompilerParams(
            collective_id=0, has_side_effects=True, vmem_limit_bytes=62 * 1024 * 1024
        ),
    )(
        mixer_rows,
        expert_rows,
        mixer_gain.reshape(1, width),
        expert_gain.reshape(1, width),
        pool_scale.reshape(1, chan),
        routes.T,
        route_weight.T,
        w_in,
        w_mix_out,
        expert_gate.reshape(expert_gate.shape[1:]),
        expert_up.reshape(expert_up.shape[1:]),
        expert_down.reshape(expert_down.shape[1:]),
    )
    if not square_ok:
        return result
    return pl.pallas_call(
        hand_over,
        out_shape=tuple(jax.ShapeDtypeStruct(v.shape, v.dtype) for v in result),
        in_specs=[vmem, vmem],
        out_specs=(vmem, vmem),
    )(*result)


def solution(mesh):
    return jax.shard_map(
        functools.partial(on_device, ep=mesh.shape["ep"], tp=mesh.shape["tp"]),
        mesh=mesh,
        in_specs=(
            P("ep", "tp"),
            P("ep", "tp"),
            P(),
            P("tp"),
            P(None, "tp"),
            P(None, "tp"),
            P(),
            P("ep", None, "tp"),
            P("ep", None, "tp"),
            P("ep", None, "tp"),
            P("ep", None),
            P("ep", None),
        ),
        out_specs=(P("ep", "tp"), P("ep", "tp")),
        check_vma=False,
    )
```

```python
import functools

import jax
import jax.numpy as jnp
from jax import lax
from jax.experimental import pallas as pl
from jax.experimental.pallas import tpu as pltpu
from jax.sharding import PartitionSpec as P

TOP = 2
norm_eps = 1e-05
pool_windows = (2, 4, 8, 16)
RIM = 16
ORDER = (
    ("XMY", 1), ("W", 2), ("P", -1), ("W", 3), ("A", 0), ("XMY", 0),
    ("A", 2), ("A", 4), ("R", 2), ("R", 4), ("W", 1), ("A", 3),
    ("H", 2), ("W", 0), ("H", 4), ("A", 6), ("R", 3), ("A", 7),
    ("V", 2), ("R", 0), ("A", 5), ("G", 2), ("V", 4), ("H", 3),
    ("R", 6), ("XMX", 0), ("R", 5), ("V", 3), ("H", 0), ("XMX", 1),
    ("R", 7), ("H", 5), ("RXM", 1), ("RXM", 0), ("V", 5), ("G", 4),
    ("V", 0), ("A", 1), ("H", 7), ("G", 0), ("ENT", -1), ("H", 6),
    ("R", 1), ("V", 7), ("H", 1), ("V", 6), ("POOL", -1), ("G", 3),
    ("V", 1), ("G", 7), ("G", 1), ("G", 5), ("RPO", 0), ("G", 6),
    ("EX", -1), ("RPO", 1), ("MIX", 0), ("MIX", 1),
)
SENDS = (
    2, 4, 1, 3, 7, 6, 5,
)
OVER_X = (
    ("R", 0, 0), ("R", 1, 0), ("R", 1, 1), ("R", 2, 0), ("R", 3, 1), ("R", 5, 0),
    ("R", 5, 1), ("R", 7, 0), ("R", 7, 1), ("RXM", 1, 0),
)
PLACES = (
    "W", "POOL", "A", "H", "G", "XMX", "R", "RXM",
    "V", "EX", "RPO", "ENT", "XMY", "MIX",
)
MESH = pl.DeviceIdType.MESH
f32 = jnp.float32
bf16 = jnp.bfloat16


def fused(
    ep,
    tp,
    xm_in,
    xe_in,
    gain_m,
    gain_e,
    scale,
    route_rows,
    rw_rows,
    w_in_h,
    w_mix_h,
    gate_h,
    up_h,
    down_h,
    out_m,
    out_e,
    w_in,
    w_mix,
    gate,
    up,
    down,
    xm,
    normed,
    block,
    disp_send,
    slots,
    hid,
    pooled,
    back_send,
    back_recv,
    ext,
    rim_send,
    rim_recv,
    acc,
    as_rows,
    as_cols,
    w_sem,
    sl_s,
    sl_r,
    xm_s,
    xm_r,
    dp_s,
    dp_r,
    rim_s,
    rim_r,
    po_s,
    po_r,
    hi_s,
    hi_r,
    bk_s,
    bk_r,
):
    me_ep = lax.axis_index("ep")
    me_tp = lax.axis_index("tp")
    rows, feat = xm_in.shape
    cap = slots.shape[2]
    chan = out_m.shape[1]
    width = feat * tp
    chunk = min(rows, 128)

    barrier = pltpu.get_barrier_semaphore()
    for d in range(1, tp):
        pl.semaphore_signal(
            barrier, inc=1, device_id={"tp": lax.rem(me_tp + d, tp)}, device_id_type=MESH
        )
    for d in range(1, ep):
        pl.semaphore_signal(
            barrier, inc=1, device_id={"ep": lax.rem(me_ep + d, ep)}, device_id_type=MESH
        )
    pl.semaphore_wait(barrier, tp + ep - 2)

    def tp_copy(ref, s, r, peer):
        return pltpu.make_async_remote_copy(
            src_ref=ref,
            dst_ref=ref,
            send_sem=s,
            recv_sem=r,
            device_id={"tp": peer},
            device_id_type=MESH,
        )

    def ep_copy(src, dst, s, r, d):
        return pltpu.make_async_remote_copy(
            src_ref=src,
            dst_ref=dst,
            send_sem=s,
            recv_sem=r,
            device_id={"ep": lax.rem(me_ep + d, ep)},
            device_id_type=MESH,
        )

    relayed = tp == 4
    col = lax.rem(me_tp, 2)
    row = me_tp // 2
    beside = row * 2 + (1 - col)
    above = (1 - row) * 2 + col
    across = (1 - row) * 2 + (1 - col)

    def send(slot, s, r):
        if relayed:
            tp_copy(slot(me_tp), s(0), r(0), beside).start()
            tp_copy(slot(me_tp), s(1), r(1), above).start()
        else:
            for d in range(1, tp):
                tp_copy(slot(me_tp), s(d - 1), r(d - 1), lax.rem(me_tp + d, tp)).start()

    def relay(slot, s, r, turn):
        if relayed:
            tp_copy(slot(beside), s(0), r(0), beside).wait_recv()
            tp_copy(slot(above), s(1), r(1), above).wait_recv()
            source = (1 - turn) * beside + turn * above
            peer = (1 - turn) * above + turn * beside
            tp_copy(slot(source), s(2), r(2), peer).start()

    def finish(slot, s, r):
        if relayed:
            tp_copy(slot(across), s(2), r(2), across).wait_recv()
        else:
            for d in range(1, tp):
                p = lax.rem(me_tp - d + tp, tp)
                tp_copy(slot(p), s(d - 1), r(d - 1), p).wait_recv()

    def drain(slot, s, r):
        for d in range(1, tp):
            tp_copy(slot(me_tp), s(d - 1), r(d - 1), lax.rem(me_tp + d, tp)).wait_send()

    def mixer_part():
        return lambda p: xm.at[p], lambda j: xm_s.at[j], lambda j: xm_r.at[j]

    def pooled_part():
        return lambda p: pooled.at[p], lambda j: po_s.at[j], lambda j: po_r.at[j]

    def slot_part(k):
        q = ep_from(k)
        return lambda p: slots.at[q, p], lambda j: sl_s.at[k, j], lambda j: sl_r.at[k, j]

    def hidden_part(k):
        q = ep_from(k)
        return lambda p: hid.at[q, p], lambda j: hi_s.at[k, j], lambda j: hi_r.at[k, j]

    def ep_from(d):
        return lax.rem(me_ep - d + ep, ep)

    xm_load = pltpu.make_async_copy(xm_in, xm.at[me_tp], w_sem.at[5])
    xm_load.start()
    xm_load.wait()
    send(*mixer_part())

    loads = [
        pltpu.make_async_copy(h, v, w_sem.at[i])
        for i, (h, v) in enumerate(
            ((w_in_h, w_in), (gate_h, gate), (up_h, up), (w_mix_h, w_mix), (down_h, down))
        )
    ]
    for load in loads:
        load.start()

    t0 = lax.broadcasted_iota(jnp.int32, (rows, rows), 0)
    t1 = lax.broadcasted_iota(jnp.int32, (rows, rows), 1)
    names = lax.broadcasted_iota(jnp.int32, (ep, rows), 0)
    named = [jnp.where(route_rows[j : j + 1, :] == names, 1.0, 0.0) for j in range(TOP)]
    ahead = jnp.dot(
        sum(named).astype(bf16),
        jnp.where(t0 < t1, 1.0, 0.0).astype(bf16),
        preferred_element_type=f32,
    )
    trow = [
        route_rows[j : j + 1, :] * cap
        + jnp.sum(named[j] * ahead, axis=0, keepdims=True).astype(jnp.int32)
        for j in range(TOP)
    ]
    as_rows[...] = jnp.zeros_like(as_rows)
    for j in range(TOP):
        as_rows[j : j + 1, :] = trow[j].astype(f32)
        as_rows[TOP + j : TOP + j + 1, :] = rw_rows[j : j + 1, :]
    as_cols[...] = as_rows[...].T

    def picked_rows(e):
        slot = lax.broadcasted_iota(jnp.int32, (cap, rows), 0) + e * cap
        hit = (slot == trow[0]) | (slot == trow[1])
        pick = jnp.where(hit, 1.0, 0.0).astype(bf16)
        return jnp.dot(pick, xe_in[...], preferred_element_type=f32).astype(bf16)

    def send_rows(d, carry):
        e = lax.rem(me_ep + d, ep)
        disp_send[e] = picked_rows(e)
        ep_copy(disp_send.at[e], slots.at[me_ep, me_tp], dp_s.at[d], dp_r.at[d], d).start()
        return carry

    lax.fori_loop(1, ep, send_rows, 0)
    slots[me_ep, me_tp] = picked_rows(me_ep)
    relay(*mixer_part(), 0)

    def arrive(k):
        q = ep_from(k)
        ep_copy(disp_send.at[q], slots.at[q, me_tp], dp_s.at[k], dp_r.at[k], k).wait_recv()
        send(*slot_part(k))

    arrive(1)

    def pass_slots(k, carry):
        arrive(k)
        relay(*slot_part(k - 1), lax.rem(k, 2))
        return carry

    early = ep // 2
    lax.fori_loop(2, early, pass_slots, 0)

    def norm_rows(parts, gain):
        parts = [v.astype(f32) for v in parts]
        mean = sum(jnp.sum(v, axis=-1, keepdims=True) for v in parts) / width
        parts = [v - mean for v in parts]
        spread = sum(jnp.sum(v * v, axis=-1, keepdims=True) for v in parts) / width
        inv = lax.rsqrt(spread + norm_eps)
        return [
            (v * inv * gain[:, p * feat : (p + 1) * feat]).astype(bf16)
            for p, v in enumerate(parts)
        ]

    finish(*mixer_part())
    loads[0].wait()

    def project(i, carry):
        at = pl.ds(pl.multiple_of(i * chunk, chunk), chunk)
        for p, v in enumerate(norm_rows([xm[p, at, :] for p in range(tp)], gain_m)):
            normed[:, p * feat : (p + 1) * feat] = v
        inner = jnp.dot(normed[...], w_in[...], preferred_element_type=f32).astype(bf16)
        ext[pl.ds(pl.multiple_of(RIM + i * chunk, RIM), chunk), :] = inner.astype(f32)
        return carry

    lax.fori_loop(0, rows // chunk, project, 0)
    rim_send[0] = ext[rows : rows + RIM, :].astype(bf16)
    rim_send[1] = ext[RIM : 2 * RIM, :].astype(bf16)
    up_rim = ep_copy(rim_send.at[0], rim_recv.at[0], rim_s.at[0], rim_r.at[0], 1)
    down_rim = ep_copy(rim_send.at[1], rim_recv.at[1], rim_s.at[1], rim_r.at[1], ep - 1)
    up_rim.start()
    down_rim.start()

    lax.fori_loop(early, ep - 1, pass_slots, 0)

    up_rim.wait_recv()
    down_rim.wait_recv()
    low = rim_recv[0].astype(f32)
    high = rim_recv[1].astype(f32)
    ext[0:RIM, :] = jnp.where(me_ep > 0, low, 0.0)
    ext[RIM + rows : 2 * RIM + rows, :] = jnp.where(me_ep < ep - 1, high, 0.0)

    group_width = chan * tp // len(pool_windows)
    channel = me_tp * chan + lax.broadcasted_iota(jnp.int32, (1, chan), 1)
    seq_len = rows * ep
    for i in range(rows // chunk):
        first = RIM + i * chunk
        position = me_ep * rows + i * chunk + lax.broadcasted_iota(jnp.int32, (chunk, 1), 0)
        running = jnp.zeros((chunk, chan), f32)
        result = jnp.zeros((chunk, chan), f32)
        last = 0
        for g, window in enumerate(pool_windows):
            half = window // 2
            for o in list(range(-half, -last)) + list(range(last, half)):
                running = running + ext[first + o : first + o + chunk, :]
            last = half
            lower = jnp.maximum(position - half, 0)
            upper = jnp.minimum(position + half, seq_len)
            counts = (upper - lower).astype(f32)
            member = (channel >= g * group_width) & (channel < (g + 1) * group_width)
            result = jnp.where(member, running / counts, result)
        values = ext[first : first + chunk, :]
        pooled[me_tp, i * chunk : (i + 1) * chunk, :] = (
            (result - values) * scale[...]
        ).astype(bf16)
    send(*pooled_part())
    pass_slots(ep - 1, 0)
    send(*slot_part(0))

    loads[1].wait()
    loads[2].wait()

    def hidden_step(k):
        q = ep_from(k)
        finish(*slot_part(k))
        for p, v in enumerate(norm_rows([slots[q, p] for p in range(tp)], gain_e)):
            block[:, p * feat : (p + 1) * feat] = v
        x = block[...]
        g = jnp.dot(x, gate[...], preferred_element_type=f32)
        u = jnp.dot(x, up[...], preferred_element_type=f32)
        hid[q, me_tp] = (g / (1.0 + jnp.exp(-g)) * u).astype(bf16)
        send(*hidden_part(k))

    units = hid.shape[3]

    def value_step(k):
        q = ep_from(k)
        finish(*hidden_part(k))
        total = jnp.zeros((cap, out_e.shape[1]), f32)
        for p in range(tp):
            total = total + jnp.dot(
                hid[q, p],
                down[p * units : (p + 1) * units, :],
                preferred_element_type=f32,
            )
        return total.astype(bf16)

    def send_value(k):
        q = ep_from(k)
        back_send[q] = value_step(k)
        ep_copy(back_send.at[q], back_recv.at[me_ep], bk_s.at[k], bk_r.at[k], ep - k).start()

    hidden_step(1)
    relay(*slot_part(ep - 1), ep % 2)
    hidden_step(2)
    relay(*slot_part(0), 1 - ep % 2)
    relay(*pooled_part(), 1)
    relay(*hidden_part(1), 0)

    loads[3].wait()
    finish(*pooled_part())

    def mix_out(i, carry):
        at = pl.ds(pl.multiple_of(i * chunk, chunk), chunk)
        total = jnp.zeros((chunk, chan), f32)
        for p in range(tp):
            total = total + jnp.dot(
                pooled[p, at, :],
                w_mix[p * chan : (p + 1) * chan, :],
                preferred_element_type=f32,
            )
        out_m[at, :] = total.astype(bf16)
        return carry

    lax.fori_loop(0, rows // chunk, mix_out, 0)
    loads[4].wait()

    def expert(k, carry):
        hidden_step(k)
        relay(*hidden_part(k - 1), lax.rem(k, 2))
        send_value(k - 2)
        return carry

    lax.fori_loop(3, ep, expert, 0)
    hidden_step(0)
    relay(*hidden_part(ep - 1), ep % 2)
    send_value(ep - 2)
    relay(*hidden_part(0), 1 - ep % 2)
    send_value(ep - 1)

    def combine(e):
        slot = lax.broadcasted_iota(jnp.int32, (rows, cap), 1) + e * cap
        weight = jnp.zeros((rows, cap), f32)
        for j in range(TOP):
            own_slot = as_cols[:, j : j + 1].astype(jnp.int32)
            weight = weight + jnp.where(slot == own_slot, as_cols[:, TOP + j : TOP + j + 1], 0.0)
        coarse = weight.astype(bf16)
        fine = (weight - coarse.astype(f32)).astype(bf16)
        v = back_recv[e]
        return jnp.dot(coarse, v, preferred_element_type=f32) + jnp.dot(
            fine, v, preferred_element_type=f32
        )

    acc[...] = jnp.zeros_like(acc)

    def gather_value(k, carry):
        e = lax.rem(me_ep + k, ep)
        ep_copy(back_send.at[e], back_recv.at[e], bk_s.at[k], bk_r.at[k], k).wait_recv()
        acc[...] += combine(e)
        return carry

    lax.fori_loop(1, ep - 2, gather_value, 0)
    back_recv[me_ep] = value_step(0)
    acc[...] += combine(me_ep)
    lax.fori_loop(ep - 2, ep, gather_value, 0)
    out_e[...] = acc[...].astype(bf16)

    drain(*mixer_part())
    drain(*pooled_part())
    up_rim.wait_send()
    down_rim.wait_send()

    def drain_ep(k, carry):
        e = lax.rem(me_ep + k, ep)
        q = ep_from(k)
        ep_copy(disp_send.at[e], slots.at[me_ep, me_tp], dp_s.at[k], dp_r.at[k], k).wait_send()
        ep_copy(back_send.at[q], back_recv.at[me_ep], bk_s.at[k], bk_r.at[k], ep - k).wait_send()
        return carry

    lax.fori_loop(1, ep, drain_ep, 0)

    def drain_tp(k, carry):
        drain(*slot_part(k))
        drain(*hidden_part(k))
        return carry

    lax.fori_loop(0, ep, drain_tp, 0)


def square(
    ep,
    tp,
    xm_in,
    xe_h,
    gain_m_h,
    gain_e_h,
    scale_h,
    routes_h,
    rw_h,
    w_in_h,
    w_mix_h,
    gate_h,
    up_h,
    down_h,
    out_m_h,
    out_e_h,
    xe_in,
    gain_m,
    gain_e,
    scale,
    route_rows,
    rw_rows,
    out_m,
    out_e,
    w_in,
    w_mix,
    gate,
    up,
    down,
    xm,
    normed,
    block,
    disp_send,
    slots,
    hid,
    pooled,
    back_send,
    back_recv,
    ext,
    rim_send,
    rim_recv,
    acc,
    fin_send,
    fin_recv,
    as_rows,
    as_cols,
    in_sem,
    out_sem,
    w_sem,
    sl_s,
    sl_r,
    xm_s,
    xm_r,
    dp_s,
    dp_r,
    rim_s,
    rim_r,
    po_s,
    po_r,
    hi_s,
    hi_r,
    bk_s,
    bk_r,
    dn_s,
    dn_r,
    fi_s,
    fi_r,
):
    me_ep = lax.axis_index("ep")
    me_tp = lax.axis_index("tp")
    rows, feat = xe_in.shape
    cap = slots.shape[2]
    chan = out_m.shape[1]
    units = hid.shape[3]
    cols = out_e.shape[1]
    width = feat * tp
    chunk = min(rows, 128)

    not_first = me_ep > 0
    not_last = me_ep < ep - 1
    col = lax.rem(me_tp, 2)
    row = me_tp // 2
    beside = row * 2 + (1 - col)
    above = (1 - row) * 2 + col
    across = (1 - row) * 2 + (1 - col)

    barrier = pltpu.get_barrier_semaphore()
    for d in range(1, tp):
        pl.semaphore_signal(
            barrier, inc=1, device_id={"tp": lax.rem(me_tp + d, tp)}, device_id_type=MESH
        )
    for d in range(1, ep):
        pl.semaphore_signal(
            barrier, inc=1, device_id={"ep": lax.rem(me_ep + d, ep)}, device_id_type=MESH
        )

    inputs = [
        pltpu.make_async_copy(h, v, in_sem.at[i])
        for i, (h, v) in enumerate(
            (
                (routes_h, route_rows),
                (rw_h, rw_rows),
                (xe_h, xe_in),
                (gain_m_h, gain_m),
                (gain_e_h, gain_e),
                (scale_h, scale),
            )
        )
    ]
    for load in inputs:
        load.start()
    xm_load = pltpu.make_async_copy(xm_in, xm.at[me_tp], w_sem.at[0])
    xm_load.start()

    def unit_rows(r, c):
        return pl.ds(pl.multiple_of((r * 2 + c) * units, units), units)

    piece = units // 2

    loads = [
        pltpu.make_async_copy(h, v, w_sem.at[i + 1])
        for i, (h, v) in enumerate(
            (
                (w_in_h, w_in),
                (gate_h, gate),
                (up_h, up),
                (w_mix_h, w_mix),
                (down_h.at[unit_rows(0, col), :], down.at[col, 0]),
                (down_h.at[unit_rows(1, col), :], down.at[col, 1]),
            )
        )
    ]
    def tp_copy(src, dst, s, r, peer):
        return pltpu.make_async_remote_copy(
            src_ref=src,
            dst_ref=dst,
            send_sem=s,
            recv_sem=r,
            device_id={"tp": peer},
            device_id_type=MESH,
        )

    def ep_copy(src, dst, s, r, d):
        return pltpu.make_async_remote_copy(
            src_ref=src,
            dst_ref=dst,
            send_sem=s,
            recv_sem=r,
            device_id={"ep": lax.rem(me_ep + d, ep)},
            device_id_type=MESH,
        )

    def send(slot, s, r):
        mine = slot(me_tp)
        tp_copy(mine, mine, s(0), r(0), beside).start()
        tp_copy(mine, mine, s(1), r(1), above).start()

    def relay(slot, s, r, turn):
        tp_copy(slot(beside), slot(beside), s(0), r(0), beside).wait_recv()
        tp_copy(slot(above), slot(above), s(1), r(1), above).wait_recv()
        source = slot((1 - turn) * beside + turn * above)
        tp_copy(source, source, s(2), r(2), (1 - turn) * above + turn * beside).start()

    def finish(slot, s, r):
        tp_copy(slot(across), slot(across), s(2), r(2), across).wait_recv()

    def drain(slot, s, r):
        mine = slot(me_tp)
        for j in range(3):
            tp_copy(mine, mine, s(j), r(j), beside).wait_send()

    def half_rows(h):
        return pl.ds(pl.multiple_of(h * (rows // 2), rows // 2), rows // 2)

    part = cap // 2

    def slot_half(k, p, h):
        return slots.at[ep_from(k), p, pl.ds(h * part, part)]

    def relay_slot(k, turns):
        slot, s, r = slot_part(k)
        tp_copy(slot(beside), slot(beside), s(0), r(0), beside).wait_recv()
        tp_copy(slot(above), slot(above), s(1), r(1), above).wait_recv()
        for h, turn in enumerate(turns):
            source = slot_half(k, (1 - turn) * beside + turn * above, h)
            peer = (1 - turn) * above + turn * beside
            tp_copy(source, source, s(2 + h), r(2 + h), peer).start()

    def finish_slot(k):
        slot, s, r = slot_part(k)
        for h in range(2):
            source = slot_half(k, across, h)
            tp_copy(source, source, s(2 + h), r(2 + h), across).wait_recv()

    def drain_slot(k):
        slot, s, r = slot_part(k)
        for j in range(2):
            tp_copy(slot(me_tp), slot(me_tp), s(j), r(j), beside).wait_send()
        for h in range(2):
            source = slot_half(k, across, h)
            tp_copy(source, source, s(2 + h), r(2 + h), beside).wait_send()

    def mixer_part(h):
        at = half_rows(h)
        return lambda p: xm.at[p, at], lambda j: xm_s.at[h, j], lambda j: xm_r.at[h, j]

    def pooled_part(h):
        at = half_rows(h)
        return lambda p: pooled.at[p, at], lambda j: po_s.at[h, j], lambda j: po_r.at[h, j]

    def ep_from(d):
        return lax.rem(me_ep - d + ep, ep)

    def slot_part(k):
        q = ep_from(k)
        return lambda p: slots.at[q, p], lambda j: sl_s.at[k, j], lambda j: sl_r.at[k, j]

    def hidden_copy(k, part):
        ref = hid.at[ep_from(k), part]
        return tp_copy(ref, ref, hi_s.at[k], hi_r.at[k], above)

    def down_copy(i):
        r, half = i // 2, i % 2
        first = (r * 2 + 1 - col) * units + half * piece
        return tp_copy(
            down_h.at[pl.ds(pl.multiple_of(first, piece), piece), :],
            down.at[col, r, pl.ds(pl.multiple_of(half * piece, piece), piece)],
            dn_s.at[i],
            dn_r.at[i],
            beside,
        )

    def mixer_x(h):
        slot, s, r = mixer_part(h)
        tp_copy(slot(me_tp), slot(me_tp), s(0), r(0), beside).start()

    def mixer_y(h):
        slot, s, r = mixer_part(h)
        tp_copy(slot(me_tp), slot(me_tp), s(1), r(1), above).start()

    for load in inputs[:2]:
        load.wait()
    t0 = lax.broadcasted_iota(jnp.int32, (rows, rows), 0)
    t1 = lax.broadcasted_iota(jnp.int32, (rows, rows), 1)
    names = lax.broadcasted_iota(jnp.int32, (ep, rows), 0)
    named = [jnp.where(route_rows[j : j + 1, :] == names, 1.0, 0.0) for j in range(TOP)]
    ahead = jnp.dot(
        sum(named).astype(bf16),
        jnp.where(t0 < t1, 1.0, 0.0).astype(bf16),
        preferred_element_type=f32,
    )
    trow = [
        route_rows[j : j + 1, :] * cap
        + jnp.sum(named[j] * ahead, axis=0, keepdims=True).astype(jnp.int32)
        for j in range(TOP)
    ]
    as_rows[...] = jnp.zeros_like(as_rows)
    for j in range(TOP):
        as_rows[j : j + 1, :] = trow[j].astype(f32)
        as_rows[TOP + j : TOP + j + 1, :] = rw_rows[j : j + 1, :]
    as_cols[...] = as_rows[...].T

    for load in inputs[2:]:
        load.wait()
    xm_load.wait()
    for load in loads:
        load.start()
    pl.semaphore_wait(barrier, tp + ep - 2)
    starts = {
        "W": lambda k: down_copy(k).start(),
        "XMX": mixer_x,
        "XMY": mixer_y,
    }
    picks_at = ORDER.index(("P", -1))
    for op, k in ORDER[:picks_at]:
        starts[op](k)

    def picked_rows(e):
        slot = lax.broadcasted_iota(jnp.int32, (cap, rows), 0) + e * cap
        hit = (slot == trow[0]) | (slot == trow[1])
        pick = jnp.where(hit, 1.0, 0.0).astype(bf16)
        return jnp.dot(pick, xe_in[...], preferred_element_type=f32).astype(bf16)

    def send_rows(n, carry):
        d = sum(jnp.where(n == i, k, 0) for i, k in enumerate(SENDS))
        e = lax.rem(me_ep + d, ep)
        disp_send[e] = picked_rows(e)
        ep_copy(disp_send.at[e], slots.at[me_ep, me_tp], dp_s.at[d], dp_r.at[d], d).start()
        return carry

    lax.fori_loop(0, ep - 1, send_rows, 0)
    slots[me_ep, me_tp] = picked_rows(me_ep)

    def arrive(k):
        @pl.when(k > 0)
        def _():
            q = ep_from(k)
            ep_copy(disp_send.at[q], slots.at[q, me_tp], dp_s.at[k], dp_r.at[k], k).wait_recv()

        send(*slot_part(k))

    def norm_rows(parts, gain):
        parts = [v.astype(f32) for v in parts]
        mean = sum(jnp.sum(v, axis=-1, keepdims=True) for v in parts) / width
        parts = [v - mean for v in parts]
        spread = sum(jnp.sum(v * v, axis=-1, keepdims=True) for v in parts) / width
        inv = lax.rsqrt(spread + norm_eps)
        return [
            (v * inv * gain[:, p * feat : (p + 1) * feat]).astype(bf16)
            for p, v in enumerate(parts)
        ]

    def project(i, carry):
        at = pl.ds(pl.multiple_of(i * chunk, chunk), chunk)
        for p, v in enumerate(norm_rows([xm[p, at, :] for p in range(tp)], gain_m)):
            normed[:, p * feat : (p + 1) * feat] = v
        inner = jnp.dot(normed[...], w_in[...], preferred_element_type=f32).astype(bf16)
        ext[pl.ds(pl.multiple_of(RIM + i * chunk, RIM), chunk), :] = inner.astype(f32)
        return carry

    up_rim = ep_copy(rim_send.at[0], rim_recv.at[0], rim_s.at[0], rim_r.at[0], 1)
    down_rim = ep_copy(rim_send.at[1], rim_recv.at[1], rim_s.at[1], rim_r.at[1], ep - 1)

    def enter():
        for h in range(2):
            finish(*mixer_part(h))
        lax.fori_loop(0, rows // chunk, project, 0)
        rim_send[0] = ext[rows : rows + RIM, :].astype(bf16)
        rim_send[1] = ext[RIM : 2 * RIM, :].astype(bf16)
        pl.when(not_last)(up_rim.start)
        pl.when(not_first)(down_rim.start)

    for load in loads:
        load.wait()

    def hidden_step(k):
        q = ep_from(k)
        finish_slot(k)
        for p, v in enumerate(norm_rows([slots[q, p] for p in range(tp)], gain_e)):
            block[:, p * feat : (p + 1) * feat] = v
        x = block[...]
        g = jnp.dot(x, gate[...], preferred_element_type=f32)
        u = jnp.dot(x, up[...], preferred_element_type=f32)
        hid[q, row] = (g / (1.0 + jnp.exp(-g)) * u).astype(bf16)
        hidden_copy(k, row).start()

    def value_step(k):
        q = ep_from(k)
        hidden_copy(k, 1 - row).wait_recv()
        return [
            (
                jnp.dot(hid[q, 0], down[c, 0], preferred_element_type=f32)
                + jnp.dot(hid[q, 1], down[c, 1], preferred_element_type=f32)
            ).astype(bf16)
            for c in range(2)
        ]

    def send_value(k):
        q = ep_from(k)
        values = value_step(k)

        @pl.when(k > 0)
        def _():
            for c in range(2):
                back_send[q, c] = values[c]
            ep_copy(back_send.at[q], back_recv.at[me_ep], bk_s.at[k], bk_r.at[k], ep - k).start()

        @pl.when(k == 0)
        def _():
            for c in range(2):
                back_recv[me_ep, c] = values[c]

    def combine(e):
        slot = lax.broadcasted_iota(jnp.int32, (rows, cap), 1) + e * cap
        hit = None
        weight = jnp.zeros((rows, 1), f32)
        for j in range(TOP):
            own_slot = as_cols[:, j : j + 1].astype(jnp.int32)
            here = (own_slot >= e * cap) & (own_slot < (e + 1) * cap)
            weight = weight + jnp.where(here, as_cols[:, TOP + j : TOP + j + 1], 0.0)
            hit = slot == own_slot if hit is None else hit | (slot == own_slot)
        pick = jnp.where(hit, 1.0, 0.0).astype(bf16)
        for c in range(2):
            acc[c] += weight * jnp.dot(pick, back_recv[e, c], preferred_element_type=f32)

    def gather_value(k):
        e = lax.rem(me_ep + k, ep)

        @pl.when(k > 0)
        def _():
            ep_copy(back_send.at[e], back_recv.at[e], bk_s.at[k], bk_r.at[k], k).wait_recv()

        combine(e)

    def pool():
        ext[0:RIM, :] = jnp.zeros((RIM, chan), f32)
        ext[RIM + rows : 2 * RIM + rows, :] = jnp.zeros((RIM, chan), f32)

        @pl.when(not_first)
        def _():
            up_rim.wait_recv()
            ext[0:RIM, :] = rim_recv[0].astype(f32)

        @pl.when(not_last)
        def _():
            down_rim.wait_recv()
            ext[RIM + rows : 2 * RIM + rows, :] = rim_recv[1].astype(f32)

        group_width = chan * tp // len(pool_windows)
        channel = me_tp * chan + lax.broadcasted_iota(jnp.int32, (1, chan), 1)
        seq_len = rows * ep
        for i in range(rows // chunk):
            first = RIM + i * chunk
            position = me_ep * rows + i * chunk + lax.broadcasted_iota(jnp.int32, (chunk, 1), 0)
            running = jnp.zeros((chunk, chan), f32)
            result = jnp.zeros((chunk, chan), f32)
            last = 0
            for g, window in enumerate(pool_windows):
                half = window // 2
                for o in list(range(-half, -last)) + list(range(last, half)):
                    running = running + ext[first + o : first + o + chunk, :]
                last = half
                lower = jnp.maximum(position - half, 0)
                upper = jnp.minimum(position + half, seq_len)
                counts = (upper - lower).astype(f32)
                member = (channel >= g * group_width) & (channel < (g + 1) * group_width)
                result = jnp.where(member, running / counts, result)
            values = ext[first : first + chunk, :]
            pooled[me_tp, i * chunk : (i + 1) * chunk, :] = (
                (result - values) * scale[...]
            ).astype(bf16)
        for h in range(2):
            send(*pooled_part(h))

    acc[...] = jnp.zeros_like(acc)

    final = tp_copy(fin_send, fin_recv, fi_s.at[0], fi_r.at[0], beside)

    def exchange(k):
        fin_send[...] = acc[1 - col].astype(bf16)
        final.start()

    def mixed_out(h):
        at = half_rows(h)
        return pltpu.make_async_copy(out_m.at[at], out_m_h.at[at], out_sem.at[h])

    def mix_out(h):
        finish(*pooled_part(h))

        def mix(i, carry):
            at = pl.ds(pl.multiple_of(h * (rows // 2) + i * chunk, chunk), chunk)
            total = jnp.zeros((chunk, chan), f32)
            for p in range(tp):
                total = total + jnp.dot(
                    pooled[p, at, :],
                    w_mix[p * chan : (p + 1) * chan, :],
                    preferred_element_type=f32,
                )
            out_m[at, :] = total.astype(bf16)
            return carry

        lax.fori_loop(0, rows // 2 // chunk, mix, 0)
        mixed_out(h).start()

    def await_down():
        for i in range(4):
            down_copy(i).wait_recv()

    body = dict(
        starts,
        A=arrive,
        H=hidden_step,
        V=send_value,
        G=gather_value,
        ENT=lambda k: enter(),
        POOL=lambda k: pool(),
        EX=exchange,
        MIX=mix_out,
    )
    turned = {
        "R": lambda k, turns: relay_slot(k, turns),
        "RXM": lambda k, turns: relay(*mixer_part(k), turns[0]),
        "RPO": lambda k, turns: relay(*pooled_part(k), turns[0]),
    }

    steps = [[]]
    for op, k in ORDER[picks_at + 1 :]:
        if steps[-1] and PLACES.index(op) <= PLACES.index(steps[-1][-1][0]):
            steps.append([])
        steps[-1].append((op, k))
    where = {op: [] for op in PLACES}
    for n, entries in enumerate(steps):
        for op, k in entries:
            where[op].append((n, k))

    def step(n, carry):
        for op in PLACES:
            spots = where[op]
            if not spots:
                continue
            due = functools.reduce(jnp.logical_or, [n == i for i, _ in spots])
            k = sum(jnp.where(n == i, v, 0) for i, v in spots)

            @pl.when(due)
            def _(op=op, k=k, spots=spots):
                if op == "V":
                    pl.when(n == spots[0][0])(await_down)
                if op in turned:
                    turns = []
                    for h in range(2):
                        ups = [i for i, v in spots if (op, v, h) in OVER_X]
                        turns.append(sum(jnp.where(n == i, 1, 0) for i in ups) if ups else 0)
                    turned[op](k, turns)
                else:
                    body[op](k)

        return carry

    lax.fori_loop(0, len(steps), step, 0)
    final.wait_recv()
    out_e[...] = (acc[col] + fin_recv[...].astype(f32)).astype(bf16)
    last = pltpu.make_async_copy(out_e, out_e_h, out_sem.at[2])
    last.start()

    final.wait_send()
    for h in range(2):
        drain(*mixer_part(h))
        drain(*pooled_part(h))
    pl.when(not_last)(up_rim.wait_send)
    pl.when(not_first)(down_rim.wait_send)
    for i in range(4):
        down_copy(i).wait_send()

    def drain_ep(k, carry):
        e = lax.rem(me_ep + k, ep)
        q = ep_from(k)
        ep_copy(disp_send.at[e], slots.at[me_ep, me_tp], dp_s.at[k], dp_r.at[k], k).wait_send()
        ep_copy(back_send.at[q], back_recv.at[me_ep], bk_s.at[k], bk_r.at[k], ep - k).wait_send()
        return carry

    lax.fori_loop(1, ep, drain_ep, 0)

    def drain_tp(k, carry):
        drain_slot(k)
        hidden_copy(k, row).wait_send()
        return carry

    lax.fori_loop(0, ep, drain_tp, 0)
    for h in range(2):
        mixed_out(h).wait()
    last.wait()


def square_scratch(ep, tp, rows, feat, cap, chan, units, cols, shapes):
    dma = pltpu.SemaphoreType.DMA
    width = feat * tp
    w_in, w_mix, gate, up = shapes
    return [
        pltpu.VMEM((rows, feat), bf16),
        pltpu.VMEM((1, width), f32),
        pltpu.VMEM((1, width), f32),
        pltpu.VMEM((1, chan), f32),
        pltpu.VMEM((TOP, rows), jnp.int32),
        pltpu.VMEM((TOP, rows), f32),
        pltpu.VMEM((rows, chan), bf16),
        pltpu.VMEM((rows, cols), bf16),
        pltpu.VMEM(w_in, bf16),
        pltpu.VMEM(w_mix, bf16),
        pltpu.VMEM(gate, bf16),
        pltpu.VMEM(up, bf16),
        pltpu.VMEM((2, 2, units, cols), bf16),
        pltpu.VMEM((tp, rows, feat), bf16),
        pltpu.VMEM((min(rows, 128), width), bf16),
        pltpu.VMEM((cap, width), bf16),
        pltpu.VMEM((ep, cap, feat), bf16),
        pltpu.VMEM((ep, tp, cap, feat), bf16),
        pltpu.VMEM((ep, 2, cap, units), bf16),
        pltpu.VMEM((tp, rows, chan), bf16),
        pltpu.VMEM((ep, 2, cap, cols), bf16),
        pltpu.VMEM((ep, 2, cap, cols), bf16),
        pltpu.VMEM((rows + 2 * RIM, chan), f32),
        pltpu.VMEM((2, RIM, chan), bf16),
        pltpu.VMEM((2, RIM, chan), bf16),
        pltpu.VMEM((2, rows, cols), f32),
        pltpu.VMEM((rows, cols), bf16),
        pltpu.VMEM((rows, cols), bf16),
        pltpu.VMEM((8, rows), f32),
        pltpu.VMEM((rows, 8), f32),
        dma((6,)),
        dma((3,)),
        dma((7,)),
        dma((ep, 4)),
        dma((ep, 4)),
        dma((2, 3)),
        dma((2, 3)),
        dma((ep,)),
        dma((ep,)),
        dma((2,)),
        dma((2,)),
        dma((2, 3)),
        dma((2, 3)),
        dma((ep,)),
        dma((ep,)),
        dma((ep,)),
        dma((ep,)),
        dma((4,)),
        dma((4,)),
        dma((1,)),
        dma((1,)),
    ]


def hand_over(m_in, e_in, m_out, e_out, held, sem):
    pieces = held.shape[1]
    rows = held.shape[2]
    ways = []
    for i, (src, dst) in enumerate(((m_in, m_out), (e_in, e_out))):
        for j in range(pieces):
            at = pl.ds(j * rows, rows)
            into = pltpu.make_async_copy(src.at[at], held.at[i, j], sem.at[0, i, j])
            into.start()
            out = pltpu.make_async_copy(held.at[i, j], dst.at[at], sem.at[1, i, j])
            ways.append((into, out))
    for into, out in ways:
        into.wait()
        out.start()
    for _, out in ways:
        out.wait()


def on_device(
    mixer_rows,
    expert_rows,
    mixer_gain,
    pool_scale,
    w_in,
    w_mix_out,
    expert_gain,
    expert_gate,
    expert_up,
    expert_down,
    routes,
    route_weight,
    *,
    ep,
    tp,
):
    rows, feat = mixer_rows.shape
    width = feat * tp
    cap = (3 * TOP * rows + 2 * ep - 1) // (2 * ep)
    chan = w_in.shape[1]
    units = expert_gate.shape[2]
    vmem = pl.BlockSpec(memory_space=pltpu.VMEM)
    hbm = pl.BlockSpec(memory_space=pl.ANY)
    dma = pltpu.SemaphoreType.DMA
    square_ok = tp == 4 and ep == len(SENDS) + 1
    whole_scratch = [
        pltpu.VMEM(w_in.shape, bf16),
        pltpu.VMEM(w_mix_out.shape, bf16),
        pltpu.VMEM(expert_gate.shape[1:], bf16),
        pltpu.VMEM(expert_up.shape[1:], bf16),
        pltpu.VMEM(expert_down.shape[1:], bf16),
        pltpu.VMEM((tp, rows, feat), bf16),
        pltpu.VMEM((min(rows, 128), width), bf16),
        pltpu.VMEM((cap, width), bf16),
        pltpu.VMEM((ep, cap, feat), bf16),
        pltpu.VMEM((ep, tp, cap, feat), bf16),
        pltpu.VMEM((ep, tp, cap, units), bf16),
        pltpu.VMEM((tp, rows, chan), bf16),
        pltpu.VMEM((ep, cap, expert_down.shape[2]), bf16),
        pltpu.VMEM((ep, cap, expert_down.shape[2]), bf16),
        pltpu.VMEM((rows + 2 * RIM, chan), f32),
        pltpu.VMEM((2, RIM, chan), bf16),
        pltpu.VMEM((2, RIM, chan), bf16),
        pltpu.VMEM((rows, expert_down.shape[2]), f32),
        pltpu.VMEM((8, rows), f32),
        pltpu.VMEM((rows, 8), f32),
        dma((6,)),
        dma((ep, tp - 1)),
        dma((ep, tp - 1)),
        dma((tp - 1,)),
        dma((tp - 1,)),
        dma((ep,)),
        dma((ep,)),
        dma((2,)),
        dma((2,)),
        dma((tp - 1,)),
        dma((tp - 1,)),
        dma((ep, tp - 1)),
        dma((ep, tp - 1)),
        dma((ep,)),
        dma((ep,)),
    ]
    if square_ok:
        shapes = (w_in.shape, w_mix_out.shape, expert_gate.shape[1:], expert_up.shape[1:])
        cols = expert_down.shape[2]
        whole_scratch = square_scratch(ep, tp, rows, feat, cap, chan, units, cols, shapes)
    result = pl.pallas_call(
        functools.partial(square if square_ok else fused, ep, tp),
        out_shape=(
            jax.ShapeDtypeStruct((rows, w_mix_out.shape[1]), bf16),
            jax.ShapeDtypeStruct((rows, expert_down.shape[2]), bf16),
        ),
        in_specs=[hbm if square_ok else vmem] * 7 + [hbm] * 5,
        out_specs=(hbm, hbm) if square_ok else (vmem, vmem),
        scratch_shapes=whole_scratch,
        compiler_params=pltpu.CompilerParams(
            collective_id=0, has_side_effects=True, vmem_limit_bytes=62 * 1024 * 1024
        ),
    )(
        mixer_rows,
        expert_rows,
        mixer_gain.reshape(1, width),
        expert_gain.reshape(1, width),
        pool_scale.reshape(1, chan),
        routes.T,
        route_weight.T,
        w_in,
        w_mix_out,
        expert_gate.reshape(expert_gate.shape[1:]),
        expert_up.reshape(expert_up.shape[1:]),
        expert_down.reshape(expert_down.shape[1:]),
    )
    if not square_ok:
        return result
    pieces = 2
    return pl.pallas_call(
        hand_over,
        out_shape=tuple(jax.ShapeDtypeStruct(v.shape, v.dtype) for v in result),
        in_specs=[hbm, hbm],
        out_specs=(hbm, hbm),
        scratch_shapes=[
            pltpu.VMEM((2, pieces, rows // pieces, cols), bf16),
            pltpu.SemaphoreType.DMA((2, 2, pieces)),
        ],
    )(*result)


def solution(mesh):
    return jax.shard_map(
        functools.partial(on_device, ep=mesh.shape["ep"], tp=mesh.shape["tp"]),
        mesh=mesh,
        in_specs=(
            P("ep", "tp"),
            P("ep", "tp"),
            P(),
            P("tp"),
            P(None, "tp"),
            P(None, "tp"),
            P(),
            P("ep", None, "tp"),
            P("ep", None, "tp"),
            P("ep", None, "tp"),
            P("ep", None),
            P("ep", None),
        ),
        out_specs=(P("ep", "tp"), P("ep", "tp")),
        check_vma=False,
    )
```

```python
import functools

import jax
import jax.numpy as jnp
from jax import lax
from jax.experimental import pallas as pl
from jax.experimental.pallas import tpu as pltpu
from jax.sharding import PartitionSpec as P

TOP = 2
norm_eps = 1e-05
pool_windows = (2, 4, 8, 16)
RIM = 16
ORDER = (
    ("XMY", 1), ("W", 2), ("P", -1), ("W", 3), ("A", 0), ("XMY", 0),
    ("A", 2), ("A", 4), ("R", 2), ("R", 4), ("W", 1), ("A", 3),
    ("H", 2), ("W", 0), ("H", 4), ("A", 6), ("R", 3), ("A", 7),
    ("V", 2), ("R", 0), ("A", 5), ("G", 2), ("V", 4), ("H", 3),
    ("R", 6), ("XMX", 0), ("R", 5), ("V", 3), ("H", 0), ("XMX", 1),
    ("R", 7), ("H", 5), ("RXM", 1), ("RXM", 0), ("V", 5), ("G", 4),
    ("V", 0), ("A", 1), ("H", 7), ("G", 0), ("ENT", -1), ("R", 1),
    ("H", 6), ("V", 7), ("H", 1), ("V", 6), ("POOL", -1), ("G", 3),
    ("G", 5), ("V", 1), ("G", 7), ("G", 1), ("RPO", 0), ("G", 6),
    ("EX", -1), ("RPO", 1), ("MIX", 0), ("MIX", 1),
)
SENDS = (
    2, 4, 1, 3, 7, 6, 5,
)
OVER_X = (
    ("R", 0, 0), ("R", 1, 0), ("R", 1, 1), ("R", 2, 0), ("R", 3, 1), ("R", 5, 0),
    ("R", 5, 1), ("R", 7, 0), ("R", 7, 1), ("RXM", 1, 0),
)
PLACES = (
    "W", "A", "POOL", "H", "G", "EX", "XMY", "RPO",
    "ENT", "RXM", "XMX", "V", "R", "MIX",
)
MESH = pl.DeviceIdType.MESH
f32 = jnp.float32
bf16 = jnp.bfloat16


def fused(
    ep,
    tp,
    xm_in,
    xe_in,
    gain_m,
    gain_e,
    scale,
    route_rows,
    rw_rows,
    w_in_h,
    w_mix_h,
    gate_h,
    up_h,
    down_h,
    out_m,
    out_e,
    w_in,
    w_mix,
    gate,
    up,
    down,
    xm,
    normed,
    block,
    disp_send,
    slots,
    hid,
    pooled,
    back_send,
    back_recv,
    ext,
    rim_send,
    rim_recv,
    acc,
    as_rows,
    as_cols,
    w_sem,
    sl_s,
    sl_r,
    xm_s,
    xm_r,
    dp_s,
    dp_r,
    rim_s,
    rim_r,
    po_s,
    po_r,
    hi_s,
    hi_r,
    bk_s,
    bk_r,
):
    me_ep = lax.axis_index("ep")
    me_tp = lax.axis_index("tp")
    rows, feat = xm_in.shape
    cap = slots.shape[2]
    chan = out_m.shape[1]
    width = feat * tp
    chunk = min(rows, 128)

    barrier = pltpu.get_barrier_semaphore()
    for d in range(1, tp):
        pl.semaphore_signal(
            barrier, inc=1, device_id={"tp": lax.rem(me_tp + d, tp)}, device_id_type=MESH
        )
    for d in range(1, ep):
        pl.semaphore_signal(
            barrier, inc=1, device_id={"ep": lax.rem(me_ep + d, ep)}, device_id_type=MESH
        )
    pl.semaphore_wait(barrier, tp + ep - 2)

    def tp_copy(ref, s, r, peer):
        return pltpu.make_async_remote_copy(
            src_ref=ref,
            dst_ref=ref,
            send_sem=s,
            recv_sem=r,
            device_id={"tp": peer},
            device_id_type=MESH,
        )

    def ep_copy(src, dst, s, r, d):
        return pltpu.make_async_remote_copy(
            src_ref=src,
            dst_ref=dst,
            send_sem=s,
            recv_sem=r,
            device_id={"ep": lax.rem(me_ep + d, ep)},
            device_id_type=MESH,
        )

    relayed = tp == 4
    col = lax.rem(me_tp, 2)
    row = me_tp // 2
    beside = row * 2 + (1 - col)
    above = (1 - row) * 2 + col
    across = (1 - row) * 2 + (1 - col)

    def send(slot, s, r):
        if relayed:
            tp_copy(slot(me_tp), s(0), r(0), beside).start()
            tp_copy(slot(me_tp), s(1), r(1), above).start()
        else:
            for d in range(1, tp):
                tp_copy(slot(me_tp), s(d - 1), r(d - 1), lax.rem(me_tp + d, tp)).start()

    def relay(slot, s, r, turn):
        if relayed:
            tp_copy(slot(beside), s(0), r(0), beside).wait_recv()
            tp_copy(slot(above), s(1), r(1), above).wait_recv()
            source = (1 - turn) * beside + turn * above
            peer = (1 - turn) * above + turn * beside
            tp_copy(slot(source), s(2), r(2), peer).start()

    def finish(slot, s, r):
        if relayed:
            tp_copy(slot(across), s(2), r(2), across).wait_recv()
        else:
            for d in range(1, tp):
                p = lax.rem(me_tp - d + tp, tp)
                tp_copy(slot(p), s(d - 1), r(d - 1), p).wait_recv()

    def drain(slot, s, r):
        for d in range(1, tp):
            tp_copy(slot(me_tp), s(d - 1), r(d - 1), lax.rem(me_tp + d, tp)).wait_send()

    def mixer_part():
        return lambda p: xm.at[p], lambda j: xm_s.at[j], lambda j: xm_r.at[j]

    def pooled_part():
        return lambda p: pooled.at[p], lambda j: po_s.at[j], lambda j: po_r.at[j]

    def slot_part(k):
        q = ep_from(k)
        return lambda p: slots.at[q, p], lambda j: sl_s.at[k, j], lambda j: sl_r.at[k, j]

    def hidden_part(k):
        q = ep_from(k)
        return lambda p: hid.at[q, p], lambda j: hi_s.at[k, j], lambda j: hi_r.at[k, j]

    def ep_from(d):
        return lax.rem(me_ep - d + ep, ep)

    xm_load = pltpu.make_async_copy(xm_in, xm.at[me_tp], w_sem.at[5])
    xm_load.start()
    xm_load.wait()
    send(*mixer_part())

    loads = [
        pltpu.make_async_copy(h, v, w_sem.at[i])
        for i, (h, v) in enumerate(
            ((w_in_h, w_in), (gate_h, gate), (up_h, up), (w_mix_h, w_mix), (down_h, down))
        )
    ]
    for load in loads:
        load.start()

    t0 = lax.broadcasted_iota(jnp.int32, (rows, rows), 0)
    t1 = lax.broadcasted_iota(jnp.int32, (rows, rows), 1)
    names = lax.broadcasted_iota(jnp.int32, (ep, rows), 0)
    named = [jnp.where(route_rows[j : j + 1, :] == names, 1.0, 0.0) for j in range(TOP)]
    ahead = jnp.dot(
        sum(named).astype(bf16),
        jnp.where(t0 < t1, 1.0, 0.0).astype(bf16),
        preferred_element_type=f32,
    )
    trow = [
        route_rows[j : j + 1, :] * cap
        + jnp.sum(named[j] * ahead, axis=0, keepdims=True).astype(jnp.int32)
        for j in range(TOP)
    ]
    as_rows[...] = jnp.zeros_like(as_rows)
    for j in range(TOP):
        as_rows[j : j + 1, :] = trow[j].astype(f32)
        as_rows[TOP + j : TOP + j + 1, :] = rw_rows[j : j + 1, :]
    as_cols[...] = as_rows[...].T

    def picked_rows(e):
        slot = lax.broadcasted_iota(jnp.int32, (cap, rows), 0) + e * cap
        hit = (slot == trow[0]) | (slot == trow[1])
        pick = jnp.where(hit, 1.0, 0.0).astype(bf16)
        return jnp.dot(pick, xe_in[...], preferred_element_type=f32).astype(bf16)

    def send_rows(d, carry):
        e = lax.rem(me_ep + d, ep)
        disp_send[e] = picked_rows(e)
        ep_copy(disp_send.at[e], slots.at[me_ep, me_tp], dp_s.at[d], dp_r.at[d], d).start()
        return carry

    lax.fori_loop(1, ep, send_rows, 0)
    slots[me_ep, me_tp] = picked_rows(me_ep)
    relay(*mixer_part(), 0)

    def arrive(k):
        q = ep_from(k)
        ep_copy(disp_send.at[q], slots.at[q, me_tp], dp_s.at[k], dp_r.at[k], k).wait_recv()
        send(*slot_part(k))

    arrive(1)

    def pass_slots(k, carry):
        arrive(k)
        relay(*slot_part(k - 1), lax.rem(k, 2))
        return carry

    early = ep // 2
    lax.fori_loop(2, early, pass_slots, 0)

    def norm_rows(parts, gain):
        parts = [v.astype(f32) for v in parts]
        mean = sum(jnp.sum(v, axis=-1, keepdims=True) for v in parts) / width
        parts = [v - mean for v in parts]
        spread = sum(jnp.sum(v * v, axis=-1, keepdims=True) for v in parts) / width
        inv = lax.rsqrt(spread + norm_eps)
        return [
            (v * inv * gain[:, p * feat : (p + 1) * feat]).astype(bf16)
            for p, v in enumerate(parts)
        ]

    finish(*mixer_part())
    loads[0].wait()

    def project(i, carry):
        at = pl.ds(pl.multiple_of(i * chunk, chunk), chunk)
        for p, v in enumerate(norm_rows([xm[p, at, :] for p in range(tp)], gain_m)):
            normed[:, p * feat : (p + 1) * feat] = v
        inner = jnp.dot(normed[...], w_in[...], preferred_element_type=f32).astype(bf16)
        ext[pl.ds(pl.multiple_of(RIM + i * chunk, RIM), chunk), :] = inner.astype(f32)
        return carry

    lax.fori_loop(0, rows // chunk, project, 0)
    rim_send[0] = ext[rows : rows + RIM, :].astype(bf16)
    rim_send[1] = ext[RIM : 2 * RIM, :].astype(bf16)
    up_rim = ep_copy(rim_send.at[0], rim_recv.at[0], rim_s.at[0], rim_r.at[0], 1)
    down_rim = ep_copy(rim_send.at[1], rim_recv.at[1], rim_s.at[1], rim_r.at[1], ep - 1)
    up_rim.start()
    down_rim.start()

    lax.fori_loop(early, ep - 1, pass_slots, 0)

    up_rim.wait_recv()
    down_rim.wait_recv()
    low = rim_recv[0].astype(f32)
    high = rim_recv[1].astype(f32)
    ext[0:RIM, :] = jnp.where(me_ep > 0, low, 0.0)
    ext[RIM + rows : 2 * RIM + rows, :] = jnp.where(me_ep < ep - 1, high, 0.0)

    group_width = chan * tp // len(pool_windows)
    channel = me_tp * chan + lax.broadcasted_iota(jnp.int32, (1, chan), 1)
    seq_len = rows * ep
    for i in range(rows // chunk):
        first = RIM + i * chunk
        position = me_ep * rows + i * chunk + lax.broadcasted_iota(jnp.int32, (chunk, 1), 0)
        running = jnp.zeros((chunk, chan), f32)
        result = jnp.zeros((chunk, chan), f32)
        last = 0
        for g, window in enumerate(pool_windows):
            half = window // 2
            for o in list(range(-half, -last)) + list(range(last, half)):
                running = running + ext[first + o : first + o + chunk, :]
            last = half
            lower = jnp.maximum(position - half, 0)
            upper = jnp.minimum(position + half, seq_len)
            counts = (upper - lower).astype(f32)
            member = (channel >= g * group_width) & (channel < (g + 1) * group_width)
            result = jnp.where(member, running / counts, result)
        values = ext[first : first + chunk, :]
        pooled[me_tp, i * chunk : (i + 1) * chunk, :] = (
            (result - values) * scale[...]
        ).astype(bf16)
    send(*pooled_part())
    pass_slots(ep - 1, 0)
    send(*slot_part(0))

    loads[1].wait()
    loads[2].wait()

    def hidden_step(k):
        q = ep_from(k)
        finish(*slot_part(k))
        for p, v in enumerate(norm_rows([slots[q, p] for p in range(tp)], gain_e)):
            block[:, p * feat : (p + 1) * feat] = v
        x = block[...]
        g = jnp.dot(x, gate[...], preferred_element_type=f32)
        u = jnp.dot(x, up[...], preferred_element_type=f32)
        hid[q, me_tp] = (g / (1.0 + jnp.exp(-g)) * u).astype(bf16)
        send(*hidden_part(k))

    units = hid.shape[3]

    def value_step(k):
        q = ep_from(k)
        finish(*hidden_part(k))
        total = jnp.zeros((cap, out_e.shape[1]), f32)
        for p in range(tp):
            total = total + jnp.dot(
                hid[q, p],
                down[p * units : (p + 1) * units, :],
                preferred_element_type=f32,
            )
        return total.astype(bf16)

    def send_value(k):
        q = ep_from(k)
        back_send[q] = value_step(k)
        ep_copy(back_send.at[q], back_recv.at[me_ep], bk_s.at[k], bk_r.at[k], ep - k).start()

    hidden_step(1)
    relay(*slot_part(ep - 1), ep % 2)
    hidden_step(2)
    relay(*slot_part(0), 1 - ep % 2)
    relay(*pooled_part(), 1)
    relay(*hidden_part(1), 0)

    loads[3].wait()
    finish(*pooled_part())

    def mix_out(i, carry):
        at = pl.ds(pl.multiple_of(i * chunk, chunk), chunk)
        total = jnp.zeros((chunk, chan), f32)
        for p in range(tp):
            total = total + jnp.dot(
                pooled[p, at, :],
                w_mix[p * chan : (p + 1) * chan, :],
                preferred_element_type=f32,
            )
        out_m[at, :] = total.astype(bf16)
        return carry

    lax.fori_loop(0, rows // chunk, mix_out, 0)
    loads[4].wait()

    def expert(k, carry):
        hidden_step(k)
        relay(*hidden_part(k - 1), lax.rem(k, 2))
        send_value(k - 2)
        return carry

    lax.fori_loop(3, ep, expert, 0)
    hidden_step(0)
    relay(*hidden_part(ep - 1), ep % 2)
    send_value(ep - 2)
    relay(*hidden_part(0), 1 - ep % 2)
    send_value(ep - 1)

    def combine(e):
        slot = lax.broadcasted_iota(jnp.int32, (rows, cap), 1) + e * cap
        weight = jnp.zeros((rows, cap), f32)
        for j in range(TOP):
            own_slot = as_cols[:, j : j + 1].astype(jnp.int32)
            weight = weight + jnp.where(slot == own_slot, as_cols[:, TOP + j : TOP + j + 1], 0.0)
        coarse = weight.astype(bf16)
        fine = (weight - coarse.astype(f32)).astype(bf16)
        v = back_recv[e]
        return jnp.dot(coarse, v, preferred_element_type=f32) + jnp.dot(
            fine, v, preferred_element_type=f32
        )

    acc[...] = jnp.zeros_like(acc)

    def gather_value(k, carry):
        e = lax.rem(me_ep + k, ep)
        ep_copy(back_send.at[e], back_recv.at[e], bk_s.at[k], bk_r.at[k], k).wait_recv()
        acc[...] += combine(e)
        return carry

    lax.fori_loop(1, ep - 2, gather_value, 0)
    back_recv[me_ep] = value_step(0)
    acc[...] += combine(me_ep)
    lax.fori_loop(ep - 2, ep, gather_value, 0)
    out_e[...] = acc[...].astype(bf16)

    drain(*mixer_part())
    drain(*pooled_part())
    up_rim.wait_send()
    down_rim.wait_send()

    def drain_ep(k, carry):
        e = lax.rem(me_ep + k, ep)
        q = ep_from(k)
        ep_copy(disp_send.at[e], slots.at[me_ep, me_tp], dp_s.at[k], dp_r.at[k], k).wait_send()
        ep_copy(back_send.at[q], back_recv.at[me_ep], bk_s.at[k], bk_r.at[k], ep - k).wait_send()
        return carry

    lax.fori_loop(1, ep, drain_ep, 0)

    def drain_tp(k, carry):
        drain(*slot_part(k))
        drain(*hidden_part(k))
        return carry

    lax.fori_loop(0, ep, drain_tp, 0)


def square(
    ep,
    tp,
    xm_in,
    xe_h,
    gain_m_h,
    gain_e_h,
    scale_h,
    routes_h,
    rw_h,
    w_in_h,
    w_mix_h,
    gate_h,
    up_h,
    down_h,
    out_m_h,
    out_e_h,
    xe_in,
    gain_m,
    gain_e,
    scale,
    route_rows,
    rw_rows,
    out_m,
    out_e,
    w_in,
    w_mix,
    gate,
    up,
    down,
    xm,
    normed,
    block,
    disp_send,
    slots,
    hid,
    pooled,
    back_send,
    back_recv,
    ext,
    rim_send,
    rim_recv,
    acc,
    fin_send,
    fin_recv,
    as_rows,
    as_cols,
    in_sem,
    out_sem,
    w_sem,
    sl_s,
    sl_r,
    xm_s,
    xm_r,
    dp_s,
    dp_r,
    rim_s,
    rim_r,
    po_s,
    po_r,
    hi_s,
    hi_r,
    bk_s,
    bk_r,
    dn_s,
    dn_r,
    fi_s,
    fi_r,
):
    me_ep = lax.axis_index("ep")
    me_tp = lax.axis_index("tp")
    rows, feat = xe_in.shape
    cap = slots.shape[2]
    chan = out_m.shape[1]
    units = hid.shape[3]
    cols = out_e.shape[1]
    width = feat * tp
    chunk = min(rows, 128)

    not_first = me_ep > 0
    not_last = me_ep < ep - 1
    col = lax.rem(me_tp, 2)
    row = me_tp // 2
    beside = row * 2 + (1 - col)
    above = (1 - row) * 2 + col
    across = (1 - row) * 2 + (1 - col)

    barrier = pltpu.get_barrier_semaphore()
    for d in range(1, tp):
        pl.semaphore_signal(
            barrier, inc=1, device_id={"tp": lax.rem(me_tp + d, tp)}, device_id_type=MESH
        )
    for d in range(1, ep):
        pl.semaphore_signal(
            barrier, inc=1, device_id={"ep": lax.rem(me_ep + d, ep)}, device_id_type=MESH
        )

    inputs = [
        pltpu.make_async_copy(h, v, in_sem.at[i])
        for i, (h, v) in enumerate(
            (
                (routes_h, route_rows),
                (rw_h, rw_rows),
                (xe_h, xe_in),
                (gain_m_h, gain_m),
                (gain_e_h, gain_e),
                (scale_h, scale),
            )
        )
    ]
    for load in inputs:
        load.start()
    xm_load = pltpu.make_async_copy(xm_in, xm.at[me_tp], w_sem.at[0])
    xm_load.start()

    def unit_rows(r, c):
        return pl.ds(pl.multiple_of((r * 2 + c) * units, units), units)

    piece = units // 2

    loads = [
        pltpu.make_async_copy(h, v, w_sem.at[i + 1])
        for i, (h, v) in enumerate(
            (
                (w_in_h, w_in),
                (gate_h, gate),
                (up_h, up),
                (w_mix_h, w_mix),
                (down_h.at[unit_rows(0, col), :], down.at[col, 0]),
                (down_h.at[unit_rows(1, col), :], down.at[col, 1]),
            )
        )
    ]
    def tp_copy(src, dst, s, r, peer):
        return pltpu.make_async_remote_copy(
            src_ref=src,
            dst_ref=dst,
            send_sem=s,
            recv_sem=r,
            device_id={"tp": peer},
            device_id_type=MESH,
        )

    def ep_copy(src, dst, s, r, d):
        return pltpu.make_async_remote_copy(
            src_ref=src,
            dst_ref=dst,
            send_sem=s,
            recv_sem=r,
            device_id={"ep": lax.rem(me_ep + d, ep)},
            device_id_type=MESH,
        )

    def send(slot, s, r):
        mine = slot(me_tp)
        tp_copy(mine, mine, s(0), r(0), beside).start()
        tp_copy(mine, mine, s(1), r(1), above).start()

    def relay(slot, s, r, turn):
        tp_copy(slot(beside), slot(beside), s(0), r(0), beside).wait_recv()
        tp_copy(slot(above), slot(above), s(1), r(1), above).wait_recv()
        source = slot((1 - turn) * beside + turn * above)
        tp_copy(source, source, s(2), r(2), (1 - turn) * above + turn * beside).start()

    def finish(slot, s, r):
        tp_copy(slot(across), slot(across), s(2), r(2), across).wait_recv()

    def drain(slot, s, r):
        mine = slot(me_tp)
        for j in range(3):
            tp_copy(mine, mine, s(j), r(j), beside).wait_send()

    def half_rows(h):
        return pl.ds(pl.multiple_of(h * (rows // 2), rows // 2), rows // 2)

    part = cap // 2

    def slot_half(k, p, h):
        return slots.at[ep_from(k), p, pl.ds(h * part, part)]

    def relay_slot(k, turns):
        slot, s, r = slot_part(k)
        tp_copy(slot(beside), slot(beside), s(0), r(0), beside).wait_recv()
        tp_copy(slot(above), slot(above), s(1), r(1), above).wait_recv()
        for h, turn in enumerate(turns):
            source = slot_half(k, (1 - turn) * beside + turn * above, h)
            peer = (1 - turn) * above + turn * beside
            tp_copy(source, source, s(2 + h), r(2 + h), peer).start()

    def finish_slot(k):
        slot, s, r = slot_part(k)
        for h in range(2):
            source = slot_half(k, across, h)
            tp_copy(source, source, s(2 + h), r(2 + h), across).wait_recv()

    def drain_slot(k):
        slot, s, r = slot_part(k)
        for j in range(2):
            tp_copy(slot(me_tp), slot(me_tp), s(j), r(j), beside).wait_send()
        for h in range(2):
            source = slot_half(k, across, h)
            tp_copy(source, source, s(2 + h), r(2 + h), beside).wait_send()

    def mixer_part(h):
        at = half_rows(h)
        return lambda p: xm.at[p, at], lambda j: xm_s.at[h, j], lambda j: xm_r.at[h, j]

    def pooled_part(h):
        at = half_rows(h)
        return lambda p: pooled.at[p, at], lambda j: po_s.at[h, j], lambda j: po_r.at[h, j]

    def ep_from(d):
        return lax.rem(me_ep - d + ep, ep)

    def slot_part(k):
        q = ep_from(k)
        return lambda p: slots.at[q, p], lambda j: sl_s.at[k, j], lambda j: sl_r.at[k, j]

    def hidden_copy(k, part):
        ref = hid.at[ep_from(k), part]
        return tp_copy(ref, ref, hi_s.at[k], hi_r.at[k], above)

    def down_copy(i):
        r, half = i // 2, i % 2
        first = (r * 2 + 1 - col) * units + half * piece
        return tp_copy(
            down_h.at[pl.ds(pl.multiple_of(first, piece), piece), :],
            down.at[col, r, pl.ds(pl.multiple_of(half * piece, piece), piece)],
            dn_s.at[i],
            dn_r.at[i],
            beside,
        )

    def mixer_x(h):
        slot, s, r = mixer_part(h)
        tp_copy(slot(me_tp), slot(me_tp), s(0), r(0), beside).start()

    def mixer_y(h):
        slot, s, r = mixer_part(h)
        tp_copy(slot(me_tp), slot(me_tp), s(1), r(1), above).start()

    for load in inputs[:2]:
        load.wait()
    t0 = lax.broadcasted_iota(jnp.int32, (rows, rows), 0)
    t1 = lax.broadcasted_iota(jnp.int32, (rows, rows), 1)
    names = lax.broadcasted_iota(jnp.int32, (ep, rows), 0)
    named = [jnp.where(route_rows[j : j + 1, :] == names, 1.0, 0.0) for j in range(TOP)]
    ahead = jnp.dot(
        sum(named).astype(bf16),
        jnp.where(t0 < t1, 1.0, 0.0).astype(bf16),
        preferred_element_type=f32,
    )
    trow = [
        route_rows[j : j + 1, :] * cap
        + jnp.sum(named[j] * ahead, axis=0, keepdims=True).astype(jnp.int32)
        for j in range(TOP)
    ]
    as_rows[...] = jnp.zeros_like(as_rows)
    for j in range(TOP):
        as_rows[j : j + 1, :] = trow[j].astype(f32)
        as_rows[TOP + j : TOP + j + 1, :] = rw_rows[j : j + 1, :]
    as_cols[...] = as_rows[...].T

    for load in inputs[2:]:
        load.wait()
    xm_load.wait()
    for load in loads:
        load.start()
    pl.semaphore_wait(barrier, tp + ep - 2)
    starts = {
        "W": lambda k: down_copy(k).start(),
        "XMX": mixer_x,
        "XMY": mixer_y,
    }
    picks_at = ORDER.index(("P", -1))
    for op, k in ORDER[:picks_at]:
        starts[op](k)

    def picked_rows(e):
        slot = lax.broadcasted_iota(jnp.int32, (cap, rows), 0) + e * cap
        hit = (slot == trow[0]) | (slot == trow[1])
        pick = jnp.where(hit, 1.0, 0.0).astype(bf16)
        return jnp.dot(pick, xe_in[...], preferred_element_type=f32).astype(bf16)

    def send_rows(n, carry):
        d = sum(jnp.where(n == i, k, 0) for i, k in enumerate(SENDS))
        e = lax.rem(me_ep + d, ep)
        disp_send[e] = picked_rows(e)
        ep_copy(disp_send.at[e], slots.at[me_ep, me_tp], dp_s.at[d], dp_r.at[d], d).start()
        return carry

    lax.fori_loop(0, ep - 1, send_rows, 0)
    slots[me_ep, me_tp] = picked_rows(me_ep)

    def arrive(k):
        @pl.when(k > 0)
        def _():
            q = ep_from(k)
            ep_copy(disp_send.at[q], slots.at[q, me_tp], dp_s.at[k], dp_r.at[k], k).wait_recv()

        send(*slot_part(k))

    def norm_rows(parts, gain):
        parts = [v.astype(f32) for v in parts]
        mean = sum(jnp.sum(v, axis=-1, keepdims=True) for v in parts) / width
        parts = [v - mean for v in parts]
        spread = sum(jnp.sum(v * v, axis=-1, keepdims=True) for v in parts) / width
        inv = lax.rsqrt(spread + norm_eps)
        return [
            (v * inv * gain[:, p * feat : (p + 1) * feat]).astype(bf16)
            for p, v in enumerate(parts)
        ]

    def project(i, carry):
        at = pl.ds(pl.multiple_of(i * chunk, chunk), chunk)
        for p, v in enumerate(norm_rows([xm[p, at, :] for p in range(tp)], gain_m)):
            normed[:, p * feat : (p + 1) * feat] = v
        inner = jnp.dot(normed[...], w_in[...], preferred_element_type=f32).astype(bf16)
        ext[pl.ds(pl.multiple_of(RIM + i * chunk, RIM), chunk), :] = inner.astype(f32)
        return carry

    up_rim = ep_copy(rim_send.at[0], rim_recv.at[0], rim_s.at[0], rim_r.at[0], 1)
    down_rim = ep_copy(rim_send.at[1], rim_recv.at[1], rim_s.at[1], rim_r.at[1], ep - 1)

    def enter():
        for h in range(2):
            finish(*mixer_part(h))
        lax.fori_loop(0, rows // chunk, project, 0)
        rim_send[0] = ext[rows : rows + RIM, :].astype(bf16)
        rim_send[1] = ext[RIM : 2 * RIM, :].astype(bf16)
        pl.when(not_last)(up_rim.start)
        pl.when(not_first)(down_rim.start)

    for load in loads:
        load.wait()

    def hidden_step(k):
        q = ep_from(k)
        finish_slot(k)
        for p, v in enumerate(norm_rows([slots[q, p] for p in range(tp)], gain_e)):
            block[:, p * feat : (p + 1) * feat] = v
        x = block[...]
        g = jnp.dot(x, gate[...], preferred_element_type=f32)
        u = jnp.dot(x, up[...], preferred_element_type=f32)
        hid[q, row] = (g / (1.0 + jnp.exp(-g)) * u).astype(bf16)
        hidden_copy(k, row).start()

    def value_step(k):
        q = ep_from(k)
        hidden_copy(k, 1 - row).wait_recv()
        return [
            (
                jnp.dot(hid[q, 0], down[c, 0], preferred_element_type=f32)
                + jnp.dot(hid[q, 1], down[c, 1], preferred_element_type=f32)
            ).astype(bf16)
            for c in range(2)
        ]

    def send_value(k):
        q = ep_from(k)
        values = value_step(k)

        @pl.when(k > 0)
        def _():
            for c in range(2):
                back_send[q, c] = values[c]
            ep_copy(back_send.at[q], back_recv.at[me_ep], bk_s.at[k], bk_r.at[k], ep - k).start()

        @pl.when(k == 0)
        def _():
            for c in range(2):
                back_recv[me_ep, c] = values[c]

    def combine(e):
        slot = lax.broadcasted_iota(jnp.int32, (rows, cap), 1) + e * cap
        hit = None
        weight = jnp.zeros((rows, 1), f32)
        for j in range(TOP):
            own_slot = as_cols[:, j : j + 1].astype(jnp.int32)
            here = (own_slot >= e * cap) & (own_slot < (e + 1) * cap)
            weight = weight + jnp.where(here, as_cols[:, TOP + j : TOP + j + 1], 0.0)
            hit = slot == own_slot if hit is None else hit | (slot == own_slot)
        pick = jnp.where(hit, 1.0, 0.0).astype(bf16)
        for c in range(2):
            acc[c] += weight * jnp.dot(pick, back_recv[e, c], preferred_element_type=f32)

    def gather_value(k):
        e = lax.rem(me_ep + k, ep)

        @pl.when(k > 0)
        def _():
            ep_copy(back_send.at[e], back_recv.at[e], bk_s.at[k], bk_r.at[k], k).wait_recv()

        combine(e)

    def pool():
        ext[0:RIM, :] = jnp.zeros((RIM, chan), f32)
        ext[RIM + rows : 2 * RIM + rows, :] = jnp.zeros((RIM, chan), f32)

        @pl.when(not_first)
        def _():
            up_rim.wait_recv()
            ext[0:RIM, :] = rim_recv[0].astype(f32)

        @pl.when(not_last)
        def _():
            down_rim.wait_recv()
            ext[RIM + rows : 2 * RIM + rows, :] = rim_recv[1].astype(f32)

        group_width = chan * tp // len(pool_windows)
        channel = me_tp * chan + lax.broadcasted_iota(jnp.int32, (1, chan), 1)
        seq_len = rows * ep
        for i in range(rows // chunk):
            first = RIM + i * chunk
            position = me_ep * rows + i * chunk + lax.broadcasted_iota(jnp.int32, (chunk, 1), 0)
            running = jnp.zeros((chunk, chan), f32)
            result = jnp.zeros((chunk, chan), f32)
            last = 0
            for g, window in enumerate(pool_windows):
                half = window // 2
                for o in list(range(-half, -last)) + list(range(last, half)):
                    running = running + ext[first + o : first + o + chunk, :]
                last = half
                lower = jnp.maximum(position - half, 0)
                upper = jnp.minimum(position + half, seq_len)
                counts = (upper - lower).astype(f32)
                member = (channel >= g * group_width) & (channel < (g + 1) * group_width)
                result = jnp.where(member, running / counts, result)
            values = ext[first : first + chunk, :]
            pooled[me_tp, i * chunk : (i + 1) * chunk, :] = (
                (result - values) * scale[...]
            ).astype(bf16)
        for h in range(2):
            send(*pooled_part(h))

    acc[...] = jnp.zeros_like(acc)

    final = tp_copy(fin_send, fin_recv, fi_s.at[0], fi_r.at[0], beside)

    def exchange(k):
        fin_send[...] = acc[1 - col].astype(bf16)
        final.start()

    def mixed_out(h):
        at = half_rows(h)
        return pltpu.make_async_copy(out_m.at[at], out_m_h.at[at], out_sem.at[h])

    def mix_out(h):
        finish(*pooled_part(h))

        def mix(i, carry):
            at = pl.ds(pl.multiple_of(h * (rows // 2) + i * chunk, chunk), chunk)
            total = jnp.zeros((chunk, chan), f32)
            for p in range(tp):
                total = total + jnp.dot(
                    pooled[p, at, :],
                    w_mix[p * chan : (p + 1) * chan, :],
                    preferred_element_type=f32,
                )
            out_m[at, :] = total.astype(bf16)
            return carry

        lax.fori_loop(0, rows // 2 // chunk, mix, 0)
        mixed_out(h).start()

    def await_down():
        for i in range(4):
            down_copy(i).wait_recv()

    body = dict(
        starts,
        A=arrive,
        H=hidden_step,
        V=send_value,
        G=gather_value,
        ENT=lambda k: enter(),
        POOL=lambda k: pool(),
        EX=exchange,
        MIX=mix_out,
    )
    turned = {
        "R": lambda k, turns: relay_slot(k, turns),
        "RXM": lambda k, turns: relay(*mixer_part(k), turns[0]),
        "RPO": lambda k, turns: relay(*pooled_part(k), turns[0]),
    }

    steps = [[]]
    for op, k in ORDER[picks_at + 1 :]:
        if steps[-1] and PLACES.index(op) <= PLACES.index(steps[-1][-1][0]):
            steps.append([])
        steps[-1].append((op, k))
    where = {op: [] for op in PLACES}
    for n, entries in enumerate(steps):
        for op, k in entries:
            where[op].append((n, k))

    def step(n, carry):
        for op in PLACES:
            spots = where[op]
            if not spots:
                continue
            due = functools.reduce(jnp.logical_or, [n == i for i, _ in spots])
            k = sum(jnp.where(n == i, v, 0) for i, v in spots)

            @pl.when(due)
            def _(op=op, k=k, spots=spots):
                if op == "V":
                    pl.when(n == spots[0][0])(await_down)
                if op in turned:
                    turns = []
                    for h in range(2):
                        ups = [i for i, v in spots if (op, v, h) in OVER_X]
                        turns.append(sum(jnp.where(n == i, 1, 0) for i in ups) if ups else 0)
                    turned[op](k, turns)
                else:
                    body[op](k)

        return carry

    lax.fori_loop(0, len(steps), step, 0)
    final.wait_recv()
    out_e[...] = (acc[col] + fin_recv[...].astype(f32)).astype(bf16)
    last = pltpu.make_async_copy(out_e, out_e_h, out_sem.at[2])
    last.start()

    final.wait_send()
    for h in range(2):
        drain(*mixer_part(h))
        drain(*pooled_part(h))
    pl.when(not_last)(up_rim.wait_send)
    pl.when(not_first)(down_rim.wait_send)
    for i in range(4):
        down_copy(i).wait_send()

    def drain_ep(k, carry):
        e = lax.rem(me_ep + k, ep)
        q = ep_from(k)
        ep_copy(disp_send.at[e], slots.at[me_ep, me_tp], dp_s.at[k], dp_r.at[k], k).wait_send()
        ep_copy(back_send.at[q], back_recv.at[me_ep], bk_s.at[k], bk_r.at[k], ep - k).wait_send()
        return carry

    lax.fori_loop(1, ep, drain_ep, 0)

    def drain_tp(k, carry):
        drain_slot(k)
        hidden_copy(k, row).wait_send()
        return carry

    lax.fori_loop(0, ep, drain_tp, 0)
    for h in range(2):
        mixed_out(h).wait()
    last.wait()


def square_scratch(ep, tp, rows, feat, cap, chan, units, cols, shapes):
    dma = pltpu.SemaphoreType.DMA
    width = feat * tp
    w_in, w_mix, gate, up = shapes
    return [
        pltpu.VMEM((rows, feat), bf16),
        pltpu.VMEM((1, width), f32),
        pltpu.VMEM((1, width), f32),
        pltpu.VMEM((1, chan), f32),
        pltpu.VMEM((TOP, rows), jnp.int32),
        pltpu.VMEM((TOP, rows), f32),
        pltpu.VMEM((rows, chan), bf16),
        pltpu.VMEM((rows, cols), bf16),
        pltpu.VMEM(w_in, bf16),
        pltpu.VMEM(w_mix, bf16),
        pltpu.VMEM(gate, bf16),
        pltpu.VMEM(up, bf16),
        pltpu.VMEM((2, 2, units, cols), bf16),
        pltpu.VMEM((tp, rows, feat), bf16),
        pltpu.VMEM((min(rows, 128), width), bf16),
        pltpu.VMEM((cap, width), bf16),
        pltpu.VMEM((ep, cap, feat), bf16),
        pltpu.VMEM((ep, tp, cap, feat), bf16),
        pltpu.VMEM((ep, 2, cap, units), bf16),
        pltpu.VMEM((tp, rows, chan), bf16),
        pltpu.VMEM((ep, 2, cap, cols), bf16),
        pltpu.VMEM((ep, 2, cap, cols), bf16),
        pltpu.VMEM((rows + 2 * RIM, chan), f32),
        pltpu.VMEM((2, RIM, chan), bf16),
        pltpu.VMEM((2, RIM, chan), bf16),
        pltpu.VMEM((2, rows, cols), f32),
        pltpu.VMEM((rows, cols), bf16),
        pltpu.VMEM((rows, cols), bf16),
        pltpu.VMEM((8, rows), f32),
        pltpu.VMEM((rows, 8), f32),
        dma((6,)),
        dma((3,)),
        dma((7,)),
        dma((ep, 4)),
        dma((ep, 4)),
        dma((2, 3)),
        dma((2, 3)),
        dma((ep,)),
        dma((ep,)),
        dma((2,)),
        dma((2,)),
        dma((2, 3)),
        dma((2, 3)),
        dma((ep,)),
        dma((ep,)),
        dma((ep,)),
        dma((ep,)),
        dma((4,)),
        dma((4,)),
        dma((1,)),
        dma((1,)),
    ]


def hand_over(m_in, e_in, m_out, e_out, held, sem):
    pieces = held.shape[1]
    rows = held.shape[2]
    ways = []
    for i, (src, dst) in enumerate(((m_in, m_out), (e_in, e_out))):
        for j in range(pieces):
            at = pl.ds(j * rows, rows)
            into = pltpu.make_async_copy(src.at[at], held.at[i, j], sem.at[0, i, j])
            into.start()
            out = pltpu.make_async_copy(held.at[i, j], dst.at[at], sem.at[1, i, j])
            ways.append((into, out))
    for into, out in ways:
        into.wait()
        out.start()
    for _, out in ways:
        out.wait()


def on_device(
    mixer_rows,
    expert_rows,
    mixer_gain,
    pool_scale,
    w_in,
    w_mix_out,
    expert_gain,
    expert_gate,
    expert_up,
    expert_down,
    routes,
    route_weight,
    *,
    ep,
    tp,
):
    rows, feat = mixer_rows.shape
    width = feat * tp
    cap = (3 * TOP * rows + 2 * ep - 1) // (2 * ep)
    chan = w_in.shape[1]
    units = expert_gate.shape[2]
    vmem = pl.BlockSpec(memory_space=pltpu.VMEM)
    hbm = pl.BlockSpec(memory_space=pl.ANY)
    dma = pltpu.SemaphoreType.DMA
    square_ok = tp == 4 and ep == len(SENDS) + 1
    whole_scratch = [
        pltpu.VMEM(w_in.shape, bf16),
        pltpu.VMEM(w_mix_out.shape, bf16),
        pltpu.VMEM(expert_gate.shape[1:], bf16),
        pltpu.VMEM(expert_up.shape[1:], bf16),
        pltpu.VMEM(expert_down.shape[1:], bf16),
        pltpu.VMEM((tp, rows, feat), bf16),
        pltpu.VMEM((min(rows, 128), width), bf16),
        pltpu.VMEM((cap, width), bf16),
        pltpu.VMEM((ep, cap, feat), bf16),
        pltpu.VMEM((ep, tp, cap, feat), bf16),
        pltpu.VMEM((ep, tp, cap, units), bf16),
        pltpu.VMEM((tp, rows, chan), bf16),
        pltpu.VMEM((ep, cap, expert_down.shape[2]), bf16),
        pltpu.VMEM((ep, cap, expert_down.shape[2]), bf16),
        pltpu.VMEM((rows + 2 * RIM, chan), f32),
        pltpu.VMEM((2, RIM, chan), bf16),
        pltpu.VMEM((2, RIM, chan), bf16),
        pltpu.VMEM((rows, expert_down.shape[2]), f32),
        pltpu.VMEM((8, rows), f32),
        pltpu.VMEM((rows, 8), f32),
        dma((6,)),
        dma((ep, tp - 1)),
        dma((ep, tp - 1)),
        dma((tp - 1,)),
        dma((tp - 1,)),
        dma((ep,)),
        dma((ep,)),
        dma((2,)),
        dma((2,)),
        dma((tp - 1,)),
        dma((tp - 1,)),
        dma((ep, tp - 1)),
        dma((ep, tp - 1)),
        dma((ep,)),
        dma((ep,)),
    ]
    if square_ok:
        shapes = (w_in.shape, w_mix_out.shape, expert_gate.shape[1:], expert_up.shape[1:])
        cols = expert_down.shape[2]
        whole_scratch = square_scratch(ep, tp, rows, feat, cap, chan, units, cols, shapes)
    result = pl.pallas_call(
        functools.partial(square if square_ok else fused, ep, tp),
        out_shape=(
            jax.ShapeDtypeStruct((rows, w_mix_out.shape[1]), bf16),
            jax.ShapeDtypeStruct((rows, expert_down.shape[2]), bf16),
        ),
        in_specs=[hbm if square_ok else vmem] * 7 + [hbm] * 5,
        out_specs=(hbm, hbm) if square_ok else (vmem, vmem),
        scratch_shapes=whole_scratch,
        compiler_params=pltpu.CompilerParams(
            collective_id=0, has_side_effects=True, vmem_limit_bytes=62 * 1024 * 1024
        ),
    )(
        mixer_rows,
        expert_rows,
        mixer_gain.reshape(1, width),
        expert_gain.reshape(1, width),
        pool_scale.reshape(1, chan),
        routes.T,
        route_weight.T,
        w_in,
        w_mix_out,
        expert_gate.reshape(expert_gate.shape[1:]),
        expert_up.reshape(expert_up.shape[1:]),
        expert_down.reshape(expert_down.shape[1:]),
    )
    if not square_ok:
        return result
    pieces = 2
    return pl.pallas_call(
        hand_over,
        out_shape=tuple(jax.ShapeDtypeStruct(v.shape, v.dtype) for v in result),
        in_specs=[hbm, hbm],
        out_specs=(hbm, hbm),
        scratch_shapes=[
            pltpu.VMEM((2, pieces, rows // pieces, cols), bf16),
            pltpu.SemaphoreType.DMA((2, 2, pieces)),
        ],
    )(*result)


def solution(mesh):
    return jax.shard_map(
        functools.partial(on_device, ep=mesh.shape["ep"], tp=mesh.shape["tp"]),
        mesh=mesh,
        in_specs=(
            P("ep", "tp"),
            P("ep", "tp"),
            P(),
            P("tp"),
            P(None, "tp"),
            P(None, "tp"),
            P(),
            P("ep", None, "tp"),
            P("ep", None, "tp"),
            P("ep", None, "tp"),
            P("ep", None),
            P("ep", None),
        ),
        out_specs=(P("ep", "tp"), P("ep", "tp")),
        check_vma=False,
    )
```
